32 devices in a mesh: sp: 8 (over z, x), tp: 4 (over y, core).
Axes of the slice: x: 2, y: 2, z: 4, core: 2. Of those that a mesh axis runs over, the one named last changes fastest.
Arguments:
- queries: bfloat16 [8192, 1024], P('sp', 'tp'), may hold values from -75 to 75
- key_rows: bfloat16 [8192, 1024], P('sp', 'tp'), may hold values from -4 to 4
- value_rows: bfloat16 [8192, 1024], P('sp', 'tp'), may hold values from -6 to 6
- cum_gate: float32 [16, 8192], P('tp'), may hold values from -1172 to 0, as said below
- residual: bfloat16 [8192, 2048], P(('sp', 'tp')), may hold values from -6 to 6
- out_weight: bfloat16 [1024, 2048], replicated, may hold values from -0.1875 to 0.1875
- gain_mix: float32 [2048], replicated, may hold values from 0.1 to 1.9
- gain_pre: float32 [2048], replicated, may hold values from 0.1 to 1.9
- gain_post: float32 [2048], replicated, may hold values from 0.1 to 1.9
- route_ids: int32 [8192, 2], P(('sp', 'tp')), may hold values from 0 to 31, all different within a row; in each aligned block of 256 rows (0 to 255, 256 to 511, ...) at most 22 rows name the same one
- route_weight: float32 [8192, 2], P(('sp', 'tp')), may hold values from 0.2 to 1
- w_gate: bfloat16 [32, 2048, 512], P(('sp', 'tp')), may hold values from -0.125 to 0.125
- w_up: bfloat16 [32, 2048, 512], P(('sp', 'tp')), may hold values from -0.125 to 0.125
- w_down: bfloat16 [32, 512, 2048], P(('sp', 'tp')), may hold values from -0.25 to 0.25
Outputs:
- layer_out: bfloat16 [8192, 2048], P(('sp', 'tp'))
The draws below stay inside these ranges and needn't reach their ends.
Inputs may be any that keep to these rules, and one draw needn't show every extreme that they name: `route_ids`: each row names 2 different experts; in the rows of one device no expert is named more than 22 times, a bound that some block reaches. `cum_gate`: along the positions each head's values never rise.
All inputs are finite; a program needn't handle non-finite values.
Results may differ from the reference program's by a relative error of at most 0.018.
Values may be sent and summed in bfloat16 or wider, within the bound.
A program may use at most 128 MiB of HBM per device.

```python
import math
import jax
import jax.numpy as jnp
import numpy as np
from jax import lax

D = 2048
ATTENTION_HEADS = 16
HEAD_DIM = 64
FF = 512
TOP = 2
TOK_DEV = 1024
TOKEN_COUNT = 8192
ROWS = 256
EXPERTS = 32
CAP = 22
N_SP = 8
N_TP = 4


def draw_queries(key, part):
    sample = jax.random.normal(jax.random.fold_in(key, 1), (TOKEN_COUNT, ATTENTION_HEADS * HEAD_DIM), jnp.float32)
    return jnp.clip(sample, -4.0, 4.0).astype(jnp.bfloat16)


def draw_key_rows(key, part):
    sample = jax.random.normal(jax.random.fold_in(key, 2), (TOKEN_COUNT, ATTENTION_HEADS * HEAD_DIM), jnp.float32)
    return jnp.clip(sample, -4.0, 4.0).astype(jnp.bfloat16)


def draw_cum_gate(key, part):
    key_o, key_s, key_f, key_r, key_b, random_key_position, random_key_log = jax.random.split(jax.random.fold_in(key, 5), 7)
    shuffle = jax.random.permutation(key_o, ATTENTION_HEADS)
    slow_head = shuffle < ATTENTION_HEADS // 2
    slow_total = jax.random.uniform(key_s, (ATTENTION_HEADS,), jnp.float32, 0.4, 1.0)
    fast_rate = jnp.exp(jax.random.uniform(key_f, (ATTENTION_HEADS,), jnp.float32, -4.6, -3.4))
    step_rate = jnp.where(slow_head, slow_total / TOKEN_COUNT, fast_rate)
    blocks = TOKEN_COUNT // TOK_DEV
    roughness = jnp.exp(jax.random.uniform(key_r, (ATTENTION_HEADS, blocks, TOK_DEV), jnp.float32, -0.7, 0.7))
    block_factor = jnp.exp(jax.random.uniform(key_b, (ATTENTION_HEADS, blocks, 1), jnp.float32, -0.7, 0.7))
    logarithm_steps = step_rate[:, None] * (roughness * block_factor).reshape(ATTENTION_HEADS, TOKEN_COUNT)
    spike_position = jax.random.randint(random_key_position, (ATTENTION_HEADS, 2), 0, TOKEN_COUNT)
    spike_decay = -jnp.log(1.0 - jax.random.uniform(random_key_log, (ATTENTION_HEADS, 2), jnp.float32, 0.2, 0.45))
    index_of_head = jnp.broadcast_to(lax.iota(jnp.int32, ATTENTION_HEADS)[:, None], (ATTENTION_HEADS, 2))
    logarithm_steps = logarithm_steps.at[index_of_head, spike_position].add(spike_decay)
    return -jnp.cumsum(logarithm_steps, axis=1)


def steps_of(own_key, extent, cuts, least, high):
    def one(position, parts):
        draws = jax.random.uniform(jax.random.fold_in(jax.random.fold_in(own_key, 6), position), (parts,), jnp.float32, least / len(cuts), high / len(cuts))
        return jnp.repeat(jnp.exp(draws), extent[position] // parts).reshape((-1,) + (1,) * (len(extent) - position - 1))

    level = one(*cuts[0])
    for cut in cuts[1:]:
        level = level * one(*cut)
    return level


def shared_out(own_key, own, number, rows, number_of, top, bound, skew):
    ranking = jax.random.permutation(own_key, number_of)
    heavy_load, ordinary = shares(number_of, rows * top, bound, skew, True), shares(number_of, rows * top, bound, skew, False)
    places = jnp.arange(number_of)

    def named(lengths, offset_by):
        used = int((lengths > 0).sum())
        fixed = max(1, used // 4)
        passed = fixed + (places - fixed + offset_by * (used - fixed)) % max(1, number_of - fixed)
        return jnp.zeros((number_of,), jnp.int32).at[ranking[jnp.where(places < fixed, places, passed)]].set(jnp.asarray(lengths, jnp.int32))

    lengths = jnp.where(number % 4 == 0, named(heavy_load, number // 4), named(ordinary, number - number // 4 - 1))
    mixed = jax.random.permutation(jax.random.fold_in(own, 3), number_of)
    source_of, taker = mixed[0:number_of // 2 * 2:2], mixed[1:number_of // 2 * 2:2]
    slack = jnp.minimum(lengths[source_of] - 1, bound - lengths[taker]) // 2
    slack = jnp.where((source_of == ranking[0]) | (taker == ranking[0]) | (lengths[taker] == 0), 0, jnp.maximum(slack, 0))
    passed = jax.random.randint(jax.random.fold_in(own, 4), (number_of // 2,), 0, 1 << 20) % (slack + 1)
    lengths = lengths.at[source_of].add(-passed).at[taker].add(passed)
    labels = jnp.searchsorted(jnp.cumsum(lengths), jnp.arange(rows * top), side="right").astype(jnp.int32)
    grid = labels.reshape(top, rows).T
    grid = grid[jax.random.permutation(jax.random.fold_in(own, 1), rows)]
    offset_by = jax.random.randint(jax.random.fold_in(own, 2), (rows, 1), 0, top)
    return jnp.take_along_axis(grid, (jnp.arange(top)[None, :] + offset_by) % top, axis=1)


def shares(count, total, reach, skew, full):
    portions = [(1 << 20) // math.isqrt(rank ** skew) + 1 for rank in range(1, count + 1)]
    largest = reach if full else min(reach, max(-(-total // count), total * portions[0] // sum(portions)))
    least = 1 if total - largest >= count - 1 else 0
    holding, spare = [largest] + [least] * (count - 1), total - largest - least * (count - 1)
    while spare > 0:
        free = [i for i in range(1, count) if holding[i] < largest] or [i for i in range(1, count) if holding[i] < reach]
        pool, remaining = sum([portions[i] for i in free]), spare
        for i in free:
            more = min(reach - holding[i], max(1, remaining * portions[i] // pool), spare)
            holding[i] = holding[i] + more
            spare = spare - more
    return np.array(holding)


def scatter_about(own_key, dims, deviation, reach, shards=(), kind=jnp.bfloat16):
    values = jax.random.normal(own_key, dims, jnp.float32) * deviation
    if len(shards) > 0:
        values = steps_of(own_key, dims, shards, -0.22, 0.18) * values
    return jnp.clip(values, min=-reach, max=reach).astype(kind)


def setup_inputs(seed: int = 0) -> dict:
    keys = jax.random.split(jax.random.key(seed), 15)
    queries = draw_queries(jax.random.fold_in(keys[14], 71), 0)
    key_rows = draw_key_rows(jax.random.fold_in(keys[14], 71), 0)
    value_rows = scatter_about(keys[2], (TOKEN_COUNT, ATTENTION_HEADS * HEAD_DIM), 1.0, 6.0, ((0, 8), (1, 4)))
    cum_gate = draw_cum_gate(jax.random.fold_in(keys[14], 71), 0)
    residual = scatter_about(keys[4], (TOKEN_COUNT, D), 1.0, 6.0, ((0, 32),))
    out_weight = scatter_about(keys[5], (ATTENTION_HEADS * HEAD_DIM, D), (ATTENTION_HEADS * HEAD_DIM) ** -0.5, 0.1875)
    gain_mix = jnp.clip(1.0 + 0.18 * jax.random.normal(keys[6], (D,), jnp.float32), 0.1, 1.9)
    gain_pre = jnp.clip(1.0 + 0.18 * jax.random.normal(keys[7], (D,), jnp.float32), 0.1, 1.9)
    gain_post = jnp.clip(1.0 + 0.18 * jax.random.normal(keys[8], (D,), jnp.float32), 0.1, 1.9)
    route_ids_keys = jax.random.split(jax.random.fold_in(keys[9], 1), TOKEN_COUNT // ROWS)
    route_ids_turns = jax.random.permutation(jax.random.fold_in(keys[9], 3), TOKEN_COUNT // ROWS)
    route_ids = jax.vmap(lambda own, number: shared_out(jax.random.fold_in(keys[9], 2), own, number, ROWS, EXPERTS, TOP, CAP, 1))(route_ids_keys, route_ids_turns).reshape((TOKEN_COUNT, TOP))
    route_weight = jnp.clip(jnp.exp(math.log(1.0) - 1.609438 * jax.random.uniform(keys[10], (TOKEN_COUNT, TOP), jnp.float32) ** steps_of(keys[10], (TOKEN_COUNT, TOP), ((0, 32),), -0.2, 0.2)), 0.2, 1.0)
    w_gate = scatter_about(keys[11], (EXPERTS, D, FF), D ** -0.5, 0.125, ((0, 32),))
    w_up = scatter_about(keys[12], (EXPERTS, D, FF), D ** -0.5, 0.125, ((0, 32),))
    w_down = scatter_about(keys[13], (EXPERTS, FF, D), FF ** -0.5, 0.25, ((0, 32),))
    return {"queries": queries, "key_rows": key_rows, "value_rows": value_rows, "cum_gate": cum_gate, "residual": residual, "out_weight": out_weight, "gain_mix": gain_mix, "gain_pre": gain_pre, "gain_post": gain_post, "route_ids": route_ids, "route_weight": route_weight, "w_gate": w_gate, "w_up": w_up, "w_down": w_down}


NORM_EPS = 1e-06
MASKED = -1e+30

def rms_scale(rows, gain):
    mean_sq = lax.optimization_barrier(jnp.mean(rows * rows, axis=-1, keepdims=True))
    return rows * lax.rsqrt(mean_sq + NORM_EPS) * gain

def attend(running, queries, gate_q, q_start, key_part, value_part, gate_k, k_start):
    row_peak, row_total, weighted = running
    scores = jnp.einsum('qhd,khd->hqk', queries.astype(jnp.float32), key_part.astype(jnp.float32)) * HEAD_DIM ** (-0.5)
    scores = scores + gate_q[:, :, None] - gate_k[:, None, :]
    query_pos = q_start + lax.iota(jnp.int32, queries.shape[0])
    key_pos = k_start + lax.iota(jnp.int32, key_part.shape[0])
    allowed = (key_pos[None, :] <= query_pos[:, None])[None]
    scores = jnp.where(allowed, scores, MASKED)
    new_peak = jnp.maximum(row_peak, lax.optimization_barrier(jnp.max(scores, axis=-1)))
    unnorm = jnp.where(allowed, jnp.exp(scores - new_peak[..., None]), 0.0)
    rescale = jnp.exp(row_peak - new_peak)
    row_total = row_total * rescale + lax.optimization_barrier(jnp.sum(unnorm, axis=-1))
    probs = lax.optimization_barrier(unnorm.astype(jnp.bfloat16)).astype(jnp.float32)
    weighted = weighted * rescale.T[:, :, None] + jnp.einsum('hqk,khd->qhd', probs, value_part.astype(jnp.float32))
    return (new_peak, row_total, weighted)

def attention(queries, key_rows, value_rows, cum_gate):
    query_heads = queries.reshape(TOKEN_COUNT, ATTENTION_HEADS, HEAD_DIM)
    key_heads = key_rows.reshape(TOKEN_COUNT, ATTENTION_HEADS, HEAD_DIM)
    value_heads = value_rows.reshape(TOKEN_COUNT, ATTENTION_HEADS, HEAD_DIM)

    def one_block(block_index):
        q_start = block_index * TOK_DEV
        query_block = lax.dynamic_slice_in_dim(query_heads, q_start, TOK_DEV, 0)
        gate_q = lax.dynamic_slice_in_dim(cum_gate, q_start, TOK_DEV, 1)
        initial = (jnp.full((ATTENTION_HEADS, TOK_DEV), MASKED, jnp.float32), jnp.zeros((ATTENTION_HEADS, TOK_DEV), jnp.float32), jnp.zeros((TOK_DEV, ATTENTION_HEADS, HEAD_DIM), jnp.float32))

        def key_block(other, running):
            k_start = (other * TOK_DEV).astype(jnp.int32)
            return attend(running, query_block, gate_q, q_start, lax.dynamic_slice_in_dim(key_heads, k_start, TOK_DEV, 0), lax.dynamic_slice_in_dim(value_heads, k_start, TOK_DEV, 0), lax.dynamic_slice_in_dim(cum_gate, k_start, TOK_DEV, 1), k_start)
        row_peak, row_total, weighted = lax.fori_loop(jnp.int32(0), block_index + 1, key_block, initial)
        return (weighted / row_total.T[:, :, None]).astype(jnp.bfloat16)
    blocks = lax.map(one_block, jnp.arange(N_SP, dtype=jnp.int32))
    return blocks.reshape(TOKEN_COUNT, ATTENTION_HEADS * HEAD_DIM)

def route_experts(normed, route_ids, route_weight, w_gate, w_up, w_down):
    sources = N_SP * N_TP
    flat_ids = route_ids.reshape(sources, ROWS * TOP)
    onehot = (flat_ids[:, :, None] == jnp.arange(EXPERTS, dtype=jnp.int32)[None, None, :]).astype(jnp.int32)
    slot_rank = (lax.optimization_barrier(jnp.sum(jnp.cumsum(onehot, axis=1) * onehot, axis=2)) - 1).astype(jnp.int32)
    slot_index = flat_ids * (sources * CAP) + jnp.arange(sources, dtype=jnp.int32)[:, None] * CAP + slot_rank
    slot_index = slot_index.reshape(-1).astype(jnp.int32)
    token_index = jnp.arange(TOKEN_COUNT * TOP, dtype=jnp.int32) // TOP
    slot_count = EXPERTS * sources * CAP
    source_row = jnp.zeros((slot_count,), jnp.int32).at[slot_index].set(token_index)
    slot_weight = jnp.zeros((slot_count,), jnp.float32).at[slot_index].set(route_weight.reshape(-1))

    def one_expert(summed, expert):
        offset = (expert * sources * CAP).astype(jnp.int32)
        picked_rows = lax.dynamic_slice_in_dim(source_row, offset, sources * CAP)
        weights = lax.dynamic_slice_in_dim(slot_weight, offset, sources * CAP)
        routed = normed[picked_rows]
        gate_act = jnp.dot(routed, w_gate[expert], preferred_element_type=jnp.float32)
        up_act = jnp.dot(routed, w_up[expert], preferred_element_type=jnp.float32)
        hidden = (jax.nn.silu(gate_act) * up_act).astype(jnp.bfloat16)
        result = jnp.dot(hidden, w_down[expert], preferred_element_type=jnp.float32).astype(jnp.bfloat16)
        summed = summed.at[picked_rows].add(weights[:, None] * result.astype(jnp.float32))
        return (summed, None)
    summed, _ = lax.scan(one_expert, jnp.zeros((TOKEN_COUNT, D), jnp.float32), jnp.arange(EXPERTS, dtype=jnp.int32))
    return summed

def reference(queries, key_rows, value_rows, cum_gate, residual, out_weight, gain_mix, gain_pre, gain_post, route_ids, route_weight, w_gate, w_up, w_down):
    attended = attention(queries, key_rows, value_rows, cum_gate)
    projected = jnp.dot(attended, out_weight, preferred_element_type=jnp.float32)
    stream = (residual.astype(jnp.float32) + rms_scale(projected, gain_mix)).astype(jnp.bfloat16)
    stream_wide = lax.optimization_barrier(stream).astype(jnp.float32)
    normed = rms_scale(stream_wide, gain_pre).astype(jnp.bfloat16)
    combined = route_experts(normed, route_ids, route_weight, w_gate, w_up, w_down)
    return (stream_wide + rms_scale(combined, gain_post)).astype(jnp.bfloat16)
```

```python
import functools
import math

import jax
import jax.numpy as jnp
from jax import lax
from jax.experimental import pallas as pl
from jax.experimental.pallas import tpu as pltpu
from jax.sharding import PartitionSpec as P

HEAD_DIM = 64
NORM_EPS = 1e-06
MASKED = -1e30
MESH = pl.DeviceIdType.MESH
CHUNKS = 4
GROUPS = 4


def rms_scale(rows, gain):
    mean_sq = jnp.mean(rows * rows, axis=-1, keepdims=True)
    return rows * lax.rsqrt(mean_sq + NORM_EPS) * gain


def bf16_parts(values):
    parts = []
    for _ in range(3):
        part = lax.reduce_precision(values, 8, 7)
        parts.append(part.astype(jnp.bfloat16))
        values = values - part
    return parts


def pack_kernel(q_ref, k_ref, v_ref, one_ref, two_ref, *, shares, n_tp):
    tok_dev, width = q_ref.shape
    first = tok_dev - two_ref.shape[1]
    rows_dev = tok_dev // n_tp
    sub = rows_dev // shares
    for h in range(width // HEAD_DIM):
        cols = pl.ds(h * HEAD_DIM, HEAD_DIM)
        pairs = jnp.concatenate((k_ref[:, cols], v_ref[:, cols]), axis=1)
        for r in range(shares):
            dest = h * shares + r
            one_ref[dest, :first] = pairs[:first]
            two_ref[dest] = pairs[first:]
            for t in range(n_tp // 2):
                low, high = (
                    q_ref[pl.ds((t + step) * rows_dev + r * sub, sub), cols]
                    for step in (0, n_tp // 2)
                )
                one_ref[dest, pl.ds(first + t * sub, sub)] = jnp.concatenate((low, high), axis=1)


def pack(queries, key_rows, value_rows, first, shares, n_tp):
    tok_dev, width = queries.shape
    dests = width // HEAD_DIM * shares
    half = tok_dev // shares // 2
    shapes = [(dests, first + half, 2 * HEAD_DIM), (dests, tok_dev - first, 2 * HEAD_DIM)]
    return pl.pallas_call(
        functools.partial(pack_kernel, shares=shares, n_tp=n_tp),
        out_shape=[jax.ShapeDtypeStruct(shape, jnp.bfloat16) for shape in shapes],
        in_specs=[pl.BlockSpec(memory_space=pltpu.VMEM)] * 3,
        out_specs=[pl.BlockSpec(memory_space=pltpu.VMEM)] * 2,
        compiler_params=pltpu.CompilerParams(vmem_limit_bytes=32 * 2**20),
        name="pack",
    )(queries, key_rows, value_rows)


def assemble_kernel(in_ref, out_ref, *, shares, n_tp, local_heads):
    half = in_ref.shape[1]
    for t in range(n_tp):
        for h in range(0, local_heads, 2):
            for r in range(shares):
                left = in_ref[(h * shares + r) * n_tp + t]
                right = in_ref[((h + 1) * shares + r) * n_tp + t]
                for part in range(2):
                    cols = slice(part * HEAD_DIM, (part + 1) * HEAD_DIM)
                    out_ref[
                        pl.ds((2 * r + part) * half, half),
                        pl.ds((t * local_heads + h) * HEAD_DIM, 2 * HEAD_DIM),
                    ] = jnp.concatenate((left[:, cols], right[:, cols]), axis=1)


def assemble(heads, shares, n_tp, local_heads):
    shape = (2 * shares * heads.shape[1], n_tp * local_heads * HEAD_DIM)
    return pl.pallas_call(
        functools.partial(
            assemble_kernel, shares=shares, n_tp=n_tp, local_heads=local_heads
        ),
        out_shape=jax.ShapeDtypeStruct(shape, jnp.bfloat16),
        in_specs=[pl.BlockSpec(memory_space=pltpu.VMEM)],
        out_specs=pl.BlockSpec(memory_space=pltpu.VMEM),
        name="assemble",
    )(heads)


def flash_kernel(*refs, begun, span, shares, sub, rows_dev, n_tp):
    if begun:
        q_ref, kv_ref, side_q_ref, side_k_ref, state_ref, o_ref, k_aug, v_aug = refs
    else:
        q_ref, kv_ref, side_q_ref, side_k_ref, o_ref, k_aug, v_aug = refs
    lo, hi = span
    count = hi - lo
    tile = pl.program_id(0)
    rank = lax.rem(lax.axis_index("sp"), shares)

    @pl.when(tile == 0)
    def _():
        lane = lax.broadcasted_iota(jnp.int32, (count, 2 * HEAD_DIM), 1)

        def one(src, carry):
            kv = kv_ref[src, :count].astype(jnp.float32)
            side = side_k_ref[src, lo:hi].astype(jnp.float32)
            k_aug[src] = jnp.where(lane < HEAD_DIM, kv, side).astype(jnp.bfloat16)
            ones = (lane == 0).astype(jnp.float32)
            v_aug[src] = jnp.where(lane < HEAD_DIM, ones, kv).astype(jnp.bfloat16)
            return carry

        lax.fori_loop(0, kv_ref.shape[0], one, 0)

    packed = q_ref[0]
    queries = jnp.concatenate((packed[:, :HEAD_DIM], packed[:, HEAD_DIM:]), axis=0)
    queries = queries * jnp.bfloat16(HEAD_DIM**-0.5)
    queries = jnp.concatenate((queries, side_q_ref[:, HEAD_DIM:]), axis=1)
    rows = queries.shape[0]
    out_lane = lax.broadcasted_iota(jnp.int32, (rows, 2 * HEAD_DIM), 1)

    def step(src, state, masked):
        peak, acc = state
        scores = lax.dot_general(
            queries, k_aug[src], (((1,), (1,)), ((), ())), preferred_element_type=jnp.float32
        )
        if masked:
            row = lax.broadcasted_iota(jnp.int32, (rows, 1), 0)
            pos = row // sub * rows_dev + rank * sub + row % sub
            key = lo + lax.broadcasted_iota(jnp.int32, (1, count), 1)
            scores = jnp.where(key <= pos, scores, MASKED)
        new_peak = jnp.maximum(peak, jnp.max(scores, axis=1, keepdims=True))
        probs = jnp.exp(scores - new_peak).astype(jnp.bfloat16)
        acc = acc * jnp.exp(peak - new_peak) + jnp.dot(
            probs, v_aug[src], preferred_element_type=jnp.float32
        )
        return new_peak, acc

    if begun:
        before = state_ref[...]
        kept = jnp.max(jnp.where(out_lane == 1, before, -jnp.inf), axis=1, keepdims=True)
        state = (kept, jnp.where(out_lane == 1, 0.0, before))
    else:
        state = (
            jnp.full((rows, 1), MASKED, jnp.float32),
            jnp.zeros((rows, 2 * HEAD_DIM), jnp.float32),
        )
    state = lax.fori_loop(0, tile, lambda i, state: step(i, state, False), state)
    peak, acc = step(tile, state, True)
    if not begun:
        o_ref[...] = jnp.where(out_lane == 1, peak, acc)
        return
    out = acc[:, HEAD_DIM:] / acc[:, :1]
    half = sub // 2
    for t in range(n_tp):
        top, low = (out[t * sub + step : t * sub + step + half] for step in (0, half))
        o_ref[t] = jnp.concatenate((top, low), axis=1).astype(o_ref.dtype)


def flash(got, kv, side_q, side_k, state, span, first, sub, rows_dev, n_tp, shares):
    n_sp, count = kv.shape[0], span[1] - span[0]
    chunk = n_tp * sub
    lanes = 2 * HEAD_DIM
    whole = pl.BlockSpec(memory_space=pltpu.VMEM)
    begun = state is not None
    wide = pl.BlockSpec((chunk, lanes), lambda i: (i, 0))
    if begun:
        out_shape = jax.ShapeDtypeStruct((n_sp * n_tp, sub // 2, lanes), jnp.bfloat16)
        out_spec = pl.BlockSpec((n_tp, sub // 2, lanes), lambda i: (i, 0, 0))
    else:
        out_shape = jax.ShapeDtypeStruct((n_sp * chunk, lanes), jnp.float32)
        out_spec = wide
    first_q = first // (chunk // 2)
    body = functools.partial(
        flash_kernel,
        begun=begun,
        span=span,
        shares=shares,
        sub=sub,
        rows_dev=rows_dev,
        n_tp=n_tp,
    )
    q_spec = pl.BlockSpec((1, chunk // 2, lanes), lambda i: (i, first_q, 0))
    pairs = n_sp * (n_sp + 1) // 2 * chunk * count
    return pl.pallas_call(
        body,
        grid=(n_sp,),
        out_shape=out_shape,
        in_specs=[q_spec, whole, wide, whole] + [wide] * begun,
        out_specs=out_spec,
        scratch_shapes=[pltpu.VMEM((n_sp, count, lanes), jnp.bfloat16)] * 2,
        compiler_params=pltpu.CompilerParams(vmem_limit_bytes=50 * 2**20),
        cost_estimate=pl.CostEstimate(
            flops=8 * lanes * pairs, bytes_accessed=2**22, transcendentals=pairs
        ),
        name="flash",
    )(got, kv, side_q, side_k, *([state] if begun else []))


def expert_kernel(
    out_ref, wg_hbm, wu_hbm, wd_hbm, weigh_ref, stream_ref, gain_ref, o_ref,
    arrived, made, returned, wg, wu, wd, gate_acc, up_acc, hidden, comb,
    w_sem, own_sem, send_sem, recv_sem, *, n_tp, chunks,
):
    n, cap, width = out_ref.shape
    part = width // chunks
    sp, tp = lax.axis_index("sp"), lax.axis_index("tp")
    me = sp * n_tp + tp

    def peer(o):
        d = lax.rem(me + o, n)
        return d, (d // n_tp, lax.rem(d, n_tp))

    loads = [
        pltpu.make_async_copy(src, dst, w_sem.at[i])
        for i, (src, dst) in enumerate(((wg_hbm, wg), (wu_hbm, wu), (wd_hbm, wd)))
    ]
    for load in loads:
        load.start()

    barrier = pltpu.get_barrier_semaphore()

    def greet(o, carry):
        pl.semaphore_signal(barrier, inc=1, device_id=peer(o)[1], device_id_type=MESH)
        return carry

    lax.fori_loop(1, n, greet, 0)
    pl.semaphore_wait(barrier, n - 1)

    def cols(c):
        return pl.ds(c * part, part)

    def send_all(src, dst, c, slot):
        def one(o, carry):
            d, where = peer(o)
            pltpu.make_async_remote_copy(
                src_ref=src.at[d, :, cols(c)],
                dst_ref=dst.at[me, :, cols(c)],
                send_sem=send_sem.at[slot],
                recv_sem=recv_sem.at[slot],
                device_id=where,
                device_id_type=MESH,
            ).start()
            return carry

        pltpu.make_async_copy(src.at[me, :, cols(c)], dst.at[me, :, cols(c)], own_sem.at[slot]).start()
        lax.fori_loop(1, n, one, 0)

    def all_copies(src, dst, c, slot):
        return pltpu.make_async_remote_copy(
            src_ref=src.at[pl.ds(0, n - 1), :, cols(c)],
            dst_ref=dst.at[pl.ds(0, n - 1), :, cols(c)],
            send_sem=send_sem.at[slot],
            recv_sem=recv_sem.at[slot],
            device_id=peer(1)[1],
            device_id_type=MESH,
        )

    def wait_all(src, dst, c, slot):
        pltpu.make_async_copy(src.at[me, :, cols(c)], dst.at[me, :, cols(c)], own_sem.at[slot]).wait()
        all_copies(src, dst, c, slot).wait_recv()

    for c in range(chunks):
        send_all(out_ref, arrived, c, c)
    for load in loads[:2]:
        load.wait()
    group = n // GROUPS
    rows = group * cap

    for c in range(chunks):
        wait_all(out_ref, arrived, c, c)

        def gate_up(g, carry, c=c):
            x = arrived[pl.ds(g * group, group), :, cols(c)].reshape(rows, part)
            at = pl.ds(pl.multiple_of(g * rows, rows), rows)
            gate = jnp.dot(x, wg[cols(c), :], preferred_element_type=jnp.float32)
            up = jnp.dot(x, wu[cols(c), :], preferred_element_type=jnp.float32)
            if c > 0:
                gate, up = gate + gate_acc[at, :], up + up_acc[at, :]
            if c < chunks - 1:
                gate_acc[at, :] = gate
                up_acc[at, :] = up
            else:
                hidden[at, :] = (jax.nn.silu(gate) * up).astype(jnp.bfloat16)
            return carry

        lax.fori_loop(0, GROUPS, gate_up, 0)
    loads[2].wait()
    for c in range(chunks):

        def down(g, carry, c=c):
            at = pl.ds(pl.multiple_of(g * rows, rows), rows)
            y = jnp.dot(hidden[at, :], wd[:, cols(c)], preferred_element_type=jnp.float32)
            made[pl.ds(g * group, group), :, cols(c)] = y.astype(jnp.bfloat16).reshape(group, cap, part)
            return carry

        lax.fori_loop(0, GROUPS, down, 0)
        send_all(made, returned, c, chunks + c)
    total = jnp.zeros((o_ref.shape[0], 1), jnp.float32)
    for c in range(chunks):
        wait_all(made, returned, c, chunks + c)
        back = returned[:, :, cols(c)].reshape(n * cap, part)
        mixed = sum(
            jnp.dot(weigh_ref[i], back, preferred_element_type=jnp.float32)
            for i in range(weigh_ref.shape[0])
        )
        comb[:, cols(c)] = mixed
        total = total + jnp.sum(mixed * mixed, axis=1, keepdims=True)
    scale = lax.rsqrt(total / width + NORM_EPS)
    for c in range(chunks):
        o_ref[:, cols(c)] = (
            stream_ref[:, cols(c)].astype(jnp.float32) + comb[:, cols(c)] * scale * gain_ref[:, cols(c)]
        ).astype(jnp.bfloat16)
    for c in range(chunks):
        all_copies(out_ref, arrived, c, c).wait_send()
        all_copies(made, returned, c, chunks + c).wait_send()


def experts(outgoing, w_gate, w_up, w_down, weigh, stream, gain, n_tp):
    n, cap, width = outgoing.shape
    hidden = w_gate.shape[1]
    slots = n * cap
    chunks = CHUNKS
    vmem = pl.BlockSpec(memory_space=pltpu.VMEM)
    hbm = pl.BlockSpec(memory_space=pl.ANY)
    bf16, f32 = jnp.bfloat16, jnp.float32
    return pl.pallas_call(
        functools.partial(expert_kernel, n_tp=n_tp, chunks=chunks),
        out_shape=jax.ShapeDtypeStruct(stream.shape, bf16),
        in_specs=[vmem, hbm, hbm, hbm, vmem, vmem, vmem],
        out_specs=vmem,
        scratch_shapes=[
            pltpu.VMEM((n, cap, width), bf16),
            pltpu.VMEM((n, cap, width), bf16),
            pltpu.VMEM((n, cap, width), bf16),
            pltpu.VMEM(w_gate.shape, bf16),
            pltpu.VMEM(w_up.shape, bf16),
            pltpu.VMEM(w_down.shape, bf16),
            pltpu.VMEM((slots, hidden), f32),
            pltpu.VMEM((slots, hidden), f32),
            pltpu.VMEM((slots, hidden), bf16),
            pltpu.VMEM(stream.shape, f32),
            pltpu.SemaphoreType.DMA((3,)),
            pltpu.SemaphoreType.DMA((2 * chunks,)),
            pltpu.SemaphoreType.DMA((2 * chunks,)),
            pltpu.SemaphoreType.DMA((2 * chunks,)),
        ],
        compiler_params=pltpu.CompilerParams(
            collective_id=1, has_side_effects=True, vmem_limit_bytes=60 * 2**20
        ),
        name="experts",
    )(outgoing, w_gate, w_up, w_down, weigh, stream, gain)


def local(
    queries,
    key_rows,
    value_rows,
    cum_gate,
    residual,
    out_weight,
    gain_mix,
    gain_pre,
    gain_post,
    route_ids,
    route_weight,
    w_gate,
    w_up,
    w_down,
):
    tok_dev, feature_width = queries.shape
    local_heads = feature_width // HEAD_DIM
    n_sp, n_tp = lax.axis_size("sp"), lax.axis_size("tp")
    shares = n_sp // local_heads
    rows_dev = residual.shape[0]
    sub = rows_dev // shares
    chunk = n_tp * sub
    half = chunk // 2
    first = tok_dev * 5 // 8 // half * half
    one, two = pack(queries, key_rows, value_rows, first, shares, n_tp)
    got = lax.all_to_all(one, "sp", split_axis=0, concat_axis=0, tiled=True)
    got, two = lax.optimization_barrier((got, two))
    got_two = lax.all_to_all(two, "sp", split_axis=0, concat_axis=0, tiled=True)

    me = lax.axis_index("sp")
    gate = lax.dynamic_index_in_dim(cum_gate, me // shares, 0, keepdims=False)
    gate_q = gate.reshape(n_sp * n_tp, shares, sub)
    gate_q = lax.dynamic_index_in_dim(gate_q, me % shares, 1, keepdims=False).reshape(-1)
    ones_q = jnp.ones((n_sp * chunk,), jnp.bfloat16)
    ones_k = jnp.ones((n_sp * tok_dev,), jnp.bfloat16)
    lanes = jnp.arange(2 * HEAD_DIM)
    place_side = (lanes == HEAD_DIM + jnp.arange(6)[:, None]).astype(jnp.bfloat16)

    def side_lanes(parts):
        return lax.dot_general(
            jnp.stack(parts), place_side, (((0,), (0,)), ((), ())), preferred_element_type=jnp.float32
        ).astype(jnp.bfloat16)

    side_q = side_lanes(bf16_parts(gate_q) + [ones_q] * 3)
    side_k = side_lanes([ones_k] * 3 + bf16_parts(-gate))
    side_k = side_k.reshape(n_sp, tok_dev, 2 * HEAD_DIM)
    fixed = (first, sub, rows_dev, n_tp, shares)
    state = flash(got, got, side_q, side_k, None, (0, first), *fixed)
    out = flash(got, got_two, side_q, side_k, state, (first, tok_dev), *fixed)
    heads = lax.all_to_all(out, ("sp", "tp"), split_axis=0, concat_axis=0, tiled=True)
    head_rows = assemble(heads, shares, n_tp, local_heads)
    projected = jnp.dot(head_rows, out_weight, preferred_element_type=jnp.float32)
    stream = (residual.astype(jnp.float32) + rms_scale(projected, gain_mix)).astype(jnp.bfloat16)
    stream_wide = lax.optimization_barrier(stream).astype(jnp.float32)
    normed = rms_scale(stream_wide, gain_pre).astype(jnp.bfloat16)
    top_count = route_ids.shape[1]
    experts_all = n_sp * n_tp
    capacity = max(2, (4 * rows_dev * top_count + 3 * experts_all - 1) // (3 * experts_all))
    capacity = (capacity + 7) // 8 * 8
    flat_ids = route_ids.reshape(-1)
    item = lax.iota(jnp.int32, rows_dev * top_count)
    earlier = (item[None, :] < item[:, None]) & (flat_ids[None, :] == flat_ids[:, None])
    slot_index = flat_ids * capacity + jnp.sum(earlier.astype(jnp.int32), axis=1)
    slot_index = slot_index.reshape(rows_dev, top_count)
    slots_all = experts_all * capacity
    slot = lax.iota(jnp.int32, slots_all)
    place = sum((slot_index[:, k, None] == slot).astype(jnp.bfloat16) for k in range(top_count))
    outgoing = lax.dot_general(
        place, normed, (((0,), (0,)), ((), ())), preferred_element_type=jnp.float32
    ).astype(jnp.bfloat16)
    outgoing = outgoing.reshape(experts_all, capacity, -1)
    weigh = sum(
        jnp.where(slot_index[:, k, None] == slot, route_weight[:, k, None], 0.0)
        for k in range(top_count)
    )
    weigh = jnp.stack(bf16_parts(weigh))
    return experts(
        outgoing, w_gate[0], w_up[0], w_down[0], weigh, stream, gain_post[None, :], n_tp
    )


def solution(mesh):
    return jax.shard_map(
        local,
        mesh=mesh,
        in_specs=(
            P("sp", "tp"),
            P("sp", "tp"),
            P("sp", "tp"),
            P("tp", None),
            P(("sp", "tp"), None),
            P(),
            P(),
            P(),
            P(),
            P(("sp", "tp"), None),
            P(("sp", "tp"), None),
            P(("sp", "tp"), None, None),
            P(("sp", "tp"), None, None),
            P(("sp", "tp"), None, None),
        ),
        out_specs=P(("sp", "tp"), None),
        check_vma=False,
    )
```

```python
import functools
import math

import jax
import jax.numpy as jnp
from jax import lax
from jax.experimental import pallas as pl
from jax.experimental.pallas import tpu as pltpu
from jax.sharding import PartitionSpec as P

HEAD_DIM = 64
NORM_EPS = 1e-06
MASKED = -1e30
MESH = pl.DeviceIdType.MESH
CHUNKS = 4
GROUPS = 4
KEY_PARTS = 1


def rms_scale(rows, gain):
    mean_sq = jnp.mean(rows * rows, axis=-1, keepdims=True)
    return rows * lax.rsqrt(mean_sq + NORM_EPS) * gain


def bf16_parts(values):
    parts = []
    for _ in range(3):
        part = lax.reduce_precision(values, 8, 7)
        parts.append(part.astype(jnp.bfloat16))
        values = values - part
    return parts


def pack_kernel(q_ref, k_ref, v_ref, kv_out, q_out, *, shares, n_tp):
    tok_dev, width = q_ref.shape
    rows_dev = tok_dev // n_tp
    sub = rows_dev // shares
    for h in range(width // HEAD_DIM):
        cols = pl.ds(h * HEAD_DIM, HEAD_DIM)
        kv_out[h] = jnp.concatenate((k_ref[:, cols], v_ref[:, cols]), axis=1)
        for r in range(shares):
            for t in range(n_tp // 2):
                low, high = (
                    q_ref[pl.ds((t + step) * rows_dev + r * sub, sub), cols]
                    for step in (0, n_tp // 2)
                )
                q_out[h * shares + r, pl.ds(t * sub, sub)] = jnp.concatenate((low, high), axis=1)


def pack(queries, key_rows, value_rows, shares, n_tp):
    tok_dev, width = queries.shape
    heads = width // HEAD_DIM
    shapes = [
        (heads, tok_dev, 2 * HEAD_DIM),
        (heads * shares, tok_dev // shares // 2, 2 * HEAD_DIM),
    ]
    return pl.pallas_call(
        functools.partial(pack_kernel, shares=shares, n_tp=n_tp),
        out_shape=[jax.ShapeDtypeStruct(shape, jnp.bfloat16) for shape in shapes],
        in_specs=[pl.BlockSpec(memory_space=pltpu.VMEM)] * 3,
        out_specs=[pl.BlockSpec(memory_space=pltpu.VMEM)] * 2,
        compiler_params=pltpu.CompilerParams(vmem_limit_bytes=32 * 2**20),
        name="pack",
    )(queries, key_rows, value_rows)


def attend_kernel(
    kv_ref, q_ref, side_q_ref, side_k_ref, o_ref,
    kv_all, q_all, k_aug, v_aug, q_aug, peak_ref, acc_ref, out_ref, heads_ref,
    own_sem, q_sem, kv_sem, head_sem, send_sem, *, n_tp, local_heads,
):
    groups = local_heads
    n_sp = q_ref.shape[0]
    shares = n_sp // groups
    tok_dev = kv_ref.shape[1]
    chunk = 2 * q_ref.shape[1]
    sub = chunk // n_tp
    rows_dev = sub * shares
    lanes = 2 * HEAD_DIM
    n = n_sp * n_tp
    sp, tp = lax.axis_index("sp"), lax.axis_index("tp")
    me = sp * n_tp + tp
    group, rank = sp // shares, lax.rem(sp, shares)

    def plane(s):
        down = jnp.where(s <= group, group - s, s)
        up = jnp.where(s <= groups - 1 - group, group + s, groups - 1 - s)
        return jnp.where(2 * group < groups, down, up)

    def block_at(i):
        return plane(i // shares) * shares + lax.rem(rank + lax.rem(i, shares), shares)

    barrier = pltpu.get_barrier_semaphore()

    def greet(o, carry):
        d = lax.rem(me + o, n)
        where = (d // n_tp, lax.rem(d, n_tp))
        pl.semaphore_signal(barrier, inc=1, device_id=where, device_id_type=MESH)
        return carry

    lax.fori_loop(1, n, greet, 0)
    own_kv = pltpu.make_async_copy(kv_ref.at[group], kv_all.at[sp], own_sem.at[0])
    own_q = pltpu.make_async_copy(q_ref.at[sp], q_all.at[sp], own_sem.at[1])
    own_kv.start()
    own_q.start()
    pl.semaphore_wait(barrier, n - 1)

    def kv_copy(src, block, dest, slot):
        return pltpu.make_async_remote_copy(
            src_ref=src, dst_ref=kv_all.at[block],
            send_sem=send_sem.at[slot], recv_sem=kv_sem.at[block],
            device_id=(dest, tp), device_id_type=MESH,
        )

    def q_copy(src, block, dest):
        return pltpu.make_async_remote_copy(
            src_ref=src, dst_ref=q_all.at[block],
            send_sem=send_sem.at[0], recv_sem=q_sem.at[block],
            device_id=(dest, tp), device_id_type=MESH,
        )

    for s in range(groups):
        for k in range(shares):
            dest = block_at(s * shares + k)
            if s or k:
                q_copy(q_ref.at[dest], sp, dest).start()
            if s == 0 and k:
                kv_copy(kv_ref.at[group], sp, dest, 1).start()
            if s and k == 0:
                kv_copy(kv_ref.at[plane(s)], sp, dest, 2).start()

    row = lax.broadcasted_iota(jnp.int32, (chunk, 1), 0)
    pos = row // sub * rows_dev + rank * sub + lax.rem(row, sub)

    def build(block):
        lane = lax.broadcasted_iota(jnp.int32, (tok_dev, lanes), 1)
        kv = kv_all[block].astype(jnp.float32)
        side = side_k_ref[block].astype(jnp.float32)
        k_aug[block] = jnp.where(lane < HEAD_DIM, kv, side).astype(jnp.bfloat16)
        ones = (lane == 0).astype(jnp.float32)
        v_aug[block] = jnp.where(lane < HEAD_DIM, ones, kv).astype(jnp.bfloat16)
        packed = q_all[block]
        queries = jnp.concatenate((packed[:, :HEAD_DIM], packed[:, HEAD_DIM:]), axis=0)
        queries = queries * jnp.bfloat16(HEAD_DIM**-0.5)
        side = side_q_ref[pl.ds(pl.multiple_of(block * chunk, chunk), chunk), HEAD_DIM:]
        q_aug[block] = jnp.concatenate((queries, side), axis=1)
        peak_ref[block] = jnp.full((chunk, lanes), MASKED, jnp.float32)
        acc_ref[block] = jnp.zeros((chunk, lanes), jnp.float32)

    def step(i, j, masked):
        for part in range(KEY_PARTS):
            count = tok_dev // KEY_PARTS
            keys = pl.ds(part * count, count)
            scores = lax.dot_general(
                q_aug[i], k_aug[j, keys], (((1,), (1,)), ((), ())),
                preferred_element_type=jnp.float32,
            )
            if masked:
                key = part * count + lax.broadcasted_iota(jnp.int32, (1, count), 1)
                scores = jnp.where(key <= pos, scores, MASKED)
            before = peak_ref[i]
            peak = jnp.maximum(before, jnp.max(scores, axis=1, keepdims=True))
            probs = jnp.exp(scores - jnp.concatenate([peak] * (count // lanes), axis=1)).astype(jnp.bfloat16)
            peak_ref[i] = peak
            acc_ref[i] = acc_ref[i] * jnp.exp(before - peak) + jnp.dot(
                probs, v_aug[j, keys], preferred_element_type=jnp.float32
            )

    def head_copy(block, t):
        slot = block * n_tp + t
        return pltpu.make_async_remote_copy(
            src_ref=out_ref.at[slot], dst_ref=heads_ref.at[me],
            send_sem=send_sem.at[4], recv_sem=head_sem,
            device_id=(block, t), device_id_type=MESH,
        )

    own_head = pltpu.make_async_copy(out_ref.at[me], heads_ref.at[me], own_sem.at[2])

    def finish(block):
        acc = acc_ref[block]
        out = acc[:, HEAD_DIM:] / acc[:, :1]
        half = sub // 2
        for t in range(n_tp):
            top, low = (out[t * sub + at : t * sub + at + half] for at in (0, half))
            out_ref[block * n_tp + t] = jnp.concatenate((top, low), axis=1).astype(jnp.bfloat16)
        for t in range(n_tp):
            mine = (block == sp) & (tp == t)

            @pl.when(mine)
            def _():
                own_head.start()

            @pl.when(jnp.logical_not(mine))
            def _(t=t):
                head_copy(block, t).start()

    def relay(i):
        block = block_at(i)
        kv_copy(kv_all.at[block], block, block, 3).wait_recv()
        for k in range(1, shares):
            dest = group * shares + lax.rem(rank + k, shares)
            kv_copy(kv_all.at[block], block, dest, 3).start()

    def one_block(i, carry):
        block = block_at(i)
        s, k = i // shares, lax.rem(i, shares)
        turn = k == shares - 1

        @pl.when(i == 0)
        def _():
            own_kv.wait()
            own_q.wait()

        @pl.when(i > 0)
        def _():
            q_copy(q_all.at[block], block, block).wait_recv()

        @pl.when(k > 0)
        def _():
            kv_copy(kv_all.at[block], block, block, 3).wait_recv()

        @pl.when(turn & (s > 0) & (s < groups - 1))
        def _():
            relay(i + 1)

        build(block)

        def pair(m, carry):
            other = block_at(m)
            step(jnp.maximum(block, other), jnp.minimum(block, other), False)

            @pl.when(i == n_sp - 1)
            def _():
                finish(other)

            return carry

        lax.fori_loop(0, i, pair, 0)
        step(block, block, True)

        @pl.when(turn & (s == 0) & (groups > 1))
        def _():
            relay(i + 1)

        return carry

    lax.fori_loop(0, n_sp, one_block, 0)
    finish(block_at(n_sp - 1))
    own_head.wait()

    def sent(buf, count, slot):
        if count:
            pltpu.make_async_remote_copy(
                src_ref=buf.at[pl.ds(0, count)], dst_ref=buf.at[pl.ds(0, count)],
                send_sem=send_sem.at[slot], recv_sem=head_sem,
                device_id=(sp, tp), device_id_type=MESH,
            ).wait_send()

    pltpu.make_async_remote_copy(
        src_ref=heads_ref.at[pl.ds(0, n - 1)], dst_ref=heads_ref.at[pl.ds(0, n - 1)],
        send_sem=send_sem.at[4], recv_sem=head_sem,
        device_id=(sp, tp), device_id_type=MESH,
    ).wait_recv()
    half = sub // 2
    for t in range(n_tp):
        for h in range(0, local_heads, 2):
            for r in range(shares):
                left = heads_ref[(h * shares + r) * n_tp + t]
                right = heads_ref[((h + 1) * shares + r) * n_tp + t]
                for part in range(2):
                    cols = slice(part * HEAD_DIM, (part + 1) * HEAD_DIM)
                    o_ref[
                        pl.ds((2 * r + part) * half, half),
                        pl.ds((t * local_heads + h) * HEAD_DIM, 2 * HEAD_DIM),
                    ] = jnp.concatenate((left[:, cols], right[:, cols]), axis=1)
    sent(q_ref, n_sp - 1, 0)
    sent(kv_all, shares - 1, 1)
    sent(kv_all, groups - 1, 2)
    sent(kv_all, (groups - 1) * (shares - 1), 3)
    sent(out_ref, n - 1, 4)


def attend(kv, q, side_q, side_k, n_tp):
    local_heads, tok_dev, lanes = kv.shape
    n_sp, half_chunk = q.shape[:2]
    chunk = 2 * half_chunk
    n = n_sp * n_tp
    sub = chunk // n_tp
    bf16, f32 = jnp.bfloat16, jnp.float32
    vmem = pl.BlockSpec(memory_space=pltpu.VMEM)
    rows_dev = tok_dev // n_tp
    return pl.pallas_call(
        functools.partial(attend_kernel, n_tp=n_tp, local_heads=local_heads),
        out_shape=jax.ShapeDtypeStruct((rows_dev, n_tp * local_heads * HEAD_DIM), bf16),
        in_specs=[vmem] * 4,
        out_specs=vmem,
        scratch_shapes=[
            pltpu.VMEM((n_sp, tok_dev, lanes), bf16),
            pltpu.VMEM((n_sp, half_chunk, lanes), bf16),
            pltpu.VMEM((n_sp, tok_dev, lanes), bf16),
            pltpu.VMEM((n_sp, tok_dev, lanes), bf16),
            pltpu.VMEM((n_sp, chunk, lanes), bf16),
            pltpu.VMEM((n_sp, chunk, lanes), f32),
            pltpu.VMEM((n_sp, chunk, lanes), f32),
            pltpu.VMEM((n, sub // 2, lanes), bf16),
            pltpu.VMEM((n, sub // 2, lanes), bf16),
            pltpu.SemaphoreType.DMA((3,)),
            pltpu.SemaphoreType.DMA((n_sp,)),
            pltpu.SemaphoreType.DMA((n_sp,)),
            pltpu.SemaphoreType.DMA,
            pltpu.SemaphoreType.DMA((5,)),
        ],
        compiler_params=pltpu.CompilerParams(
            collective_id=0, has_side_effects=True, vmem_limit_bytes=56 * 2**20
        ),
        name="attend",
    )(kv, q, side_q, side_k)


def expert_kernel(
    out_ref, wg_hbm, wu_hbm, wd_hbm, weigh_ref, stream_ref, gain_ref, o_ref,
    arrived, made, returned, wg, wu, wd, gate_acc, up_acc, hidden, comb,
    w_sem, own_sem, send_sem, recv_sem, *, n_tp, chunks,
):
    n, cap, width = out_ref.shape
    part = width // chunks
    sp, tp = lax.axis_index("sp"), lax.axis_index("tp")
    me = sp * n_tp + tp

    def peer(o):
        d = lax.rem(me + o, n)
        return d, (d // n_tp, lax.rem(d, n_tp))

    loads = [
        pltpu.make_async_copy(src, dst, w_sem.at[i])
        for i, (src, dst) in enumerate(((wg_hbm, wg), (wu_hbm, wu), (wd_hbm, wd)))
    ]
    for load in loads:
        load.start()

    barrier = pltpu.get_barrier_semaphore()

    def greet(o, carry):
        pl.semaphore_signal(barrier, inc=1, device_id=peer(o)[1], device_id_type=MESH)
        return carry

    lax.fori_loop(1, n, greet, 0)
    pl.semaphore_wait(barrier, n - 1)

    def cols(c):
        return pl.ds(c * part, part)

    def send_all(src, dst, c, slot):
        def one(o, carry):
            d, where = peer(o)
            pltpu.make_async_remote_copy(
                src_ref=src.at[d, :, cols(c)],
                dst_ref=dst.at[me, :, cols(c)],
                send_sem=send_sem.at[slot],
                recv_sem=recv_sem.at[slot],
                device_id=where,
                device_id_type=MESH,
            ).start()
            return carry

        pltpu.make_async_copy(src.at[me, :, cols(c)], dst.at[me, :, cols(c)], own_sem.at[slot]).start()
        lax.fori_loop(1, n, one, 0)

    def all_copies(src, dst, c, slot):
        return pltpu.make_async_remote_copy(
            src_ref=src.at[pl.ds(0, n - 1), :, cols(c)],
            dst_ref=dst.at[pl.ds(0, n - 1), :, cols(c)],
            send_sem=send_sem.at[slot],
            recv_sem=recv_sem.at[slot],
            device_id=peer(1)[1],
            device_id_type=MESH,
        )

    def wait_all(src, dst, c, slot):
        pltpu.make_async_copy(src.at[me, :, cols(c)], dst.at[me, :, cols(c)], own_sem.at[slot]).wait()
        all_copies(src, dst, c, slot).wait_recv()

    for c in range(chunks):
        send_all(out_ref, arrived, c, c)
    for load in loads[:2]:
        load.wait()
    group = n // GROUPS
    rows = group * cap

    for c in range(chunks):
        wait_all(out_ref, arrived, c, c)

        def gate_up(g, carry, c=c):
            x = arrived[pl.ds(g * group, group), :, cols(c)].reshape(rows, part)
            at = pl.ds(pl.multiple_of(g * rows, rows), rows)
            gate = jnp.dot(x, wg[cols(c), :], preferred_element_type=jnp.float32)
            up = jnp.dot(x, wu[cols(c), :], preferred_element_type=jnp.float32)
            if c > 0:
                gate, up = gate + gate_acc[at, :], up + up_acc[at, :]
            if c < chunks - 1:
                gate_acc[at, :] = gate
                up_acc[at, :] = up
            else:
                hidden[at, :] = (jax.nn.silu(gate) * up).astype(jnp.bfloat16)
            return carry

        lax.fori_loop(0, GROUPS, gate_up, 0)
    loads[2].wait()
    for c in range(chunks):

        def down(g, carry, c=c):
            at = pl.ds(pl.multiple_of(g * rows, rows), rows)
            y = jnp.dot(hidden[at, :], wd[:, cols(c)], preferred_element_type=jnp.float32)
            made[pl.ds(g * group, group), :, cols(c)] = y.astype(jnp.bfloat16).reshape(group, cap, part)
            return carry

        lax.fori_loop(0, GROUPS, down, 0)
        send_all(made, returned, c, chunks + c)
    total = jnp.zeros((o_ref.shape[0], 1), jnp.float32)
    for c in range(chunks):
        wait_all(made, returned, c, chunks + c)
        back = returned[:, :, cols(c)].reshape(n * cap, part)
        mixed = sum(
            jnp.dot(weigh_ref[i], back, preferred_element_type=jnp.float32)
            for i in range(weigh_ref.shape[0])
        )
        comb[:, cols(c)] = mixed
        total = total + jnp.sum(mixed * mixed, axis=1, keepdims=True)
    scale = lax.rsqrt(total / width + NORM_EPS)
    for c in range(chunks):
        o_ref[:, cols(c)] = (
            stream_ref[:, cols(c)].astype(jnp.float32) + comb[:, cols(c)] * scale * gain_ref[:, cols(c)]
        ).astype(jnp.bfloat16)
    for c in range(chunks):
        all_copies(out_ref, arrived, c, c).wait_send()
        all_copies(made, returned, c, chunks + c).wait_send()


def experts(outgoing, w_gate, w_up, w_down, weigh, stream, gain, n_tp):
    n, cap, width = outgoing.shape
    hidden = w_gate.shape[1]
    slots = n * cap
    chunks = CHUNKS
    vmem = pl.BlockSpec(memory_space=pltpu.VMEM)
    hbm = pl.BlockSpec(memory_space=pl.ANY)
    bf16, f32 = jnp.bfloat16, jnp.float32
    return pl.pallas_call(
        functools.partial(expert_kernel, n_tp=n_tp, chunks=chunks),
        out_shape=jax.ShapeDtypeStruct(stream.shape, bf16),
        in_specs=[vmem, hbm, hbm, hbm, vmem, vmem, vmem],
        out_specs=vmem,
        scratch_shapes=[
            pltpu.VMEM((n, cap, width), bf16),
            pltpu.VMEM((n, cap, width), bf16),
            pltpu.VMEM((n, cap, width), bf16),
            pltpu.VMEM(w_gate.shape, bf16),
            pltpu.VMEM(w_up.shape, bf16),
            pltpu.VMEM(w_down.shape, bf16),
            pltpu.VMEM((slots, hidden), f32),
            pltpu.VMEM((slots, hidden), f32),
            pltpu.VMEM((slots, hidden), bf16),
            pltpu.VMEM(stream.shape, f32),
            pltpu.SemaphoreType.DMA((3,)),
            pltpu.SemaphoreType.DMA((2 * chunks,)),
            pltpu.SemaphoreType.DMA((2 * chunks,)),
            pltpu.SemaphoreType.DMA((2 * chunks,)),
        ],
        compiler_params=pltpu.CompilerParams(
            collective_id=1, has_side_effects=True, vmem_limit_bytes=60 * 2**20
        ),
        name="experts",
    )(outgoing, w_gate, w_up, w_down, weigh, stream, gain)


def local(
    queries,
    key_rows,
    value_rows,
    cum_gate,
    residual,
    out_weight,
    gain_mix,
    gain_pre,
    gain_post,
    route_ids,
    route_weight,
    w_gate,
    w_up,
    w_down,
):
    tok_dev, feature_width = queries.shape
    local_heads = feature_width // HEAD_DIM
    n_sp, n_tp = lax.axis_size("sp"), lax.axis_size("tp")
    shares = n_sp // local_heads
    rows_dev = residual.shape[0]
    sub = rows_dev // shares
    chunk = n_tp * sub
    kv, q = pack(queries, key_rows, value_rows, shares, n_tp)

    me = lax.axis_index("sp")
    gate = lax.dynamic_index_in_dim(cum_gate, me // shares, 0, keepdims=False)
    gate_q = gate.reshape(n_sp * n_tp, shares, sub)
    gate_q = lax.dynamic_index_in_dim(gate_q, me % shares, 1, keepdims=False).reshape(-1)
    ones_q = jnp.ones((n_sp * chunk,), jnp.bfloat16)
    ones_k = jnp.ones((n_sp * tok_dev,), jnp.bfloat16)
    lanes = jnp.arange(2 * HEAD_DIM)
    place_side = (lanes == HEAD_DIM + jnp.arange(6)[:, None]).astype(jnp.bfloat16)

    def side_lanes(parts):
        return lax.dot_general(
            jnp.stack(parts), place_side, (((0,), (0,)), ((), ())), preferred_element_type=jnp.float32
        ).astype(jnp.bfloat16)

    side_q = side_lanes(bf16_parts(gate_q) + [ones_q] * 3)
    side_k = side_lanes([ones_k] * 3 + bf16_parts(-gate))
    side_k = side_k.reshape(n_sp, tok_dev, 2 * HEAD_DIM)
    head_rows = attend(kv, q, side_q, side_k, n_tp)
    projected = jnp.dot(head_rows, out_weight, preferred_element_type=jnp.float32)
    stream = (residual.astype(jnp.float32) + rms_scale(projected, gain_mix)).astype(jnp.bfloat16)
    stream_wide = lax.optimization_barrier(stream).astype(jnp.float32)
    normed = rms_scale(stream_wide, gain_pre).astype(jnp.bfloat16)
    top_count = route_ids.shape[1]
    experts_all = n_sp * n_tp
    capacity = max(2, (4 * rows_dev * top_count + 3 * experts_all - 1) // (3 * experts_all))
    capacity = (capacity + 7) // 8 * 8
    flat_ids = route_ids.reshape(-1)
    item = lax.iota(jnp.int32, rows_dev * top_count)
    earlier = (item[None, :] < item[:, None]) & (flat_ids[None, :] == flat_ids[:, None])
    slot_index = flat_ids * capacity + jnp.sum(earlier.astype(jnp.int32), axis=1)
    slot_index = slot_index.reshape(rows_dev, top_count)
    slots_all = experts_all * capacity
    slot = lax.iota(jnp.int32, slots_all)
    place = sum((slot_index[:, k, None] == slot).astype(jnp.bfloat16) for k in range(top_count))
    outgoing = lax.dot_general(
        place, normed, (((0,), (0,)), ((), ())), preferred_element_type=jnp.float32
    ).astype(jnp.bfloat16)
    outgoing = outgoing.reshape(experts_all, capacity, -1)
    weigh = sum(
        jnp.where(slot_index[:, k, None] == slot, route_weight[:, k, None], 0.0)
        for k in range(top_count)
    )
    weigh = jnp.stack(bf16_parts(weigh))
    return experts(
        outgoing, w_gate[0], w_up[0], w_down[0], weigh, stream, gain_post[None, :], n_tp
    )


def solution(mesh):
    return jax.shard_map(
        local,
        mesh=mesh,
        in_specs=(
            P("sp", "tp"),
            P("sp", "tp"),
            P("sp", "tp"),
            P("tp", None),
            P(("sp", "tp"), None),
            P(),
            P(),
            P(),
            P(),
            P(("sp", "tp"), None),
            P(("sp", "tp"), None),
            P(("sp", "tp"), None, None),
            P(("sp", "tp"), None, None),
            P(("sp", "tp"), None, None),
        ),
        out_specs=P(("sp", "tp"), None),
        check_vma=False,
    )
```

```python
import functools
import math

import jax
import jax.numpy as jnp
from jax import lax
from jax.experimental import pallas as pl
from jax.experimental.pallas import tpu as pltpu
from jax.sharding import PartitionSpec as P

HEAD_DIM = 64
NORM_EPS = 1e-06
MASKED = -1e30
MESH = pl.DeviceIdType.MESH
CHUNKS = 4
GROUPS = 4
KEY_PARTS = 1
WEIGH_COLS = 256


def bf16_parts(values):
    parts = []
    for _ in range(3):
        part = lax.reduce_precision(values, 8, 7)
        parts.append(part.astype(jnp.bfloat16))
        values = values - part
    return parts


def pack_kernel(q_ref, k_ref, v_ref, kv_out, q_out, *, shares, n_tp):
    tok_dev, width = q_ref.shape
    rows_dev = tok_dev // n_tp
    sub = rows_dev // shares
    for h in range(width // HEAD_DIM):
        cols = pl.ds(h * HEAD_DIM, HEAD_DIM)
        kv_out[h] = jnp.concatenate((k_ref[:, cols], v_ref[:, cols]), axis=1)
        for r in range(shares):
            for t in range(n_tp // 2):
                low, high = (
                    q_ref[pl.ds((t + step) * rows_dev + r * sub, sub), cols]
                    for step in (0, n_tp // 2)
                )
                q_out[h * shares + r, pl.ds(t * sub, sub)] = jnp.concatenate((low, high), axis=1)


def pack(queries, key_rows, value_rows, shares, n_tp):
    tok_dev, width = queries.shape
    heads = width // HEAD_DIM
    shapes = [
        (heads, tok_dev, 2 * HEAD_DIM),
        (heads * shares, tok_dev // shares // 2, 2 * HEAD_DIM),
    ]
    return pl.pallas_call(
        functools.partial(pack_kernel, shares=shares, n_tp=n_tp),
        out_shape=[jax.ShapeDtypeStruct(shape, jnp.bfloat16) for shape in shapes],
        in_specs=[pl.BlockSpec(memory_space=pltpu.VMEM)] * 3,
        out_specs=[pl.BlockSpec(memory_space=pltpu.VMEM)] * 2,
        compiler_params=pltpu.CompilerParams(vmem_limit_bytes=32 * 2**20),
        name="pack",
    )(queries, key_rows, value_rows)


def attend_kernel(
    kv_ref, q_ref, side_q_ref, side_k_ref, o_ref,
    kv_all, q_all, k_aug, v_aug, q_aug, peak_ref, acc_ref, out_ref, heads_ref,
    own_sem, q_sem, kv_sem, head_sem, send_sem, *, n_tp, local_heads,
):
    groups = local_heads
    n_sp = q_ref.shape[0]
    shares = n_sp // groups
    tok_dev = kv_ref.shape[1]
    chunk = 2 * q_ref.shape[1]
    sub = chunk // n_tp
    rows_dev = sub * shares
    lanes = 2 * HEAD_DIM
    n = n_sp * n_tp
    sp, tp = lax.axis_index("sp"), lax.axis_index("tp")
    me = sp * n_tp + tp
    group, rank = sp // shares, lax.rem(sp, shares)

    def plane(s):
        down = jnp.where(s <= group, group - s, s)
        up = jnp.where(s <= groups - 1 - group, group + s, groups - 1 - s)
        return jnp.where(2 * group < groups, down, up)

    def block_at(i):
        return plane(i // shares) * shares + lax.rem(rank + lax.rem(i, shares), shares)

    barrier = pltpu.get_barrier_semaphore()

    def greet(o, carry):
        d = lax.rem(me + o, n)
        where = (d // n_tp, lax.rem(d, n_tp))
        pl.semaphore_signal(barrier, inc=1, device_id=where, device_id_type=MESH)
        return carry

    lax.fori_loop(1, n, greet, 0)
    own_kv = pltpu.make_async_copy(kv_ref.at[group], kv_all.at[sp], own_sem.at[0])
    own_q = pltpu.make_async_copy(q_ref.at[sp], q_all.at[sp], own_sem.at[1])
    own_kv.start()
    own_q.start()
    pl.semaphore_wait(barrier, n - 1)

    def kv_copy(src, block, dest, slot):
        return pltpu.make_async_remote_copy(
            src_ref=src, dst_ref=kv_all.at[block],
            send_sem=send_sem.at[slot], recv_sem=kv_sem.at[block],
            device_id=(dest, tp), device_id_type=MESH,
        )

    def q_copy(src, block, dest):
        return pltpu.make_async_remote_copy(
            src_ref=src, dst_ref=q_all.at[block],
            send_sem=send_sem.at[0], recv_sem=q_sem.at[block],
            device_id=(dest, tp), device_id_type=MESH,
        )

    for s in range(groups):
        for k in range(shares):
            dest = block_at(s * shares + k)
            if s or k:
                q_copy(q_ref.at[dest], sp, dest).start()
            if s == 0 and k:
                kv_copy(kv_ref.at[group], sp, dest, 1).start()
            if s and k == 0:
                kv_copy(kv_ref.at[plane(s)], sp, dest, 2).start()

    row = lax.broadcasted_iota(jnp.int32, (chunk, 1), 0)
    pos = row // sub * rows_dev + rank * sub + lax.rem(row, sub)

    def build(block):
        lane = lax.broadcasted_iota(jnp.int32, (tok_dev, lanes), 1)
        kv = kv_all[block].astype(jnp.float32)
        side = side_k_ref[block].astype(jnp.float32)
        k_aug[block] = jnp.where(lane < HEAD_DIM, kv, side).astype(jnp.bfloat16)
        ones = (lane == 0).astype(jnp.float32)
        v_aug[block] = jnp.where(lane < HEAD_DIM, ones, kv).astype(jnp.bfloat16)
        packed = q_all[block]
        queries = jnp.concatenate((packed[:, :HEAD_DIM], packed[:, HEAD_DIM:]), axis=0)
        queries = queries * jnp.bfloat16(HEAD_DIM**-0.5)
        side = side_q_ref[pl.ds(pl.multiple_of(block * chunk, chunk), chunk), HEAD_DIM:]
        q_aug[block] = jnp.concatenate((queries, side), axis=1)
        peak_ref[block] = jnp.full((chunk, lanes), MASKED, jnp.float32)
        acc_ref[block] = jnp.zeros((chunk, lanes), jnp.float32)

    def step(i, j, masked):
        for part in range(KEY_PARTS):
            count = tok_dev // KEY_PARTS
            keys = pl.ds(part * count, count)
            scores = lax.dot_general(
                q_aug[i], k_aug[j, keys], (((1,), (1,)), ((), ())),
                preferred_element_type=jnp.float32,
            )
            if masked:
                key = part * count + lax.broadcasted_iota(jnp.int32, (1, count), 1)
                scores = jnp.where(key <= pos, scores, MASKED)
            before = peak_ref[i]
            peak = jnp.maximum(before, jnp.max(scores, axis=1, keepdims=True))
            probs = jnp.exp(scores - jnp.concatenate([peak] * (count // lanes), axis=1)).astype(jnp.bfloat16)
            peak_ref[i] = peak
            acc_ref[i] = acc_ref[i] * jnp.exp(before - peak) + jnp.dot(
                probs, v_aug[j, keys], preferred_element_type=jnp.float32
            )

    def head_copy(block, t):
        slot = block * n_tp + t
        return pltpu.make_async_remote_copy(
            src_ref=out_ref.at[slot], dst_ref=heads_ref.at[me],
            send_sem=send_sem.at[4], recv_sem=head_sem,
            device_id=(block, t), device_id_type=MESH,
        )

    own_head = pltpu.make_async_copy(out_ref.at[me], heads_ref.at[me], own_sem.at[2])

    def finish(block):
        acc = acc_ref[block]
        out = acc[:, HEAD_DIM:] / acc[:, :1]
        half = sub // 2
        for t in range(n_tp):
            top, low = (out[t * sub + at : t * sub + at + half] for at in (0, half))
            out_ref[block * n_tp + t] = jnp.concatenate((top, low), axis=1).astype(jnp.bfloat16)
        for t in range(n_tp):
            mine = (block == sp) & (tp == t)

            @pl.when(mine)
            def _():
                own_head.start()

            @pl.when(jnp.logical_not(mine))
            def _(t=t):
                head_copy(block, t).start()

    def relay(i):
        block = block_at(i)
        kv_copy(kv_all.at[block], block, block, 3).wait_recv()
        for k in range(1, shares):
            dest = group * shares + lax.rem(rank + k, shares)
            kv_copy(kv_all.at[block], block, dest, 3).start()

    def one_block(i, carry):
        block = block_at(i)
        s, k = i // shares, lax.rem(i, shares)
        turn = k == shares - 1

        @pl.when(i == 0)
        def _():
            own_kv.wait()
            own_q.wait()

        @pl.when(i > 0)
        def _():
            q_copy(q_all.at[block], block, block).wait_recv()

        @pl.when(k > 0)
        def _():
            kv_copy(kv_all.at[block], block, block, 3).wait_recv()

        @pl.when(turn & (s > 0) & (s < groups - 1))
        def _():
            relay(i + 1)

        build(block)

        def pair(m, carry):
            other = block_at(m)
            step(jnp.maximum(block, other), jnp.minimum(block, other), False)

            @pl.when(i == n_sp - 1)
            def _():
                finish(other)

            return carry

        lax.fori_loop(0, i, pair, 0)
        step(block, block, True)

        @pl.when(turn & (s == 0) & (groups > 1))
        def _():
            relay(i + 1)

        return carry

    lax.fori_loop(0, n_sp, one_block, 0)
    finish(block_at(n_sp - 1))
    own_head.wait()

    def sent(buf, count, slot):
        if count:
            pltpu.make_async_remote_copy(
                src_ref=buf.at[pl.ds(0, count)], dst_ref=buf.at[pl.ds(0, count)],
                send_sem=send_sem.at[slot], recv_sem=head_sem,
                device_id=(sp, tp), device_id_type=MESH,
            ).wait_send()

    pltpu.make_async_remote_copy(
        src_ref=heads_ref.at[pl.ds(0, n - 1)], dst_ref=heads_ref.at[pl.ds(0, n - 1)],
        send_sem=send_sem.at[4], recv_sem=head_sem,
        device_id=(sp, tp), device_id_type=MESH,
    ).wait_recv()
    half = sub // 2
    for t in range(n_tp):
        for h in range(0, local_heads, 2):
            for r in range(shares):
                left = heads_ref[(h * shares + r) * n_tp + t]
                right = heads_ref[((h + 1) * shares + r) * n_tp + t]
                for part in range(2):
                    cols = slice(part * HEAD_DIM, (part + 1) * HEAD_DIM)
                    o_ref[
                        pl.ds((2 * r + part) * half, half),
                        pl.ds((t * local_heads + h) * HEAD_DIM, 2 * HEAD_DIM),
                    ] = jnp.concatenate((left[:, cols], right[:, cols]), axis=1)
    sent(q_ref, n_sp - 1, 0)
    sent(kv_all, shares - 1, 1)
    sent(kv_all, groups - 1, 2)
    sent(kv_all, (groups - 1) * (shares - 1), 3)
    sent(out_ref, n - 1, 4)


def attend(kv, q, side_q, side_k, n_tp):
    local_heads, tok_dev, lanes = kv.shape
    n_sp, half_chunk = q.shape[:2]
    chunk = 2 * half_chunk
    n = n_sp * n_tp
    sub = chunk // n_tp
    bf16, f32 = jnp.bfloat16, jnp.float32
    vmem = pl.BlockSpec(memory_space=pltpu.VMEM)
    rows_dev = tok_dev // n_tp
    return pl.pallas_call(
        functools.partial(attend_kernel, n_tp=n_tp, local_heads=local_heads),
        out_shape=jax.ShapeDtypeStruct((rows_dev, n_tp * local_heads * HEAD_DIM), bf16),
        in_specs=[vmem] * 4,
        out_specs=vmem,
        scratch_shapes=[
            pltpu.VMEM((n_sp, tok_dev, lanes), bf16),
            pltpu.VMEM((n_sp, half_chunk, lanes), bf16),
            pltpu.VMEM((n_sp, tok_dev, lanes), bf16),
            pltpu.VMEM((n_sp, tok_dev, lanes), bf16),
            pltpu.VMEM((n_sp, chunk, lanes), bf16),
            pltpu.VMEM((n_sp, chunk, lanes), f32),
            pltpu.VMEM((n_sp, chunk, lanes), f32),
            pltpu.VMEM((n, sub // 2, lanes), bf16),
            pltpu.VMEM((n, sub // 2, lanes), bf16),
            pltpu.SemaphoreType.DMA((3,)),
            pltpu.SemaphoreType.DMA((n_sp,)),
            pltpu.SemaphoreType.DMA((n_sp,)),
            pltpu.SemaphoreType.DMA,
            pltpu.SemaphoreType.DMA((5,)),
        ],
        compiler_params=pltpu.CompilerParams(
            collective_id=0, has_side_effects=True, vmem_limit_bytes=56 * 2**20
        ),
        name="attend",
    )(kv, q, side_q, side_k)


def expert_kernel(
    heads_ref, ow_ref, res_ref, gains_ref, ids_ref, weight_ref, wg_hbm, wu_hbm, wd_hbm, o_ref,
    sent, arrived, made, returned, wg, wu, wd, gate_acc, up_acc, hidden, comb, stream, normed, weigh,
    w_sem, own_sem, send_sem, recv_sem, *, n_tp, chunks, tight,
):
    n, cap, width = sent.shape
    rows_dev = stream.shape[0]
    part = width // chunks
    last = chunks - 1
    fold = chunks == 4 and cap - tight == 2 and tight > 8
    keep = cap - 8
    group = n // GROUPS
    rows = group * cap
    f32, bf16 = jnp.float32, jnp.bfloat16
    sp, tp = lax.axis_index("sp"), lax.axis_index("tp")
    me = sp * n_tp + tp

    def peer(o):
        d = lax.rem(me + o, n)
        return d, (d // n_tp, lax.rem(d, n_tp))

    loads = [
        pltpu.make_async_copy(src, dst, w_sem.at[i])
        for i, (src, dst) in enumerate(((wg_hbm, wg), (wu_hbm, wu), (wd_hbm, wd)))
    ]
    for load in loads:
        load.start()

    barrier = pltpu.get_barrier_semaphore()

    def greet(o, carry):
        pl.semaphore_signal(barrier, inc=1, device_id=peer(o)[1], device_id_type=MESH)
        return carry

    lax.fori_loop(1, n, greet, 0)

    def cols(c):
        return pl.ds(c * part, part)

    expert = lax.broadcasted_iota(jnp.int32, (n, rows_dev), 0)
    tri = (
        lax.broadcasted_iota(jnp.int32, (rows_dev, rows_dev), 0)
        < lax.broadcasted_iota(jnp.int32, (rows_dev, rows_dev), 1)
    ).astype(f32).astype(bf16)
    taken = jnp.zeros((n, 1), f32)
    slots = []
    for k in range(ids_ref.shape[0]):
        ids = ids_ref[pl.ds(k, 1), :]
        named = (expert == ids).astype(f32)
        ahead = jnp.dot(named.astype(bf16), tri, preferred_element_type=f32) + taken
        rank = jnp.sum(named * ahead, axis=0, keepdims=True)
        taken = taken + jnp.sum(named, axis=1, keepdims=True)
        slots.append(ids * cap + rank.astype(jnp.int32))

    heads = heads_ref[...]
    total = jnp.zeros((rows_dev, 1), f32)
    for c in range(chunks):
        proj = jnp.dot(heads, ow_ref[:, cols(c)], preferred_element_type=f32)
        comb[:, cols(c)] = proj
        total = total + jnp.sum(proj * proj, axis=1, keepdims=True)
    scale = lax.rsqrt(total / width + NORM_EPS)
    total = jnp.zeros((rows_dev, 1), f32)
    for c in range(chunks):
        wide = res_ref[:, cols(c)].astype(f32) + comb[:, cols(c)] * scale * gains_ref[pl.ds(0, 1), cols(c)]
        stream[:, cols(c)] = wide.astype(bf16)
        wide = stream[:, cols(c)].astype(f32)
        total = total + jnp.sum(wide * wide, axis=1, keepdims=True)
    scale = lax.rsqrt(total / width + NORM_EPS)
    for c in range(chunks):
        wide = stream[:, cols(c)].astype(f32)
        normed[:, cols(c)] = (wide * scale * gains_ref[pl.ds(1, 1), cols(c)]).astype(bf16)
    pl.semaphore_wait(barrier, n - 1)

    def window(ref, at, c):
        if fold and c == last:
            return ref.at[at, pl.ds(0, keep), cols(c)]
        return ref.at[at, :, cols(c)]

    def send_all(src, dst, c, slot):
        def one(o, carry):
            d, where = peer(o)
            pltpu.make_async_remote_copy(
                src_ref=window(src, d, c),
                dst_ref=window(dst, me, c),
                send_sem=send_sem.at[slot],
                recv_sem=recv_sem.at[slot],
                device_id=where,
                device_id_type=MESH,
            ).start()
            return carry

        pltpu.make_async_copy(window(src, me, c), window(dst, me, c), own_sem.at[slot]).start()
        lax.fori_loop(1, n, one, 0)

    def all_copies(src, dst, c, slot):
        return pltpu.make_async_remote_copy(
            src_ref=window(src, pl.ds(0, n - 1), c),
            dst_ref=window(dst, pl.ds(0, n - 1), c),
            send_sem=send_sem.at[slot],
            recv_sem=recv_sem.at[slot],
            device_id=peer(1)[1],
            device_id_type=MESH,
        )

    def wait_all(src, dst, c, slot):
        pltpu.make_async_copy(window(src, me, c), window(dst, me, c), own_sem.at[slot]).wait()
        all_copies(src, dst, c, slot).wait_recv()

    spare = lax.broadcasted_iota(jnp.int32, (group, 8, part), 1)

    def unfold(ref):
        def one(g, carry):
            at = pl.ds(g * group, group)
            new = jnp.zeros((group, 8, part), f32)
            for c in range(last):
                tail = ref[at, keep:cap, cols(c)].astype(f32)
                new = jnp.where(spare == c, tail[:, 6:7], new)
                new = jnp.where(spare == last + c, tail[:, 7:8], new)
            ref[at, keep:cap, cols(last)] = new.astype(bf16)
            return carry

        lax.fori_loop(0, GROUPS, one, 0)

    for c in range(chunks):

        def gather(g, carry, c=c):
            row = g * rows + lax.broadcasted_iota(jnp.int32, (rows, rows_dev), 0)

            def named(target):
                return sum((target == slot).astype(f32) for slot in slots).astype(bf16)

            y = jnp.dot(named(row), normed[:, cols(c)], preferred_element_type=f32)
            if fold and c < last:
                at = lax.rem(row, cap)
                aim = jnp.where(at == tight, row - 6 + c, jnp.where(at == tight + 1, row - 4 + c, -1))
                y = y + jnp.dot(named(aim), normed[:, cols(last)], preferred_element_type=f32)
            sent[pl.ds(g * group, group), :, cols(c)] = y.astype(bf16).reshape(group, cap, part)
            return carry

        lax.fori_loop(0, GROUPS, gather, 0)
        send_all(sent, arrived, c, c)

    def weights(g, carry):
        at = pl.ds(pl.multiple_of(g * WEIGH_COLS, WEIGH_COLS), WEIGH_COLS)
        row = g * WEIGH_COLS + lax.broadcasted_iota(jnp.int32, (WEIGH_COLS, rows_dev), 0)
        mix = sum(
            jnp.where(row == slot, weight_ref[pl.ds(k, 1), :], 0.0) for k, slot in enumerate(slots)
        ).T
        for i in range(weigh.shape[0]):
            piece = mix.astype(bf16)
            weigh[i, :, at] = piece
            mix = mix - piece.astype(f32)
        return carry

    lax.fori_loop(0, n * cap // WEIGH_COLS, weights, 0)
    for load in loads[:2]:
        load.wait()

    for c in range(chunks):
        wait_all(sent, arrived, c, c)

        def gate_up(g, carry, c=c):
            x = arrived[pl.ds(g * group, group), :, cols(c)].reshape(rows, part)
            at = pl.ds(pl.multiple_of(g * rows, rows), rows)
            gate = jnp.dot(x, wg[cols(c), :], preferred_element_type=f32)
            up = jnp.dot(x, wu[cols(c), :], preferred_element_type=f32)
            if c > 0:
                gate, up = gate + gate_acc[at, :], up + up_acc[at, :]
            if c < last:
                gate_acc[at, :] = gate
                up_acc[at, :] = up
            else:
                hidden[at, :] = (jax.nn.silu(gate) * up).astype(bf16)
            return carry

        lax.fori_loop(0, GROUPS, gate_up, 0)
        if fold and c == last - 1:
            unfold(arrived)
    loads[2].wait()
    order = (last, *range(last))
    for c in order:

        def down(g, carry, c=c):
            at = pl.ds(pl.multiple_of(g * rows, rows), rows)
            some = pl.ds(g * group, group)
            y = jnp.dot(hidden[at, :], wd[:, cols(c)], preferred_element_type=f32)
            made[some, :, cols(c)] = y.astype(bf16).reshape(group, cap, part)
            if fold and c < last:
                tail = made[some, keep:cap, cols(c)].astype(f32)
                other = made[some, keep:cap, cols(last)].astype(f32)
                tail = jnp.where(spare == 6, other[:, c : c + 1], tail)
                tail = jnp.where(spare == 7, other[:, last + c : last + c + 1], tail)
                made[some, keep:cap, cols(c)] = tail.astype(bf16)
            return carry

        lax.fori_loop(0, GROUPS, down, 0)
        send_all(made, returned, c, chunks + c)
    total = jnp.zeros((rows_dev, 1), f32)

    def combine(c, total):
        back = returned[:, :, cols(c)].reshape(n * cap, part)
        mixed = sum(
            jnp.dot(weigh[i], back, preferred_element_type=f32) for i in range(weigh.shape[0])
        )
        comb[:, cols(c)] = mixed
        return total + jnp.sum(mixed * mixed, axis=1, keepdims=True)

    for c in order:
        wait_all(made, returned, c, chunks + c)
        if not (fold and c == last):
            total = combine(c, total)
    if fold:
        unfold(returned)
        total = combine(last, total)
    scale = lax.rsqrt(total / width + NORM_EPS)
    for c in range(chunks):
        o_ref[:, cols(c)] = (
            stream[:, cols(c)].astype(f32) + comb[:, cols(c)] * scale * gains_ref[pl.ds(2, 1), cols(c)]
        ).astype(bf16)
    for c in range(chunks):
        all_copies(sent, arrived, c, c).wait_send()
        all_copies(made, returned, c, chunks + c).wait_send()


def experts(heads, out_weight, residual, gains, ids, weight, w_gate, w_up, w_down, n, n_tp, tight):
    rows_dev, width = residual.shape
    cap = (tight + 7) // 8 * 8
    hidden = w_gate.shape[1]
    slots = n * cap
    chunks = CHUNKS
    vmem = pl.BlockSpec(memory_space=pltpu.VMEM)
    hbm = pl.BlockSpec(memory_space=pl.ANY)
    bf16, f32 = jnp.bfloat16, jnp.float32
    return pl.pallas_call(
        functools.partial(expert_kernel, n_tp=n_tp, chunks=chunks, tight=tight),
        out_shape=jax.ShapeDtypeStruct(residual.shape, bf16),
        in_specs=[vmem] * 6 + [hbm] * 3,
        out_specs=vmem,
        scratch_shapes=[
            pltpu.VMEM((n, cap, width), bf16),
            pltpu.VMEM((n, cap, width), bf16),
            pltpu.VMEM((n, cap, width), bf16),
            pltpu.VMEM((n, cap, width), bf16),
            pltpu.VMEM(w_gate.shape, bf16),
            pltpu.VMEM(w_up.shape, bf16),
            pltpu.VMEM(w_down.shape, bf16),
            pltpu.VMEM((slots, hidden), f32),
            pltpu.VMEM((slots, hidden), f32),
            pltpu.VMEM((slots, hidden), bf16),
            pltpu.VMEM(residual.shape, f32),
            pltpu.VMEM(residual.shape, bf16),
            pltpu.VMEM(residual.shape, bf16),
            pltpu.VMEM((2, rows_dev, slots), bf16),
            pltpu.SemaphoreType.DMA((3,)),
            pltpu.SemaphoreType.DMA((2 * chunks,)),
            pltpu.SemaphoreType.DMA((2 * chunks,)),
            pltpu.SemaphoreType.DMA((2 * chunks,)),
        ],
        compiler_params=pltpu.CompilerParams(
            collective_id=1, has_side_effects=True, vmem_limit_bytes=56 * 2**20
        ),
        name="experts",
    )(heads, out_weight, residual, gains, ids, weight, w_gate, w_up, w_down)


def local(
    queries,
    key_rows,
    value_rows,
    cum_gate,
    residual,
    out_weight,
    gain_mix,
    gain_pre,
    gain_post,
    route_ids,
    route_weight,
    w_gate,
    w_up,
    w_down,
):
    tok_dev, feature_width = queries.shape
    local_heads = feature_width // HEAD_DIM
    n_sp, n_tp = lax.axis_size("sp"), lax.axis_size("tp")
    shares = n_sp // local_heads
    rows_dev = residual.shape[0]
    sub = rows_dev // shares
    chunk = n_tp * sub
    kv, q = pack(queries, key_rows, value_rows, shares, n_tp)

    me = lax.axis_index("sp")
    gate = lax.dynamic_index_in_dim(cum_gate, me // shares, 0, keepdims=False)
    gate_q = gate.reshape(n_sp * n_tp, shares, sub)
    gate_q = lax.dynamic_index_in_dim(gate_q, me % shares, 1, keepdims=False).reshape(-1)
    ones_q = jnp.ones((n_sp * chunk,), jnp.bfloat16)
    ones_k = jnp.ones((n_sp * tok_dev,), jnp.bfloat16)
    lanes = jnp.arange(2 * HEAD_DIM)
    place_side = (lanes == HEAD_DIM + jnp.arange(6)[:, None]).astype(jnp.bfloat16)

    def side_lanes(parts):
        return lax.dot_general(
            jnp.stack(parts), place_side, (((0,), (0,)), ((), ())), preferred_element_type=jnp.float32
        ).astype(jnp.bfloat16)

    side_q = side_lanes(bf16_parts(gate_q) + [ones_q] * 3)
    side_k = side_lanes([ones_k] * 3 + bf16_parts(-gate))
    side_k = side_k.reshape(n_sp, tok_dev, 2 * HEAD_DIM)
    head_rows = attend(kv, q, side_q, side_k, n_tp)
    top_count = route_ids.shape[1]
    experts_all = n_sp * n_tp
    tight = max(2, (4 * rows_dev * top_count + 3 * experts_all - 1) // (3 * experts_all))
    return experts(
        head_rows, out_weight, residual, jnp.stack((gain_mix, gain_pre, gain_post)),
        route_ids.T, route_weight.T, w_gate[0], w_up[0], w_down[0], experts_all, n_tp, tight,
    )


def solution(mesh):
    return jax.shard_map(
        local,
        mesh=mesh,
        in_specs=(
            P("sp", "tp"),
            P("sp", "tp"),
            P("sp", "tp"),
            P("tp", None),
            P(("sp", "tp"), None),
            P(),
            P(),
            P(),
            P(),
            P(("sp", "tp"), None),
            P(("sp", "tp"), None),
            P(("sp", "tp"), None, None),
            P(("sp", "tp"), None, None),
            P(("sp", "tp"), None, None),
        ),
        out_specs=P(("sp", "tp"), None),
        check_vma=False,
    )
```

```python
import functools
import math

import jax
import jax.numpy as jnp
from jax import lax
from jax.experimental import pallas as pl
from jax.experimental.pallas import tpu as pltpu
from jax.sharding import PartitionSpec as P

HEAD_DIM = 64
NORM_EPS = 1e-06
MASKED = -1e30
MESH = pl.DeviceIdType.MESH
CHUNKS = 4
GROUPS = 4
EXP2_SCALE = math.log2(math.e)
WEIGH_COLS = 256


def attend_kernel(
    q_hbm, k_hbm, v_hbm, gate_ref, o_ref,
    q_in, k_in, v_in, kv_ref, q_ref,
    kv_all, q_all, k_aug, v_turned, q_aug, side_ref, peak_ref, acc_ref, scores_a, scores_b, out_ref, heads_ref,
    in_sem, own_sem, q_sem, kv_sem, head_sem, send_sem, *, n_tp, local_heads,
):
    groups = local_heads
    n_sp = q_ref.shape[0]
    shares = n_sp // groups
    tok_dev = kv_ref.shape[1]
    f32, bf16 = jnp.float32, jnp.bfloat16
    chunk = 2 * q_ref.shape[1]
    sub = chunk // n_tp
    rows_dev = sub * shares
    lanes = 2 * HEAD_DIM
    n = n_sp * n_tp
    sp, tp = lax.axis_index("sp"), lax.axis_index("tp")
    me = sp * n_tp + tp
    group, rank = sp // shares, lax.rem(sp, shares)

    def plane(s):
        down = jnp.where(s <= group, group - s, s)
        up = jnp.where(s <= groups - 1 - group, group + s, groups - 1 - s)
        return jnp.where(2 * group < groups, down, up)

    def block_at(i):
        return plane(i // shares) * shares + lax.rem(rank + lax.rem(i, shares), shares)

    loads = [
        pltpu.make_async_copy(src, dst, in_sem.at[i])
        for i, (src, dst) in enumerate(((q_hbm, q_in), (k_hbm, k_in), (v_hbm, v_in)))
    ]
    for load in loads:
        load.start()
    barrier = pltpu.get_barrier_semaphore()

    def greet(o, carry):
        d = lax.rem(me + o, n)
        where = (d // n_tp, lax.rem(d, n_tp))
        pl.semaphore_signal(barrier, inc=1, device_id=where, device_id_type=MESH)
        return carry

    lax.fori_loop(1, n, greet, 0)
    for load in loads:
        load.wait()
    for h in range(groups):
        head = pl.ds(h * HEAD_DIM, HEAD_DIM)
        kv_ref[h] = jnp.concatenate((k_in[:, head], v_in[:, head]), axis=1)
        for r in range(shares):
            for t in range(n_tp // 2):
                low, high = (
                    q_in[pl.ds((t + half) * rows_dev + r * sub, sub), head]
                    for half in (0, n_tp // 2)
                )
                q_ref[h * shares + r, pl.ds(t * sub, sub)] = jnp.concatenate((low, high), axis=1)
    kv_all[sp] = kv_ref[group]
    q_all[sp] = q_ref[sp]
    pl.semaphore_wait(barrier, n - 1)

    def kv_copy(src, block, dest, slot):
        return pltpu.make_async_remote_copy(
            src_ref=src, dst_ref=kv_all.at[block],
            send_sem=send_sem.at[slot], recv_sem=kv_sem.at[block],
            device_id=(dest, tp), device_id_type=MESH,
        )

    def q_copy(src, block, dest):
        return pltpu.make_async_remote_copy(
            src_ref=src, dst_ref=q_all.at[block],
            send_sem=send_sem.at[0], recv_sem=q_sem.at[block],
            device_id=(dest, tp), device_id_type=MESH,
        )

    for s in range(groups):
        for k in range(shares):
            dest = block_at(s * shares + k)
            if s or k:
                q_copy(q_ref.at[dest], sp, dest).start()
            if s == 0 and k:
                kv_copy(kv_ref.at[group], sp, dest, 1).start()
            if s and k == 0:
                kv_copy(kv_ref.at[plane(s)], sp, dest, 2).start()

    slot = lax.broadcasted_iota(jnp.int32, (8, tok_dev), 0)
    place = lax.broadcasted_iota(jnp.int32, (8, lanes), 1) - HEAD_DIM
    place = (place == lax.broadcasted_iota(jnp.int32, (8, lanes), 0)).astype(f32).astype(bf16)

    def spread(rows):
        return lax.dot_general(
            rows.astype(bf16), place, (((0,), (0,)), ((), ())), preferred_element_type=f32
        )

    def build(block):
        at = pl.ds(pl.multiple_of(block * tok_dev, tok_dev), tok_dev)
        gate = gate_ref[pl.ds(group, 1), at] * EXP2_SCALE
        for_k = (slot < 3).astype(f32)
        for_q = ((slot >= 3) & (slot < 6)).astype(f32)
        for i in range(3):
            piece = gate.astype(bf16).astype(f32)
            gate = gate - piece
            for_k = jnp.where(slot == 3 + i, -piece, for_k)
            for_q = jnp.where(slot == i, piece, for_q)
        side_ref[...] = spread(for_q)
        lane = lax.broadcasted_iota(jnp.int32, (tok_dev, lanes), 1)
        kv = kv_all[block].astype(f32)
        k_aug[block, :, :lanes] = jnp.where(lane < HEAD_DIM, kv, spread(for_k)).astype(bf16)
        k_aug[block, :, lanes:] = jnp.where(lane < HEAD_DIM, kv, 0.0).astype(bf16)
        turned = kv.T
        v_turned[block, :HEAD_DIM] = turned[HEAD_DIM:].astype(bf16)
        v_turned[block, HEAD_DIM:] = jnp.ones((16, tok_dev), bf16)
        packed = q_all[block]
        queries = jnp.concatenate((packed[:, :HEAD_DIM], packed[:, HEAD_DIM:]), axis=0)
        queries = queries.astype(f32) * (HEAD_DIM**-0.5 * EXP2_SCALE)
        high = queries.astype(bf16)
        low = (queries - high.astype(f32)).astype(bf16)
        for t in range(n_tp):
            rows = pl.ds(t * sub, sub)
            side = side_ref[pl.ds(pl.multiple_of(t * rows_dev + rank * sub, sub), sub), HEAD_DIM:]
            q_aug[block, rows, :lanes] = jnp.concatenate(
                (high[t * sub : (t + 1) * sub], side.astype(bf16)), axis=1
            )
        q_aug[block, :, lanes:] = jnp.concatenate((low, jnp.zeros_like(low)), axis=1)
        peak_ref[block] = jnp.full((1, chunk), MASKED, f32)
        acc_ref[block] = jnp.zeros((HEAD_DIM + 16, chunk), f32)

    halves = 2 if chunk >= 512 else 1
    half_rows = chunk // halves
    scores = (scores_a, scores_b)[:halves]

    def score(h, i, j):
        found = lax.dot_general(
            k_aug[j], q_aug[i, pl.ds(h * half_rows, half_rows)], (((1,), (1,)), ((), ())),
            preferred_element_type=f32,
        )
        scores[h][...] = found
        return jnp.max(found, axis=0, keepdims=True)

    def weigh(h, top, i, j, masked):
        rows = pl.ds(h * half_rows, half_rows)
        count = tok_dev // halves * (h + 1) if masked else tok_dev
        found = scores[h][:count]
        if masked:
            key = lax.broadcasted_iota(jnp.int32, (count, 1), 0)
            row = lax.broadcasted_iota(jnp.int32, (1, half_rows), 1) + h * half_rows
            pos = row // sub * rows_dev + rank * sub + lax.rem(row, sub)
            found = jnp.where(key <= pos, found, MASKED)
            top = jnp.max(found, axis=0, keepdims=True)
        before = peak_ref[i, :, rows]
        peak = jnp.maximum(before, top)
        probs = jnp.exp2(found - peak).astype(bf16)
        peak_ref[i, :, rows] = peak
        acc_ref[i, :, rows] = acc_ref[i, :, rows] * jnp.exp2(before - peak) + jnp.dot(
            v_turned[j, :, :count], probs, preferred_element_type=f32
        )

    def step(i, j, i_next, j_next, top, masked):
        for h in range(halves):
            ahead = (h + 1, i, j) if h + 1 < halves else (0, i_next, j_next)
            early = halves > 1 and not (masked and h + 1 == halves)
            if early:
                found = score(*ahead)
            weigh(h, top, i, j, masked)
            if not early and not masked:
                found = score(*ahead)
            top = found if early or not masked else top
        return top

    def head_copy(block, t):
        slot = block * n_tp + t
        return pltpu.make_async_remote_copy(
            src_ref=out_ref.at[slot], dst_ref=heads_ref.at[me],
            send_sem=send_sem.at[4], recv_sem=head_sem,
            device_id=(block, t), device_id_type=MESH,
        )

    own_head = pltpu.make_async_copy(out_ref.at[me], heads_ref.at[me], own_sem)

    def finish(block):
        acc = acc_ref[block]
        out = (acc[:HEAD_DIM] / acc[HEAD_DIM : HEAD_DIM + 1]).T
        half = sub // 2
        for t in range(n_tp):
            top, low = (out[t * sub + at : t * sub + at + half] for at in (0, half))
            out_ref[block * n_tp + t] = jnp.concatenate((top, low), axis=1).astype(jnp.bfloat16)
        for t in range(n_tp):
            mine = (block == sp) & (tp == t)

            @pl.when(mine)
            def _():
                own_head.start()

            @pl.when(jnp.logical_not(mine))
            def _(t=t):
                head_copy(block, t).start()

    def relay(i):
        block = block_at(i)
        kv_copy(kv_all.at[block], block, block, 3).wait_recv()
        for k in range(1, shares):
            dest = group * shares + lax.rem(rank + k, shares)
            kv_copy(kv_all.at[block], block, dest, 3).start()

    def one_block(i, carry):
        block = block_at(i)
        s, k = i // shares, lax.rem(i, shares)
        turn = k == shares - 1

        @pl.when(i > 0)
        def _():
            q_copy(q_all.at[block], block, block).wait_recv()

        @pl.when(k > 0)
        def _():
            kv_copy(kv_all.at[block], block, block, 3).wait_recv()

        @pl.when(turn & (s > 0) & (s < groups - 1))
        def _():
            relay(i + 1)

        build(block)

        def blocks(m):
            other = jnp.where(m < i, block_at(jnp.maximum(i - 1 - m, 0)), block)
            return jnp.maximum(block, other), jnp.minimum(block, other)

        def pair(m, top):
            other = block_at(i - 1 - m)
            top = step(*blocks(m), *blocks(m + 1), top, False)

            @pl.when(i == n_sp - 1)
            def _():
                finish(other)

            return top

        top = lax.fori_loop(0, i, pair, score(0, *blocks(0)))
        step(block, block, block, block, top, True)

        @pl.when(turn & (s == 0) & (groups > 1))
        def _():
            relay(i + 1)

        return carry

    lax.fori_loop(0, n_sp, one_block, 0)
    finish(block_at(n_sp - 1))
    own_head.wait()

    def sent(buf, count, slot):
        if count:
            pltpu.make_async_remote_copy(
                src_ref=buf.at[pl.ds(0, count)], dst_ref=buf.at[pl.ds(0, count)],
                send_sem=send_sem.at[slot], recv_sem=head_sem,
                device_id=(sp, tp), device_id_type=MESH,
            ).wait_send()

    pltpu.make_async_remote_copy(
        src_ref=heads_ref.at[pl.ds(0, n - 1)], dst_ref=heads_ref.at[pl.ds(0, n - 1)],
        send_sem=send_sem.at[4], recv_sem=head_sem,
        device_id=(sp, tp), device_id_type=MESH,
    ).wait_recv()
    half = sub // 2
    for t in range(n_tp):
        for h in range(0, local_heads, 2):
            for r in range(shares):
                left = heads_ref[(h * shares + r) * n_tp + t]
                right = heads_ref[((h + 1) * shares + r) * n_tp + t]
                for part in range(2):
                    cols = slice(part * HEAD_DIM, (part + 1) * HEAD_DIM)
                    o_ref[
                        pl.ds((2 * r + part) * half, half),
                        pl.ds((t * local_heads + h) * HEAD_DIM, 2 * HEAD_DIM),
                    ] = jnp.concatenate((left[:, cols], right[:, cols]), axis=1)
    sent(q_ref, n_sp - 1, 0)
    sent(kv_all, shares - 1, 1)
    sent(kv_all, groups - 1, 2)
    sent(kv_all, (groups - 1) * (shares - 1), 3)
    sent(out_ref, n - 1, 4)


def attend(queries, key_rows, value_rows, gate, n_sp, n_tp):
    tok_dev, width = queries.shape
    local_heads = width // HEAD_DIM
    lanes = 2 * HEAD_DIM
    shares = n_sp // local_heads
    rows_dev = tok_dev // n_tp
    sub = rows_dev // shares
    chunk = n_tp * sub
    n = n_sp * n_tp
    bf16, f32 = jnp.bfloat16, jnp.float32
    vmem = pl.BlockSpec(memory_space=pltpu.VMEM)
    hbm = pl.BlockSpec(memory_space=pl.ANY)
    return pl.pallas_call(
        functools.partial(attend_kernel, n_tp=n_tp, local_heads=local_heads),
        out_shape=jax.ShapeDtypeStruct((rows_dev, n_tp * width), bf16),
        in_specs=[hbm] * 3 + [vmem],
        out_specs=vmem,
        scratch_shapes=[pltpu.VMEM((tok_dev, width), bf16)] * 3
        + [
            pltpu.VMEM((local_heads, tok_dev, lanes), bf16),
            pltpu.VMEM((n_sp, chunk // 2, lanes), bf16),
            pltpu.VMEM((n_sp, tok_dev, lanes), bf16),
            pltpu.VMEM((n_sp, chunk // 2, lanes), bf16),
            pltpu.VMEM((n_sp, tok_dev, 2 * lanes), bf16),
            pltpu.VMEM((n_sp, HEAD_DIM + 16, tok_dev), bf16),
            pltpu.VMEM((n_sp, chunk, 2 * lanes), bf16),
            pltpu.VMEM((tok_dev, lanes), f32),
            pltpu.VMEM((n_sp, 1, chunk), f32),
            pltpu.VMEM((n_sp, HEAD_DIM + 16, chunk), f32),
            pltpu.VMEM((tok_dev, chunk // 2 if chunk >= 512 else chunk), f32),
            pltpu.VMEM((tok_dev, chunk // 2 if chunk >= 512 else chunk), f32),
            pltpu.VMEM((n, sub // 2, lanes), bf16),
            pltpu.VMEM((n, sub // 2, lanes), bf16),
            pltpu.SemaphoreType.DMA((3,)),
            pltpu.SemaphoreType.DMA,
            pltpu.SemaphoreType.DMA((n_sp,)),
            pltpu.SemaphoreType.DMA((n_sp,)),
            pltpu.SemaphoreType.DMA,
            pltpu.SemaphoreType.DMA((5,)),
        ],
        compiler_params=pltpu.CompilerParams(
            collective_id=0, has_side_effects=True, vmem_limit_bytes=52 * 2**20
        ),
        name="attend",
    )(queries, key_rows, value_rows, gate)


def expert_kernel(
    heads_ref, ow_ref, res_ref, gains_ref, ids_ref, weight_ref, wg_hbm, wu_hbm, wd_hbm, o_ref,
    sent, arrived, made, returned, wg, wu, wd, gate_acc, up_acc, hidden, comb, stream, normed, weigh,
    w_sem, own_sem, send_sem, recv_sem, *, n_tp, chunks, tight,
):
    n, cap, width = sent.shape
    rows_dev = stream.shape[0]
    part = width // chunks
    last = chunks - 1
    fold = chunks == 4 and cap - tight == 2 and tight > 8
    keep = cap - 8
    group = n // GROUPS
    rows = group * cap
    f32, bf16 = jnp.float32, jnp.bfloat16
    sp, tp = lax.axis_index("sp"), lax.axis_index("tp")
    me = sp * n_tp + tp

    def peer(o):
        d = lax.rem(me + o, n)
        return d, (d // n_tp, lax.rem(d, n_tp))

    loads = [
        pltpu.make_async_copy(src, dst, w_sem.at[i])
        for i, (src, dst) in enumerate(((wg_hbm, wg), (wu_hbm, wu), (wd_hbm, wd)))
    ]
    for load in loads:
        load.start()

    barrier = pltpu.get_barrier_semaphore()

    def greet(o, carry):
        pl.semaphore_signal(barrier, inc=1, device_id=peer(o)[1], device_id_type=MESH)
        return carry

    lax.fori_loop(1, n, greet, 0)

    def cols(c):
        return pl.ds(c * part, part)

    expert = lax.broadcasted_iota(jnp.int32, (n, rows_dev), 0)
    tri = (
        lax.broadcasted_iota(jnp.int32, (rows_dev, rows_dev), 0)
        < lax.broadcasted_iota(jnp.int32, (rows_dev, rows_dev), 1)
    ).astype(f32).astype(bf16)
    taken = jnp.zeros((n, 1), f32)
    slots = []
    for k in range(ids_ref.shape[0]):
        ids = ids_ref[pl.ds(k, 1), :]
        named = (expert == ids).astype(f32)
        ahead = jnp.dot(named.astype(bf16), tri, preferred_element_type=f32) + taken
        rank = jnp.sum(named * ahead, axis=0, keepdims=True)
        taken = taken + jnp.sum(named, axis=1, keepdims=True)
        slots.append(ids * cap + rank.astype(jnp.int32))

    heads = heads_ref[...]
    total = jnp.zeros((rows_dev, 1), f32)
    for c in range(chunks):
        proj = jnp.dot(heads, ow_ref[:, cols(c)], preferred_element_type=f32)
        comb[:, cols(c)] = proj
        total = total + jnp.sum(proj * proj, axis=1, keepdims=True)
    scale = lax.rsqrt(total / width + NORM_EPS)
    total = jnp.zeros((rows_dev, 1), f32)
    for c in range(chunks):
        wide = res_ref[:, cols(c)].astype(f32) + comb[:, cols(c)] * scale * gains_ref[pl.ds(0, 1), cols(c)]
        stream[:, cols(c)] = wide.astype(bf16)
        wide = stream[:, cols(c)].astype(f32)
        total = total + jnp.sum(wide * wide, axis=1, keepdims=True)
    scale = lax.rsqrt(total / width + NORM_EPS)
    for c in range(chunks):
        wide = stream[:, cols(c)].astype(f32)
        normed[:, cols(c)] = (wide * scale * gains_ref[pl.ds(1, 1), cols(c)]).astype(bf16)
    pl.semaphore_wait(barrier, n - 1)

    def window(ref, at, c):
        if fold and c == last:
            return ref.at[at, pl.ds(0, keep), cols(c)]
        return ref.at[at, :, cols(c)]

    def send_all(src, dst, c, slot):
        def one(o, carry):
            d, where = peer(o)
            pltpu.make_async_remote_copy(
                src_ref=window(src, d, c),
                dst_ref=window(dst, me, c),
                send_sem=send_sem.at[slot],
                recv_sem=recv_sem.at[slot],
                device_id=where,
                device_id_type=MESH,
            ).start()
            return carry

        pltpu.make_async_copy(window(src, me, c), window(dst, me, c), own_sem.at[slot]).start()
        lax.fori_loop(1, n, one, 0)

    def all_copies(src, dst, c, slot):
        return pltpu.make_async_remote_copy(
            src_ref=window(src, pl.ds(0, n - 1), c),
            dst_ref=window(dst, pl.ds(0, n - 1), c),
            send_sem=send_sem.at[slot],
            recv_sem=recv_sem.at[slot],
            device_id=peer(1)[1],
            device_id_type=MESH,
        )

    def wait_all(src, dst, c, slot):
        pltpu.make_async_copy(window(src, me, c), window(dst, me, c), own_sem.at[slot]).wait()
        all_copies(src, dst, c, slot).wait_recv()

    spare = lax.broadcasted_iota(jnp.int32, (group, 8, part), 1)

    def unfold(ref):
        def one(g, carry):
            at = pl.ds(g * group, group)
            new = jnp.zeros((group, 8, part), f32)
            for c in range(last):
                tail = ref[at, keep:cap, cols(c)].astype(f32)
                new = jnp.where(spare == c, tail[:, 6:7], new)
                new = jnp.where(spare == last + c, tail[:, 7:8], new)
            ref[at, keep:cap, cols(last)] = new.astype(bf16)
            return carry

        lax.fori_loop(0, GROUPS, one, 0)

    for c in range(chunks):

        def gather(g, carry, c=c):
            row = g * rows + lax.broadcasted_iota(jnp.int32, (rows, rows_dev), 0)

            def named(target):
                return sum((target == slot).astype(f32) for slot in slots).astype(bf16)

            y = jnp.dot(named(row), normed[:, cols(c)], preferred_element_type=f32)
            if fold and c < last:
                at = lax.rem(row, cap)
                aim = jnp.where(at == tight, row - 6 + c, jnp.where(at == tight + 1, row - 4 + c, -1))
                y = y + jnp.dot(named(aim), normed[:, cols(last)], preferred_element_type=f32)
            sent[pl.ds(g * group, group), :, cols(c)] = y.astype(bf16).reshape(group, cap, part)
            return carry

        lax.fori_loop(0, GROUPS, gather, 0)
        send_all(sent, arrived, c, c)

    def weights(g, carry):
        at = pl.ds(pl.multiple_of(g * WEIGH_COLS, WEIGH_COLS), WEIGH_COLS)
        row = g * WEIGH_COLS + lax.broadcasted_iota(jnp.int32, (WEIGH_COLS, rows_dev), 0)
        mix = sum(
            jnp.where(row == slot, weight_ref[pl.ds(k, 1), :], 0.0) for k, slot in enumerate(slots)
        ).T
        for i in range(weigh.shape[0]):
            piece = mix.astype(bf16)
            weigh[i, :, at] = piece
            mix = mix - piece.astype(f32)
        return carry

    lax.fori_loop(0, n * cap // WEIGH_COLS, weights, 0)
    for load in loads[:2]:
        load.wait()

    for c in range(chunks):
        wait_all(sent, arrived, c, c)

        def gate_up(g, carry, c=c):
            x = arrived[pl.ds(g * group, group), :, cols(c)].reshape(rows, part)
            at = pl.ds(pl.multiple_of(g * rows, rows), rows)
            gate = jnp.dot(x, wg[cols(c), :], preferred_element_type=f32)
            up = jnp.dot(x, wu[cols(c), :], preferred_element_type=f32)
            if c > 0:
                gate, up = gate + gate_acc[at, :], up + up_acc[at, :]
            if c < last:
                gate_acc[at, :] = gate
                up_acc[at, :] = up
            else:
                hidden[at, :] = (jax.nn.silu(gate) * up).astype(bf16)
            return carry

        lax.fori_loop(0, GROUPS, gate_up, 0)
        if fold and c == last - 1:
            unfold(arrived)
    loads[2].wait()
    order = (last, *range(last))
    for c in order:

        def down(g, carry, c=c):
            at = pl.ds(pl.multiple_of(g * rows, rows), rows)
            some = pl.ds(g * group, group)
            y = jnp.dot(hidden[at, :], wd[:, cols(c)], preferred_element_type=f32)
            made[some, :, cols(c)] = y.astype(bf16).reshape(group, cap, part)
            if fold and c < last:
                tail = made[some, keep:cap, cols(c)].astype(f32)
                other = made[some, keep:cap, cols(last)].astype(f32)
                tail = jnp.where(spare == 6, other[:, c : c + 1], tail)
                tail = jnp.where(spare == 7, other[:, last + c : last + c + 1], tail)
                made[some, keep:cap, cols(c)] = tail.astype(bf16)
            return carry

        lax.fori_loop(0, GROUPS, down, 0)
        send_all(made, returned, c, chunks + c)
    total = jnp.zeros((rows_dev, 1), f32)

    def combine(c, total):
        back = returned[:, :, cols(c)].reshape(n * cap, part)
        mixed = sum(
            jnp.dot(weigh[i], back, preferred_element_type=f32) for i in range(weigh.shape[0])
        )
        comb[:, cols(c)] = mixed
        return total + jnp.sum(mixed * mixed, axis=1, keepdims=True)

    for c in order:
        wait_all(made, returned, c, chunks + c)
        if not (fold and c == last):
            total = combine(c, total)
    if fold:
        unfold(returned)
        total = combine(last, total)
    scale = lax.rsqrt(total / width + NORM_EPS)
    for c in range(chunks):
        o_ref[:, cols(c)] = (
            stream[:, cols(c)].astype(f32) + comb[:, cols(c)] * scale * gains_ref[pl.ds(2, 1), cols(c)]
        ).astype(bf16)
    for c in range(chunks):
        all_copies(sent, arrived, c, c).wait_send()
        all_copies(made, returned, c, chunks + c).wait_send()


def experts(heads, out_weight, residual, gains, ids, weight, w_gate, w_up, w_down, n, n_tp, tight):
    rows_dev, width = residual.shape
    cap = (tight + 7) // 8 * 8
    hidden = w_gate.shape[1]
    slots = n * cap
    chunks = CHUNKS
    vmem = pl.BlockSpec(memory_space=pltpu.VMEM)
    hbm = pl.BlockSpec(memory_space=pl.ANY)
    bf16, f32 = jnp.bfloat16, jnp.float32
    return pl.pallas_call(
        functools.partial(expert_kernel, n_tp=n_tp, chunks=chunks, tight=tight),
        out_shape=jax.ShapeDtypeStruct(residual.shape, bf16),
        in_specs=[vmem] * 6 + [hbm] * 3,
        out_specs=vmem,
        scratch_shapes=[
            pltpu.VMEM((n, cap, width), bf16),
            pltpu.VMEM((n, cap, width), bf16),
            pltpu.VMEM((n, cap, width), bf16),
            pltpu.VMEM((n, cap, width), bf16),
            pltpu.VMEM(w_gate.shape, bf16),
            pltpu.VMEM(w_up.shape, bf16),
            pltpu.VMEM(w_down.shape, bf16),
            pltpu.VMEM((slots, hidden), f32),
            pltpu.VMEM((slots, hidden), f32),
            pltpu.VMEM((slots, hidden), bf16),
            pltpu.VMEM(residual.shape, f32),
            pltpu.VMEM(residual.shape, bf16),
            pltpu.VMEM(residual.shape, bf16),
            pltpu.VMEM((2, rows_dev, slots), bf16),
            pltpu.SemaphoreType.DMA((3,)),
            pltpu.SemaphoreType.DMA((2 * chunks,)),
            pltpu.SemaphoreType.DMA((2 * chunks,)),
            pltpu.SemaphoreType.DMA((2 * chunks,)),
        ],
        compiler_params=pltpu.CompilerParams(
            collective_id=1, has_side_effects=True, vmem_limit_bytes=56 * 2**20
        ),
        name="experts",
    )(heads, out_weight, residual, gains, ids, weight, w_gate, w_up, w_down)


def local(
    queries,
    key_rows,
    value_rows,
    cum_gate,
    residual,
    out_weight,
    gain_mix,
    gain_pre,
    gain_post,
    route_ids,
    route_weight,
    w_gate,
    w_up,
    w_down,
):
    n_sp, n_tp = lax.axis_size("sp"), lax.axis_size("tp")
    rows_dev = residual.shape[0]
    head_rows = attend(queries, key_rows, value_rows, cum_gate, n_sp, n_tp)
    top_count = route_ids.shape[1]
    experts_all = n_sp * n_tp
    tight = max(2, (4 * rows_dev * top_count + 3 * experts_all - 1) // (3 * experts_all))
    return experts(
        head_rows, out_weight, residual, jnp.stack((gain_mix, gain_pre, gain_post)),
        route_ids.T, route_weight.T, w_gate[0], w_up[0], w_down[0], experts_all, n_tp, tight,
    )


def solution(mesh):
    return jax.shard_map(
        local,
        mesh=mesh,
        in_specs=(
            P("sp", "tp"),
            P("sp", "tp"),
            P("sp", "tp"),
            P("tp", None),
            P(("sp", "tp"), None),
            P(),
            P(),
            P(),
            P(),
            P(("sp", "tp"), None),
            P(("sp", "tp"), None),
            P(("sp", "tp"), None, None),
            P(("sp", "tp"), None, None),
            P(("sp", "tp"), None, None),
        ),
        out_specs=P(("sp", "tp"), None),
        check_vma=False,
    )
```

```python
import functools
import math

import jax
import jax.numpy as jnp
from jax import lax
from jax.experimental import pallas as pl
from jax.experimental.pallas import tpu as pltpu
from jax.sharding import PartitionSpec as P

HEAD_DIM = 64
NORM_EPS = 1e-06
MASKED = -1e30
MESH = pl.DeviceIdType.MESH
CHUNKS = 4
GROUPS = 4
EXP2_SCALE = math.log2(math.e)
WEIGH_COLS = 256
KV_PARTS = 2


def attend_kernel(
    q_hbm, k_hbm, v_hbm, gate_ref, o_ref,
    q_in, k_in, v_in, kv_ref, q_ref,
    kv_all, q_all, k_aug, v_turned, q_aug, side_ref, peak_ref, acc_ref, scores_a, scores_b, out_ref, heads_ref,
    in_sem, own_sem, q_sem, kv_sem, head_sem, send_sem, *, n_tp, local_heads,
):
    groups = local_heads
    n_sp = q_ref.shape[0]
    shares = n_sp // groups
    tok_dev = kv_ref.shape[1]
    f32, bf16 = jnp.float32, jnp.bfloat16
    chunk = 2 * q_ref.shape[1]
    sub = chunk // n_tp
    rows_dev = sub * shares
    lanes = 2 * HEAD_DIM
    n = n_sp * n_tp
    sp, tp = lax.axis_index("sp"), lax.axis_index("tp")
    me = sp * n_tp + tp
    group, rank = sp // shares, lax.rem(sp, shares)

    def plane(s):
        down = jnp.where(s <= group, group - s, s)
        up = jnp.where(s <= groups - 1 - group, group + s, groups - 1 - s)
        return jnp.where(2 * group < groups, down, up)

    def target(s):
        down = jnp.where(group > 0, groups + group - s, s)
        down = jnp.where(s <= group, group - s, down)
        up = jnp.where(group < groups - 1, s - groups + group, groups - 1 - s)
        up = jnp.where(s <= groups - 1 - group, group + s, up)
        return jnp.where(2 * group < groups, down, up)

    def block_at(i):
        return plane(i // shares) * shares + lax.rem(rank + lax.rem(i, shares), shares)

    loads = [
        pltpu.make_async_copy(src, dst, in_sem.at[i])
        for i, (src, dst) in enumerate(((q_hbm, q_in), (k_hbm, k_in), (v_hbm, v_in)))
    ]
    for load in loads:
        load.start()
    barrier = pltpu.get_barrier_semaphore()

    def greet(o, carry):
        d = lax.rem(me + o, n)
        where = (d // n_tp, lax.rem(d, n_tp))
        pl.semaphore_signal(barrier, inc=1, device_id=where, device_id_type=MESH)
        return carry

    lax.fori_loop(1, n, greet, 0)
    for load in loads:
        load.wait()
    for h in range(groups):
        head = pl.ds(h * HEAD_DIM, HEAD_DIM)
        kv_ref[h] = jnp.concatenate((k_in[:, head], v_in[:, head]), axis=1)
        for r in range(shares):
            for t in range(n_tp // 2):
                low, high = (
                    q_in[pl.ds((t + half) * rows_dev + r * sub, sub), head]
                    for half in (0, n_tp // 2)
                )
                q_ref[h * shares + r, pl.ds(t * sub, sub)] = jnp.concatenate((low, high), axis=1)
    kv_all[sp] = kv_ref[group]
    q_all[sp] = q_ref[sp]
    pl.semaphore_wait(barrier, n - 1)

    def kv_copies(src, index, block, dest, slot):
        size = tok_dev // KV_PARTS
        return [
            pltpu.make_async_remote_copy(
                src_ref=src.at[index, pl.ds(part * size, size)],
                dst_ref=kv_all.at[block, pl.ds(part * size, size)],
                send_sem=send_sem.at[slot], recv_sem=kv_sem.at[block, part],
                device_id=(dest, tp), device_id_type=MESH,
            )
            for part in range(KV_PARTS)
        ]

    def kv_send(*where):
        for copy in kv_copies(*where):
            copy.start()

    def q_copy(src, block, dest):
        return pltpu.make_async_remote_copy(
            src_ref=src, dst_ref=q_all.at[block],
            send_sem=send_sem.at[0], recv_sem=q_sem.at[block],
            device_id=(dest, tp), device_id_type=MESH,
        )

    for s in range(groups):
        for k in range(shares):
            dest = block_at(k) if s == 0 else target(s) * shares + lax.rem(rank + k, shares)
            if s or k:
                q_copy(q_ref.at[dest], sp, dest).start()
            if s == 0 and k:
                kv_send(kv_ref, group, sp, dest, 1)
            if s and k == 0:
                kv_send(kv_ref, target(s), sp, dest, 2)

    slot = lax.broadcasted_iota(jnp.int32, (8, tok_dev), 0)
    place = lax.broadcasted_iota(jnp.int32, (8, lanes), 1) - HEAD_DIM
    place = (place == lax.broadcasted_iota(jnp.int32, (8, lanes), 0)).astype(f32).astype(bf16)

    def spread(rows):
        return lax.dot_general(
            rows.astype(bf16), place, (((0,), (0,)), ((), ())), preferred_element_type=f32
        )

    def build(block):
        at = pl.ds(pl.multiple_of(block * tok_dev, tok_dev), tok_dev)
        gate = gate_ref[pl.ds(group, 1), at] * EXP2_SCALE
        for_k = (slot < 3).astype(f32)
        for_q = ((slot >= 3) & (slot < 6)).astype(f32)
        for i in range(3):
            piece = gate.astype(bf16).astype(f32)
            gate = gate - piece
            for_k = jnp.where(slot == 3 + i, -piece, for_k)
            for_q = jnp.where(slot == i, piece, for_q)
        side_ref[...] = spread(for_q)
        lane = lax.broadcasted_iota(jnp.int32, (tok_dev, lanes), 1)
        kv = kv_all[block].astype(f32)
        k_aug[block, :, :lanes] = jnp.where(lane < HEAD_DIM, kv, spread(for_k)).astype(bf16)
        k_aug[block, :, lanes:] = jnp.where(lane < HEAD_DIM, kv, 0.0).astype(bf16)
        turned = kv.T
        v_turned[block, :HEAD_DIM] = turned[HEAD_DIM:].astype(bf16)
        v_turned[block, HEAD_DIM:] = jnp.ones((16, tok_dev), bf16)
        packed = q_all[block]
        queries = jnp.concatenate((packed[:, :HEAD_DIM], packed[:, HEAD_DIM:]), axis=0)
        queries = queries.astype(f32) * (HEAD_DIM**-0.5 * EXP2_SCALE)
        high = queries.astype(bf16)
        low = (queries - high.astype(f32)).astype(bf16)
        for t in range(n_tp):
            rows = pl.ds(t * sub, sub)
            side = side_ref[pl.ds(pl.multiple_of(t * rows_dev + rank * sub, sub), sub), HEAD_DIM:]
            q_aug[block, rows, :lanes] = jnp.concatenate(
                (high[t * sub : (t + 1) * sub], side.astype(bf16)), axis=1
            )
        q_aug[block, :, lanes:] = jnp.concatenate((low, jnp.zeros_like(low)), axis=1)
        peak_ref[block] = jnp.full((1, chunk), MASKED, f32)
        acc_ref[block] = jnp.zeros((HEAD_DIM + 16, chunk), f32)

    halves = 2 if chunk >= 512 else 1
    half_rows = chunk // halves
    scores = (scores_a, scores_b)[:halves]

    def score(h, i, j):
        found = lax.dot_general(
            k_aug[j], q_aug[i, pl.ds(h * half_rows, half_rows)], (((1,), (1,)), ((), ())),
            preferred_element_type=f32,
        )
        scores[h][...] = found
        return jnp.max(found, axis=0, keepdims=True)

    def weigh(h, top, i, j, masked):
        rows = pl.ds(h * half_rows, half_rows)
        count = tok_dev // halves * (h + 1) if masked else tok_dev
        found = scores[h][:count]
        if masked:
            key = lax.broadcasted_iota(jnp.int32, (count, 1), 0)
            row = lax.broadcasted_iota(jnp.int32, (1, half_rows), 1) + h * half_rows
            pos = row // sub * rows_dev + rank * sub + lax.rem(row, sub)
            found = jnp.where(key <= pos, found, MASKED)
            top = jnp.max(found, axis=0, keepdims=True)
        before = peak_ref[i, :, rows]
        peak = jnp.maximum(before, top)
        probs = jnp.exp2(found - peak).astype(bf16)
        peak_ref[i, :, rows] = peak
        acc_ref[i, :, rows] = acc_ref[i, :, rows] * jnp.exp2(before - peak) + jnp.dot(
            v_turned[j, :, :count], probs, preferred_element_type=f32
        )

    def step(i, j, i_next, j_next, top, masked):
        for h in range(halves):
            ahead = (h + 1, i, j) if h + 1 < halves else (0, i_next, j_next)
            early = halves > 1 and not (masked and h + 1 == halves)
            if early:
                found = score(*ahead)
            weigh(h, top, i, j, masked)
            if not early and not masked:
                found = score(*ahead)
            top = found if early or not masked else top
        return top

    def head_copy(block, t):
        slot = block * n_tp + t
        return pltpu.make_async_remote_copy(
            src_ref=out_ref.at[slot], dst_ref=heads_ref.at[me],
            send_sem=send_sem.at[4], recv_sem=head_sem,
            device_id=(block, t), device_id_type=MESH,
        )

    own_head = pltpu.make_async_copy(out_ref.at[me], heads_ref.at[me], own_sem)

    def finish(block):
        acc = acc_ref[block]
        out = (acc[:HEAD_DIM] / acc[HEAD_DIM : HEAD_DIM + 1]).T
        half = sub // 2
        for t in range(n_tp):
            top, low = (out[t * sub + at : t * sub + at + half] for at in (0, half))
            out_ref[block * n_tp + t] = jnp.concatenate((top, low), axis=1).astype(jnp.bfloat16)
        for t in range(n_tp):
            mine = (block == sp) & (tp == t)

            @pl.when(mine)
            def _():
                own_head.start()

            @pl.when(jnp.logical_not(mine))
            def _(t=t):
                head_copy(block, t).start()

    def relay(i):
        block = block_at(i)
        for part in range(KV_PARTS):
            kv_copies(kv_all, block, block, block, 3)[part].wait_recv()
            for k in range(1, shares):
                dest = group * shares + lax.rem(rank + k, shares)
                kv_copies(kv_all, block, block, dest, 3)[part].start()

    def one_block(i, carry):
        block = block_at(i)
        s, k = i // shares, lax.rem(i, shares)
        turn = (k == shares - 1) & (s < groups - 1)
        outer = (group == 0) | (group == groups - 1)
        early = (s > 0) & jnp.where(outer, s < groups - 2, s == groups - 2)

        @pl.when(turn & early)
        def _():
            relay(i + 1)

        @pl.when(i > 0)
        def _():
            q_copy(q_all.at[block], block, block).wait_recv()

        @pl.when(k > 0)
        def _():
            for copy in kv_copies(kv_all, block, block, block, 3):
                copy.wait_recv()

        build(block)

        def blocks(m):
            other = jnp.where(m < i, block_at(jnp.maximum(i - 1 - m, 0)), block)
            return jnp.maximum(block, other), jnp.minimum(block, other)

        def pair(m, top):
            other = block_at(i - 1 - m)
            top = step(*blocks(m), *blocks(m + 1), top, False)

            @pl.when(i == n_sp - 1)
            def _():
                finish(other)

            return top

        top = lax.fori_loop(0, i, pair, score(0, *blocks(0)))
        step(block, block, block, block, top, True)

        @pl.when(turn & jnp.logical_not(early))
        def _():
            relay(i + 1)

        return carry

    lax.fori_loop(0, n_sp, one_block, 0)
    finish(block_at(n_sp - 1))
    own_head.wait()

    def sent(buf, count, slot):
        if count:
            pltpu.make_async_remote_copy(
                src_ref=buf.at[pl.ds(0, count)], dst_ref=buf.at[pl.ds(0, count)],
                send_sem=send_sem.at[slot], recv_sem=head_sem,
                device_id=(sp, tp), device_id_type=MESH,
            ).wait_send()

    pltpu.make_async_remote_copy(
        src_ref=heads_ref.at[pl.ds(0, n - 1)], dst_ref=heads_ref.at[pl.ds(0, n - 1)],
        send_sem=send_sem.at[4], recv_sem=head_sem,
        device_id=(sp, tp), device_id_type=MESH,
    ).wait_recv()
    half = sub // 2
    for t in range(n_tp):
        for h in range(0, local_heads, 2):
            for r in range(shares):
                left = heads_ref[(h * shares + r) * n_tp + t]
                right = heads_ref[((h + 1) * shares + r) * n_tp + t]
                for part in range(2):
                    cols = slice(part * HEAD_DIM, (part + 1) * HEAD_DIM)
                    o_ref[
                        pl.ds((2 * r + part) * half, half),
                        pl.ds((t * local_heads + h) * HEAD_DIM, 2 * HEAD_DIM),
                    ] = jnp.concatenate((left[:, cols], right[:, cols]), axis=1)
    sent(q_ref, n_sp - 1, 0)
    sent(kv_all, shares - 1, 1)
    sent(kv_all, groups - 1, 2)
    sent(kv_all, (groups - 1) * (shares - 1), 3)
    sent(out_ref, n - 1, 4)


def attend(queries, key_rows, value_rows, gate, n_sp, n_tp):
    tok_dev, width = queries.shape
    local_heads = width // HEAD_DIM
    lanes = 2 * HEAD_DIM
    shares = n_sp // local_heads
    rows_dev = tok_dev // n_tp
    sub = rows_dev // shares
    chunk = n_tp * sub
    n = n_sp * n_tp
    bf16, f32 = jnp.bfloat16, jnp.float32
    vmem = pl.BlockSpec(memory_space=pltpu.VMEM)
    hbm = pl.BlockSpec(memory_space=pl.ANY)
    return pl.pallas_call(
        functools.partial(attend_kernel, n_tp=n_tp, local_heads=local_heads),
        out_shape=jax.ShapeDtypeStruct((rows_dev, n_tp * width), bf16),
        in_specs=[hbm] * 3 + [vmem],
        out_specs=vmem,
        scratch_shapes=[pltpu.VMEM((tok_dev, width), bf16)] * 3
        + [
            pltpu.VMEM((local_heads, tok_dev, lanes), bf16),
            pltpu.VMEM((n_sp, chunk // 2, lanes), bf16),
            pltpu.VMEM((n_sp, tok_dev, lanes), bf16),
            pltpu.VMEM((n_sp, chunk // 2, lanes), bf16),
            pltpu.VMEM((n_sp, tok_dev, 2 * lanes), bf16),
            pltpu.VMEM((n_sp, HEAD_DIM + 16, tok_dev), bf16),
            pltpu.VMEM((n_sp, chunk, 2 * lanes), bf16),
            pltpu.VMEM((tok_dev, lanes), f32),
            pltpu.VMEM((n_sp, 1, chunk), f32),
            pltpu.VMEM((n_sp, HEAD_DIM + 16, chunk), f32),
            pltpu.VMEM((tok_dev, chunk // 2 if chunk >= 512 else chunk), f32),
            pltpu.VMEM((tok_dev, chunk // 2 if chunk >= 512 else chunk), f32),
            pltpu.VMEM((n, sub // 2, lanes), bf16),
            pltpu.VMEM((n, sub // 2, lanes), bf16),
            pltpu.SemaphoreType.DMA((3,)),
            pltpu.SemaphoreType.DMA,
            pltpu.SemaphoreType.DMA((n_sp,)),
            pltpu.SemaphoreType.DMA((n_sp, KV_PARTS)),
            pltpu.SemaphoreType.DMA,
            pltpu.SemaphoreType.DMA((5,)),
        ],
        compiler_params=pltpu.CompilerParams(
            collective_id=0, has_side_effects=True, vmem_limit_bytes=60 * 2**20
        ),
        name="attend",
    )(queries, key_rows, value_rows, gate)


def expert_kernel(
    heads_ref, ow_hbm, res_hbm, mix_ref, pre_ref, post_ref, ids_ref, weight_ref, wg_hbm, wu_hbm, wd_hbm, o_ref,
    ow_ref, res_ref, sent, arrived, made, returned, wg, wu, wd, gate_acc, up_acc, hidden, comb, stream, normed, weigh,
    w_sem, own_sem, send_sem, recv_sem, *, n_tp, chunks, tight,
):
    n, cap, width = sent.shape
    rows_dev = stream.shape[0]
    part = width // chunks
    last = chunks - 1
    fold = chunks == 4 and cap - tight == 2 and tight > 8
    keep = cap - 8
    group = n // GROUPS
    rows = group * cap
    f32, bf16 = jnp.float32, jnp.bfloat16
    sp, tp = lax.axis_index("sp"), lax.axis_index("tp")
    me = sp * n_tp + tp

    def peer(o):
        d = lax.rem(me + o, n)
        return d, (d // n_tp, lax.rem(d, n_tp))

    firsts = [
        pltpu.make_async_copy(
            ow_hbm.at[:, pl.ds(c * part, part)], ow_ref.at[:, pl.ds(c * part, part)], w_sem.at[4 + c]
        )
        for c in range(chunks)
    ]
    loads = [
        pltpu.make_async_copy(src, dst, w_sem.at[i])
        for i, (src, dst) in enumerate(
            ((wg_hbm, wg), (wu_hbm, wu), (wd_hbm, wd), (res_hbm, res_ref))
        )
    ]
    for load in (*firsts, loads[3], *loads[:3]):
        load.start()

    barrier = pltpu.get_barrier_semaphore()

    def greet(o, carry):
        pl.semaphore_signal(barrier, inc=1, device_id=peer(o)[1], device_id_type=MESH)
        return carry

    lax.fori_loop(1, n, greet, 0)

    def cols(c):
        return pl.ds(c * part, part)

    expert = lax.broadcasted_iota(jnp.int32, (n, rows_dev), 0)
    tri = (
        lax.broadcasted_iota(jnp.int32, (rows_dev, rows_dev), 0)
        < lax.broadcasted_iota(jnp.int32, (rows_dev, rows_dev), 1)
    ).astype(f32).astype(bf16)
    taken = jnp.zeros((n, 1), f32)
    slots = []
    for k in range(ids_ref.shape[0]):
        ids = ids_ref[pl.ds(k, 1), :]
        named = (expert == ids).astype(f32)
        ahead = jnp.dot(named.astype(bf16), tri, preferred_element_type=f32) + taken
        rank = jnp.sum(named * ahead, axis=0, keepdims=True)
        taken = taken + jnp.sum(named, axis=1, keepdims=True)
        slots.append(ids * cap + rank.astype(jnp.int32))

    heads = heads_ref[...]
    total = jnp.zeros((rows_dev, 1), f32)
    for c in range(chunks):
        firsts[c].wait()
        proj = jnp.dot(heads, ow_ref[:, cols(c)], preferred_element_type=f32)
        comb[:, cols(c)] = proj
        total = total + jnp.sum(proj * proj, axis=1, keepdims=True)
    scale = lax.rsqrt(total / width + NORM_EPS)
    total = jnp.zeros((rows_dev, 1), f32)
    loads[3].wait()
    for c in range(chunks):
        wide = res_ref[:, cols(c)].astype(f32) + comb[:, cols(c)] * scale * mix_ref[:, cols(c)]
        stream[:, cols(c)] = wide.astype(bf16)
        wide = stream[:, cols(c)].astype(f32)
        total = total + jnp.sum(wide * wide, axis=1, keepdims=True)
    scale = lax.rsqrt(total / width + NORM_EPS)
    for c in range(chunks):
        wide = stream[:, cols(c)].astype(f32)
        normed[:, cols(c)] = (wide * scale * pre_ref[:, cols(c)]).astype(bf16)
    pl.semaphore_wait(barrier, n - 1)

    def window(ref, at, c):
        if fold and c == last:
            return ref.at[at, pl.ds(0, keep), cols(c)]
        return ref.at[at, :, cols(c)]

    def send_all(src, dst, c, slot):
        def one(o, carry):
            d, where = peer(o)
            pltpu.make_async_remote_copy(
                src_ref=window(src, d, c),
                dst_ref=window(dst, me, c),
                send_sem=send_sem.at[slot],
                recv_sem=recv_sem.at[slot],
                device_id=where,
                device_id_type=MESH,
            ).start()
            return carry

        pltpu.make_async_copy(window(src, me, c), window(dst, me, c), own_sem.at[slot]).start()
        lax.fori_loop(1, n, one, 0)

    def all_copies(src, dst, c, slot):
        return pltpu.make_async_remote_copy(
            src_ref=window(src, pl.ds(0, n - 1), c),
            dst_ref=window(dst, pl.ds(0, n - 1), c),
            send_sem=send_sem.at[slot],
            recv_sem=recv_sem.at[slot],
            device_id=peer(1)[1],
            device_id_type=MESH,
        )

    def wait_all(src, dst, c, slot):
        pltpu.make_async_copy(window(src, me, c), window(dst, me, c), own_sem.at[slot]).wait()
        all_copies(src, dst, c, slot).wait_recv()

    spare = lax.broadcasted_iota(jnp.int32, (group, 8, part), 1)

    def unfold(ref):
        def one(g, carry):
            at = pl.ds(g * group, group)
            new = jnp.zeros((group, 8, part), f32)
            for c in range(last):
                tail = ref[at, keep:cap, cols(c)].astype(f32)
                new = jnp.where(spare == c, tail[:, 6:7], new)
                new = jnp.where(spare == last + c, tail[:, 7:8], new)
            ref[at, keep:cap, cols(last)] = new.astype(bf16)
            return carry

        lax.fori_loop(0, GROUPS, one, 0)

    for c in range(chunks):

        def gather(g, carry, c=c):
            row = g * rows + lax.broadcasted_iota(jnp.int32, (rows, rows_dev), 0)

            def named(target):
                return sum((target == slot).astype(f32) for slot in slots).astype(bf16)

            y = jnp.dot(named(row), normed[:, cols(c)], preferred_element_type=f32)
            if fold and c < last:
                at = lax.rem(row, cap)
                aim = jnp.where(at == tight, row - 6 + c, jnp.where(at == tight + 1, row - 4 + c, -1))
                y = y + jnp.dot(named(aim), normed[:, cols(last)], preferred_element_type=f32)
            sent[pl.ds(g * group, group), :, cols(c)] = y.astype(bf16).reshape(group, cap, part)
            return carry

        lax.fori_loop(0, GROUPS, gather, 0)
        send_all(sent, arrived, c, c)

    def weights(g, carry):
        at = pl.ds(pl.multiple_of(g * WEIGH_COLS, WEIGH_COLS), WEIGH_COLS)
        row = g * WEIGH_COLS + lax.broadcasted_iota(jnp.int32, (WEIGH_COLS, rows_dev), 0)
        mix = sum(
            jnp.where(row == slot, weight_ref[pl.ds(k, 1), :], 0.0) for k, slot in enumerate(slots)
        ).T
        for i in range(weigh.shape[0]):
            piece = mix.astype(bf16)
            weigh[i, :, at] = piece
            mix = mix - piece.astype(f32)
        return carry

    lax.fori_loop(0, n * cap // WEIGH_COLS, weights, 0)
    for load in loads[:2]:
        load.wait()

    for c in range(chunks):
        wait_all(sent, arrived, c, c)

        def gate_up(g, carry, c=c):
            x = arrived[pl.ds(g * group, group), :, cols(c)].reshape(rows, part)
            at = pl.ds(pl.multiple_of(g * rows, rows), rows)
            gate = jnp.dot(x, wg[cols(c), :], preferred_element_type=f32)
            up = jnp.dot(x, wu[cols(c), :], preferred_element_type=f32)
            if c > 0:
                gate, up = gate + gate_acc[at, :], up + up_acc[at, :]
            if c < last:
                gate_acc[at, :] = gate
                up_acc[at, :] = up
            else:
                hidden[at, :] = (jax.nn.silu(gate) * up).astype(bf16)
            return carry

        lax.fori_loop(0, GROUPS, gate_up, 0)
        if fold and c == last - 1:
            unfold(arrived)
    loads[2].wait()
    order = (last, *range(last))
    for c in order:

        def down(g, carry, c=c):
            at = pl.ds(pl.multiple_of(g * rows, rows), rows)
            some = pl.ds(g * group, group)
            y = jnp.dot(hidden[at, :], wd[:, cols(c)], preferred_element_type=f32)
            made[some, :, cols(c)] = y.astype(bf16).reshape(group, cap, part)
            if fold and c < last:
                tail = made[some, keep:cap, cols(c)].astype(f32)
                other = made[some, keep:cap, cols(last)].astype(f32)
                tail = jnp.where(spare == 6, other[:, c : c + 1], tail)
                tail = jnp.where(spare == 7, other[:, last + c : last + c + 1], tail)
                made[some, keep:cap, cols(c)] = tail.astype(bf16)
            return carry

        lax.fori_loop(0, GROUPS, down, 0)
        send_all(made, returned, c, chunks + c)
    total = jnp.zeros((rows_dev, 1), f32)

    def combine(c, total):
        back = returned[:, :, cols(c)].reshape(n * cap, part)
        mixed = sum(
            jnp.dot(weigh[i], back, preferred_element_type=f32) for i in range(weigh.shape[0])
        )
        comb[:, cols(c)] = mixed
        return total + jnp.sum(mixed * mixed, axis=1, keepdims=True)

    for c in order:
        wait_all(made, returned, c, chunks + c)
        if not (fold and c == last):
            total = combine(c, total)
    if fold:
        unfold(returned)
        total = combine(last, total)
    scale = lax.rsqrt(total / width + NORM_EPS)
    for c in range(chunks):
        o_ref[:, cols(c)] = (
            stream[:, cols(c)].astype(f32) + comb[:, cols(c)] * scale * post_ref[:, cols(c)]
        ).astype(bf16)
    for c in range(chunks):
        all_copies(sent, arrived, c, c).wait_send()
        all_copies(made, returned, c, chunks + c).wait_send()


def experts(heads, out_weight, residual, gain_mix, gain_pre, gain_post, ids, weight, w_gate, w_up, w_down, n, n_tp, tight):
    rows_dev, width = residual.shape
    cap = (tight + 7) // 8 * 8
    hidden = w_gate.shape[1]
    slots = n * cap
    chunks = CHUNKS
    vmem = pl.BlockSpec(memory_space=pltpu.VMEM)
    hbm = pl.BlockSpec(memory_space=pl.ANY)
    bf16, f32 = jnp.bfloat16, jnp.float32
    return pl.pallas_call(
        functools.partial(expert_kernel, n_tp=n_tp, chunks=chunks, tight=tight),
        out_shape=jax.ShapeDtypeStruct(residual.shape, bf16),
        in_specs=[vmem] + [hbm] * 2 + [vmem] * 5 + [hbm] * 3,
        out_specs=vmem,
        scratch_shapes=[
            pltpu.VMEM(out_weight.shape, bf16),
            pltpu.VMEM(residual.shape, bf16),
            pltpu.VMEM((n, cap, width), bf16),
            pltpu.VMEM((n, cap, width), bf16),
            pltpu.VMEM((n, cap, width), bf16),
            pltpu.VMEM((n, cap, width), bf16),
            pltpu.VMEM(w_gate.shape, bf16),
            pltpu.VMEM(w_up.shape, bf16),
            pltpu.VMEM(w_down.shape, bf16),
            pltpu.VMEM((slots, hidden), f32),
            pltpu.VMEM((slots, hidden), f32),
            pltpu.VMEM((slots, hidden), bf16),
            pltpu.VMEM(residual.shape, f32),
            pltpu.VMEM(residual.shape, bf16),
            pltpu.VMEM(residual.shape, bf16),
            pltpu.VMEM((2, rows_dev, slots), bf16),
            pltpu.SemaphoreType.DMA((4 + chunks,)),
            pltpu.SemaphoreType.DMA((2 * chunks,)),
            pltpu.SemaphoreType.DMA((2 * chunks,)),
            pltpu.SemaphoreType.DMA((2 * chunks,)),
        ],
        compiler_params=pltpu.CompilerParams(
            collective_id=1, has_side_effects=True, vmem_limit_bytes=56 * 2**20
        ),
        name="experts",
    )(heads, out_weight, residual, gain_mix, gain_pre, gain_post, ids, weight, w_gate, w_up, w_down)


def local(
    queries,
    key_rows,
    value_rows,
    cum_gate,
    residual,
    out_weight,
    gain_mix,
    gain_pre,
    gain_post,
    route_ids,
    route_weight,
    w_gate,
    w_up,
    w_down,
):
    n_sp, n_tp = lax.axis_size("sp"), lax.axis_size("tp")
    rows_dev = residual.shape[0]
    head_rows = attend(queries, key_rows, value_rows, cum_gate, n_sp, n_tp)
    top_count = route_ids.shape[1]
    experts_all = n_sp * n_tp
    tight = max(2, (4 * rows_dev * top_count + 3 * experts_all - 1) // (3 * experts_all))
    return experts(
        head_rows, out_weight, residual, gain_mix[None], gain_pre[None], gain_post[None],
        route_ids.T, route_weight.T, w_gate[0], w_up[0], w_down[0], experts_all, n_tp, tight,
    )


def solution(mesh):
    return jax.shard_map(
        local,
        mesh=mesh,
        in_specs=(
            P("sp", "tp"),
            P("sp", "tp"),
            P("sp", "tp"),
            P("tp", None),
            P(("sp", "tp"), None),
            P(),
            P(),
            P(),
            P(),
            P(("sp", "tp"), None),
            P(("sp", "tp"), None),
            P(("sp", "tp"), None, None),
            P(("sp", "tp"), None, None),
            P(("sp", "tp"), None, None),
        ),
        out_specs=P(("sp", "tp"), None),
        check_vma=False,
    )
```

```python
import functools
import math

import jax
import jax.numpy as jnp
from jax import lax
from jax.experimental import pallas as pl
from jax.experimental.pallas import tpu as pltpu
from jax.sharding import PartitionSpec as P

HEAD_DIM = 64
NORM_EPS = 1e-06
MASKED = -1e30
MESH = pl.DeviceIdType.MESH
CHUNKS = 4
GROUPS = 4
EXP2_SCALE = math.log2(math.e)
WEIGH_COLS = 256
KV_PARTS = 2


def attend_kernel(
    q_hbm, k_hbm, v_hbm, gate_ref, o_ref,
    q_in, k_in, v_in, kv_ref, q_ref,
    kv_all, q_all, k_aug, v_turned, q_aug, side_ref, out_ref, heads_ref,
    in_sem, own_sem, q_sem, kv_sem, head_sem, send_sem, *halved, n_tp, local_heads,
):
    halves = len(halved) // 3
    peaks, accs, scores = (halved[i * halves : (i + 1) * halves] for i in range(3))
    groups = local_heads
    n_sp = q_ref.shape[0]
    shares = n_sp // groups
    tok_dev = kv_ref.shape[1]
    f32, bf16 = jnp.float32, jnp.bfloat16
    chunk = 2 * q_ref.shape[1]
    sub = chunk // n_tp
    rows_dev = sub * shares
    half_rows = chunk // halves
    lanes = 2 * HEAD_DIM
    n = n_sp * n_tp
    sp, tp = lax.axis_index("sp"), lax.axis_index("tp")
    me = sp * n_tp + tp
    group, rank = sp // shares, lax.rem(sp, shares)

    def plane(s):
        down = jnp.where(s <= group, group - s, s)
        up = jnp.where(s <= groups - 1 - group, group + s, groups - 1 - s)
        return jnp.where(2 * group < groups, down, up)

    def target(s):
        down = jnp.where(group > 0, groups + group - s, s)
        down = jnp.where(s <= group, group - s, down)
        up = jnp.where(group < groups - 1, s - groups + group, groups - 1 - s)
        up = jnp.where(s <= groups - 1 - group, group + s, up)
        return jnp.where(2 * group < groups, down, up)

    def block_at(i):
        return plane(i // shares) * shares + lax.rem(rank + lax.rem(i, shares), shares)

    loads = [
        pltpu.make_async_copy(src, dst, in_sem.at[i])
        for i, (src, dst) in enumerate(((q_hbm, q_in), (k_hbm, k_in), (v_hbm, v_in)))
    ]
    for load in loads:
        load.start()
    barrier = pltpu.get_barrier_semaphore()

    def greet(o, carry):
        d = lax.rem(me + o, n)
        where = (d // n_tp, lax.rem(d, n_tp))
        pl.semaphore_signal(barrier, inc=1, device_id=where, device_id_type=MESH)
        return carry

    lax.fori_loop(1, n, greet, 0)
    for load in loads:
        load.wait()
    for h in range(groups):
        head = pl.ds(h * HEAD_DIM, HEAD_DIM)
        kv_ref[h] = jnp.concatenate((k_in[:, head], v_in[:, head]), axis=1)
        for r in range(shares):
            for t in range(n_tp // 2):
                low, high = (
                    q_in[pl.ds((t + half) * rows_dev + r * sub, sub), head]
                    for half in (0, n_tp // 2)
                )
                q_ref[h * shares + r, pl.ds(t * sub, sub)] = jnp.concatenate((low, high), axis=1)
    kv_all[sp] = kv_ref[group]
    q_all[sp] = q_ref[sp]
    pl.semaphore_wait(barrier, n - 1)

    def kv_copies(src, index, block, dest, slot):
        size = tok_dev // KV_PARTS
        return [
            pltpu.make_async_remote_copy(
                src_ref=src.at[index, pl.ds(part * size, size)],
                dst_ref=kv_all.at[block, pl.ds(part * size, size)],
                send_sem=send_sem.at[slot], recv_sem=kv_sem.at[block, part],
                device_id=(dest, tp), device_id_type=MESH,
            )
            for part in range(KV_PARTS)
        ]

    def kv_send(*where):
        for copy in kv_copies(*where):
            copy.start()

    def q_copy(src, block, dest):
        return pltpu.make_async_remote_copy(
            src_ref=src, dst_ref=q_all.at[block],
            send_sem=send_sem.at[0], recv_sem=q_sem.at[block],
            device_id=(dest, tp), device_id_type=MESH,
        )

    for s in range(groups):
        for k in range(shares):
            dest = block_at(k) if s == 0 else target(s) * shares + lax.rem(rank + k, shares)
            if s or k:
                q_copy(q_ref.at[dest], sp, dest).start()
            if s == 0 and k:
                kv_send(kv_ref, group, sp, dest, 1)
            if s and k == 0:
                kv_send(kv_ref, target(s), sp, dest, 2)

    slot = lax.broadcasted_iota(jnp.int32, (8, tok_dev), 0)
    place = lax.broadcasted_iota(jnp.int32, (8, lanes), 1) - HEAD_DIM
    place = (place == lax.broadcasted_iota(jnp.int32, (8, lanes), 0)).astype(f32).astype(bf16)

    def spread(rows):
        return lax.dot_general(
            rows.astype(bf16), place, (((0,), (0,)), ((), ())), preferred_element_type=f32
        )

    def sides(block):
        at = pl.ds(pl.multiple_of(block * tok_dev, tok_dev), tok_dev)
        gate = gate_ref[pl.ds(group, 1), at] * EXP2_SCALE
        for_k = (slot < 3).astype(f32)
        for_q = ((slot >= 3) & (slot < 6)).astype(f32)
        for i in range(3):
            piece = gate.astype(bf16).astype(f32)
            gate = gate - piece
            for_k = jnp.where(slot == 3 + i, -piece, for_k)
            for_q = jnp.where(slot == i, piece, for_q)
        side_ref[...] = spread(for_q)
        k_aug[block, :, :lanes] = spread(for_k).astype(bf16)
        for t in range(n_tp):
            rows = pl.ds(t * sub, sub)
            side = side_ref[pl.ds(pl.multiple_of(t * rows_dev + rank * sub, sub), sub)]
            q_aug[block, rows, :lanes] = side.astype(bf16)
        for h in range(halves):
            peaks[h][block] = jnp.full((1, half_rows), MASKED, f32)
            accs[h][block] = jnp.zeros((HEAD_DIM + 16, half_rows), f32)

    def build(block):
        lane = lax.broadcasted_iota(jnp.int32, (tok_dev, lanes), 1)
        kv = kv_all[block].astype(f32)
        k_aug[block, :, :lanes] = jnp.where(
            lane < HEAD_DIM, kv, k_aug[block, :, :lanes].astype(f32)
        ).astype(bf16)
        k_aug[block, :, lanes:] = jnp.where(lane < HEAD_DIM, kv, 0.0).astype(bf16)
        turned = kv.T
        v_turned[block, :HEAD_DIM] = turned[HEAD_DIM:].astype(bf16)
        v_turned[block, HEAD_DIM:] = jnp.ones((16, tok_dev), bf16)
        packed = q_all[block]
        queries = jnp.concatenate((packed[:, :HEAD_DIM], packed[:, HEAD_DIM:]), axis=0)
        queries = queries.astype(f32) * (HEAD_DIM**-0.5 * EXP2_SCALE)
        high = queries.astype(bf16)
        low = (queries - high.astype(f32)).astype(bf16)
        q_aug[block, :, :lanes] = jnp.concatenate((high, q_aug[block, :, HEAD_DIM:lanes]), axis=1)
        q_aug[block, :, lanes:] = jnp.concatenate((low, jnp.zeros_like(low)), axis=1)

    def score(h, i, j):
        found = lax.dot_general(
            k_aug[j], q_aug[i, pl.ds(h * half_rows, half_rows)], (((1,), (1,)), ((), ())),
            preferred_element_type=f32,
        )
        scores[h][...] = found
        return jnp.max(found, axis=0, keepdims=True)

    def weigh(h, top, i, j, masked):
        count = tok_dev // halves * (h + 1) if masked else tok_dev
        found = scores[h][:count]
        if masked:
            key = lax.broadcasted_iota(jnp.int32, (count, 1), 0)
            row = lax.broadcasted_iota(jnp.int32, (1, half_rows), 1) + h * half_rows
            pos = row // sub * rows_dev + rank * sub + lax.rem(row, sub)
            found = jnp.where(key <= pos, found, MASKED)
            top = jnp.max(found, axis=0, keepdims=True)
        before = peaks[h][i]
        peak = jnp.maximum(before, top)
        probs = jnp.exp2(found - peak).astype(bf16)
        peaks[h][i] = peak
        accs[h][i] = accs[h][i] * jnp.exp2(before - peak) + jnp.dot(
            v_turned[j, :, :count], probs, preferred_element_type=f32
        )

    def step(i, j, i_next, j_next, top, masked):
        for h in range(halves):
            ahead = (h + 1, i, j) if h + 1 < halves else (0, i_next, j_next)
            early = h + 1 < halves
            if early:
                found = score(*ahead)
            weigh(h, top, i, j, masked)
            if not early and not masked:
                found = score(*ahead)
            top = found if early or not masked else top
        return top

    def head_copy(block, t):
        slot = block * n_tp + t
        return pltpu.make_async_remote_copy(
            src_ref=out_ref.at[slot], dst_ref=heads_ref.at[me],
            send_sem=send_sem.at[4], recv_sem=head_sem,
            device_id=(block, t), device_id_type=MESH,
        )

    own_head = pltpu.make_async_copy(out_ref.at[me], heads_ref.at[me], own_sem)

    def finish(block):
        parts = [accs[h][block] for h in range(halves)]
        parts = [(acc[:HEAD_DIM] / acc[HEAD_DIM : HEAD_DIM + 1]).T for acc in parts]
        out = jnp.concatenate(parts, axis=0)
        half = sub // 2
        for t in range(n_tp):
            top, low = (out[t * sub + at : t * sub + at + half] for at in (0, half))
            out_ref[block * n_tp + t] = jnp.concatenate((top, low), axis=1).astype(jnp.bfloat16)
        for t in range(n_tp):
            mine = (block == sp) & (tp == t)

            @pl.when(mine)
            def _():
                own_head.start()

            @pl.when(jnp.logical_not(mine))
            def _(t=t):
                head_copy(block, t).start()

    def relay(i):
        block = block_at(i)
        for part in range(KV_PARTS):
            kv_copies(kv_all, block, block, block, 3)[part].wait_recv()
            for k in range(1, shares):
                dest = group * shares + lax.rem(rank + k, shares)
                kv_copies(kv_all, block, block, dest, 3)[part].start()

    def one_block(i, carry):
        block = block_at(i)
        s, k = i // shares, lax.rem(i, shares)
        turn = (k == shares - 1) & (s < groups - 1)
        outer = (group == 0) | (group == groups - 1)
        early = (s > 0) & jnp.where(outer, s < groups - 2, s == groups - 2)

        @pl.when(turn & early)
        def _():
            relay(i + 1)

        @pl.when(i > 0)
        def _():
            q_copy(q_all.at[block], block, block).wait_recv()

        @pl.when(k > 0)
        def _():
            for copy in kv_copies(kv_all, block, block, block, 3):
                copy.wait_recv()

        build(block)

        def blocks(m):
            other = jnp.where(m < i, block_at(jnp.maximum(i - 1 - m, 0)), block)
            return jnp.maximum(block, other), jnp.minimum(block, other)

        def pair(m, top):
            other = block_at(i - 1 - m)
            top = step(*blocks(m), *blocks(m + 1), top, False)

            @pl.when(i == n_sp - 1)
            def _():
                finish(other)

            return top

        top = lax.fori_loop(0, i, pair, score(0, *blocks(0)))
        step(block, block, block, block, top, True)

        @pl.when(turn & jnp.logical_not(early))
        def _():
            relay(i + 1)

        return carry

    def one_side(i, carry):
        sides(block_at(i))
        return carry

    sides(sp)
    one_block(0, 0)
    lax.fori_loop(1, n_sp, one_side, 0)
    lax.fori_loop(1, n_sp, one_block, 0)
    finish(block_at(n_sp - 1))
    own_head.wait()

    def sent(buf, count, slot):
        if count:
            pltpu.make_async_remote_copy(
                src_ref=buf.at[pl.ds(0, count)], dst_ref=buf.at[pl.ds(0, count)],
                send_sem=send_sem.at[slot], recv_sem=head_sem,
                device_id=(sp, tp), device_id_type=MESH,
            ).wait_send()

    pltpu.make_async_remote_copy(
        src_ref=heads_ref.at[pl.ds(0, n - 1)], dst_ref=heads_ref.at[pl.ds(0, n - 1)],
        send_sem=send_sem.at[4], recv_sem=head_sem,
        device_id=(sp, tp), device_id_type=MESH,
    ).wait_recv()
    half = sub // 2
    for t in range(n_tp):
        for h in range(0, local_heads, 2):
            for r in range(shares):
                left = heads_ref[(h * shares + r) * n_tp + t]
                right = heads_ref[((h + 1) * shares + r) * n_tp + t]
                for part in range(2):
                    cols = slice(part * HEAD_DIM, (part + 1) * HEAD_DIM)
                    o_ref[
                        pl.ds((2 * r + part) * half, half),
                        pl.ds((t * local_heads + h) * HEAD_DIM, 2 * HEAD_DIM),
                    ] = jnp.concatenate((left[:, cols], right[:, cols]), axis=1)
    sent(q_ref, n_sp - 1, 0)
    sent(kv_all, shares - 1, 1)
    sent(kv_all, groups - 1, 2)
    sent(kv_all, (groups - 1) * (shares - 1), 3)
    sent(out_ref, n - 1, 4)


def attend(queries, key_rows, value_rows, gate, n_sp, n_tp):
    tok_dev, width = queries.shape
    local_heads = width // HEAD_DIM
    lanes = 2 * HEAD_DIM
    shares = n_sp // local_heads
    rows_dev = tok_dev // n_tp
    sub = rows_dev // shares
    chunk = n_tp * sub
    n = n_sp * n_tp
    halves = 2 if chunk >= 512 else 1
    half_rows = chunk // halves
    bf16, f32 = jnp.bfloat16, jnp.float32
    vmem = pl.BlockSpec(memory_space=pltpu.VMEM)
    hbm = pl.BlockSpec(memory_space=pl.ANY)
    return pl.pallas_call(
        functools.partial(attend_kernel, n_tp=n_tp, local_heads=local_heads),
        out_shape=jax.ShapeDtypeStruct((rows_dev, n_tp * width), bf16),
        in_specs=[hbm] * 3 + [vmem],
        out_specs=vmem,
        scratch_shapes=[pltpu.VMEM((tok_dev, width), bf16)] * 3
        + [
            pltpu.VMEM((local_heads, tok_dev, lanes), bf16),
            pltpu.VMEM((n_sp, chunk // 2, lanes), bf16),
            pltpu.VMEM((n_sp, tok_dev, lanes), bf16),
            pltpu.VMEM((n_sp, chunk // 2, lanes), bf16),
            pltpu.VMEM((n_sp, tok_dev, 2 * lanes), bf16),
            pltpu.VMEM((n_sp, HEAD_DIM + 16, tok_dev), bf16),
            pltpu.VMEM((n_sp, chunk, 2 * lanes), bf16),
            pltpu.VMEM((tok_dev, lanes), f32),
            pltpu.VMEM((n, sub // 2, lanes), bf16),
            pltpu.VMEM((n, sub // 2, lanes), bf16),
            pltpu.SemaphoreType.DMA((3,)),
            pltpu.SemaphoreType.DMA,
            pltpu.SemaphoreType.DMA((n_sp,)),
            pltpu.SemaphoreType.DMA((n_sp, KV_PARTS)),
            pltpu.SemaphoreType.DMA,
            pltpu.SemaphoreType.DMA((5,)),
        ]
        + [pltpu.VMEM((n_sp, 1, half_rows), f32)] * halves
        + [pltpu.VMEM((n_sp, HEAD_DIM + 16, half_rows), f32)] * halves
        + [pltpu.VMEM((tok_dev, half_rows), f32)] * halves,
        compiler_params=pltpu.CompilerParams(
            collective_id=0, has_side_effects=True, vmem_limit_bytes=60 * 2**20
        ),
        name="attend",
    )(queries, key_rows, value_rows, gate)


def expert_kernel(
    heads_ref, ow_hbm, res_hbm, mix_ref, pre_ref, post_ref, ids_ref, weight_ref, wg_hbm, wu_hbm, wd_hbm, o_ref,
    ow_ref, res_ref, sent, arrived, made, returned, wg, wu, wd, gate_acc, up_acc, hidden, comb, stream, normed, weigh,
    w_sem, own_sem, send_sem, recv_sem, *, n_tp, chunks, tight,
):
    n, cap, width = sent.shape
    rows_dev = stream.shape[0]
    part = width // chunks
    last = chunks - 1
    fold = chunks == 4 and cap - tight == 2 and tight > 8
    keep = cap - 8
    group = n // GROUPS
    rows = group * cap
    f32, bf16 = jnp.float32, jnp.bfloat16
    sp, tp = lax.axis_index("sp"), lax.axis_index("tp")
    me = sp * n_tp + tp

    def peer(o):
        d = lax.rem(me + o, n)
        return d, (d // n_tp, lax.rem(d, n_tp))

    firsts = [
        pltpu.make_async_copy(
            ow_hbm.at[:, pl.ds(c * part, part)], ow_ref.at[:, pl.ds(c * part, part)], w_sem.at[4 + c]
        )
        for c in range(chunks)
    ]
    loads = [
        pltpu.make_async_copy(src, dst, w_sem.at[i])
        for i, (src, dst) in enumerate(
            ((wg_hbm, wg), (wu_hbm, wu), (wd_hbm, wd), (res_hbm, res_ref))
        )
    ]
    for load in (*firsts, loads[3], *loads[:3]):
        load.start()

    barrier = pltpu.get_barrier_semaphore()

    def greet(o, carry):
        pl.semaphore_signal(barrier, inc=1, device_id=peer(o)[1], device_id_type=MESH)
        return carry

    lax.fori_loop(1, n, greet, 0)

    def cols(c):
        return pl.ds(c * part, part)

    expert = lax.broadcasted_iota(jnp.int32, (n, rows_dev), 0)
    tri = (
        lax.broadcasted_iota(jnp.int32, (rows_dev, rows_dev), 0)
        < lax.broadcasted_iota(jnp.int32, (rows_dev, rows_dev), 1)
    ).astype(f32).astype(bf16)
    taken = jnp.zeros((n, 1), f32)
    slots = []
    for k in range(ids_ref.shape[0]):
        ids = ids_ref[pl.ds(k, 1), :]
        named = (expert == ids).astype(f32)
        ahead = jnp.dot(named.astype(bf16), tri, preferred_element_type=f32) + taken
        rank = jnp.sum(named * ahead, axis=0, keepdims=True)
        taken = taken + jnp.sum(named, axis=1, keepdims=True)
        slots.append(ids * cap + rank.astype(jnp.int32))

    heads = heads_ref[...]
    total = jnp.zeros((rows_dev, 1), f32)
    for c in range(chunks):
        firsts[c].wait()
        proj = jnp.dot(heads, ow_ref[:, cols(c)], preferred_element_type=f32)
        comb[:, cols(c)] = proj
        total = total + jnp.sum(proj * proj, axis=1, keepdims=True)
    scale = lax.rsqrt(total / width + NORM_EPS)
    total = jnp.zeros((rows_dev, 1), f32)
    loads[3].wait()
    for c in range(chunks):
        wide = res_ref[:, cols(c)].astype(f32) + comb[:, cols(c)] * scale * mix_ref[:, cols(c)]
        stream[:, cols(c)] = wide.astype(bf16)
        wide = stream[:, cols(c)].astype(f32)
        total = total + jnp.sum(wide * wide, axis=1, keepdims=True)
    scale = lax.rsqrt(total / width + NORM_EPS)
    for c in range(chunks):
        wide = stream[:, cols(c)].astype(f32)
        normed[:, cols(c)] = (wide * scale * pre_ref[:, cols(c)]).astype(bf16)
    pl.semaphore_wait(barrier, n - 1)

    def window(ref, at, c):
        if fold and c == last:
            return ref.at[at, pl.ds(0, keep), cols(c)]
        return ref.at[at, :, cols(c)]

    def send_all(src, dst, c, slot):
        def one(o, carry):
            d, where = peer(o)
            pltpu.make_async_remote_copy(
                src_ref=window(src, d, c),
                dst_ref=window(dst, me, c),
                send_sem=send_sem.at[slot],
                recv_sem=recv_sem.at[slot],
                device_id=where,
                device_id_type=MESH,
            ).start()
            return carry

        pltpu.make_async_copy(window(src, me, c), window(dst, me, c), own_sem.at[slot]).start()
        lax.fori_loop(1, n, one, 0)

    def all_copies(src, dst, c, slot):
        return pltpu.make_async_remote_copy(
            src_ref=window(src, pl.ds(0, n - 1), c),
            dst_ref=window(dst, pl.ds(0, n - 1), c),
            send_sem=send_sem.at[slot],
            recv_sem=recv_sem.at[slot],
            device_id=peer(1)[1],
            device_id_type=MESH,
        )

    def wait_all(src, dst, c, slot):
        pltpu.make_async_copy(window(src, me, c), window(dst, me, c), own_sem.at[slot]).wait()
        all_copies(src, dst, c, slot).wait_recv()

    spare = lax.broadcasted_iota(jnp.int32, (group, 8, part), 1)

    def unfold(ref):
        def one(g, carry):
            at = pl.ds(g * group, group)
            new = jnp.zeros((group, 8, part), f32)
            for c in range(last):
                tail = ref[at, keep:cap, cols(c)].astype(f32)
                new = jnp.where(spare == c, tail[:, 6:7], new)
                new = jnp.where(spare == last + c, tail[:, 7:8], new)
            ref[at, keep:cap, cols(last)] = new.astype(bf16)
            return carry

        lax.fori_loop(0, GROUPS, one, 0)

    for c in range(chunks):

        def gather(g, carry, c=c):
            row = g * rows + lax.broadcasted_iota(jnp.int32, (rows, rows_dev), 0)

            def named(target):
                return sum((target == slot).astype(f32) for slot in slots).astype(bf16)

            y = jnp.dot(named(row), normed[:, cols(c)], preferred_element_type=f32)
            if fold and c < last:
                at = lax.rem(row, cap)
                aim = jnp.where(at == tight, row - 6 + c, jnp.where(at == tight + 1, row - 4 + c, -1))
                y = y + jnp.dot(named(aim), normed[:, cols(last)], preferred_element_type=f32)
            sent[pl.ds(g * group, group), :, cols(c)] = y.astype(bf16).reshape(group, cap, part)
            return carry

        lax.fori_loop(0, GROUPS, gather, 0)
        send_all(sent, arrived, c, c)

    def weights(g, carry):
        at = pl.ds(pl.multiple_of(g * WEIGH_COLS, WEIGH_COLS), WEIGH_COLS)
        row = g * WEIGH_COLS + lax.broadcasted_iota(jnp.int32, (WEIGH_COLS, rows_dev), 0)
        mix = sum(
            jnp.where(row == slot, weight_ref[pl.ds(k, 1), :], 0.0) for k, slot in enumerate(slots)
        ).T
        for i in range(weigh.shape[0]):
            piece = mix.astype(bf16)
            weigh[i, :, at] = piece
            mix = mix - piece.astype(f32)
        return carry

    lax.fori_loop(0, n * cap // WEIGH_COLS, weights, 0)
    for load in loads[:2]:
        load.wait()

    for c in range(chunks):
        wait_all(sent, arrived, c, c)

        def gate_up(g, carry, c=c):
            x = arrived[pl.ds(g * group, group), :, cols(c)].reshape(rows, part)
            at = pl.ds(pl.multiple_of(g * rows, rows), rows)
            gate = jnp.dot(x, wg[cols(c), :], preferred_element_type=f32)
            up = jnp.dot(x, wu[cols(c), :], preferred_element_type=f32)
            if c > 0:
                gate, up = gate + gate_acc[at, :], up + up_acc[at, :]
            if c < last:
                gate_acc[at, :] = gate
                up_acc[at, :] = up
            else:
                hidden[at, :] = (jax.nn.silu(gate) * up).astype(bf16)
            return carry

        lax.fori_loop(0, GROUPS, gate_up, 0)
        if fold and c == last - 1:
            unfold(arrived)
    loads[2].wait()
    order = (last, *range(last))
    for c in order:

        def down(g, carry, c=c):
            at = pl.ds(pl.multiple_of(g * rows, rows), rows)
            some = pl.ds(g * group, group)
            y = jnp.dot(hidden[at, :], wd[:, cols(c)], preferred_element_type=f32)
            made[some, :, cols(c)] = y.astype(bf16).reshape(group, cap, part)
            if fold and c < last:
                tail = made[some, keep:cap, cols(c)].astype(f32)
                other = made[some, keep:cap, cols(last)].astype(f32)
                tail = jnp.where(spare == 6, other[:, c : c + 1], tail)
                tail = jnp.where(spare == 7, other[:, last + c : last + c + 1], tail)
                made[some, keep:cap, cols(c)] = tail.astype(bf16)
            return carry

        lax.fori_loop(0, GROUPS, down, 0)
        send_all(made, returned, c, chunks + c)
    total = jnp.zeros((rows_dev, 1), f32)

    def combine(c, total):
        back = returned[:, :, cols(c)].reshape(n * cap, part)
        mixed = sum(
            jnp.dot(weigh[i], back, preferred_element_type=f32) for i in range(weigh.shape[0])
        )
        comb[:, cols(c)] = mixed
        return total + jnp.sum(mixed * mixed, axis=1, keepdims=True)

    for c in order:
        wait_all(made, returned, c, chunks + c)
        if not (fold and c == last):
            total = combine(c, total)
    if fold:
        unfold(returned)
        total = combine(last, total)
    scale = lax.rsqrt(total / width + NORM_EPS)
    for c in range(chunks):
        o_ref[:, cols(c)] = (
            stream[:, cols(c)].astype(f32) + comb[:, cols(c)] * scale * post_ref[:, cols(c)]
        ).astype(bf16)
    for c in range(chunks):
        all_copies(sent, arrived, c, c).wait_send()
        all_copies(made, returned, c, chunks + c).wait_send()


def experts(heads, out_weight, residual, gain_mix, gain_pre, gain_post, ids, weight, w_gate, w_up, w_down, n, n_tp, tight):
    rows_dev, width = residual.shape
    cap = (tight + 7) // 8 * 8
    hidden = w_gate.shape[1]
    slots = n * cap
    chunks = CHUNKS
    vmem = pl.BlockSpec(memory_space=pltpu.VMEM)
    hbm = pl.BlockSpec(memory_space=pl.ANY)
    bf16, f32 = jnp.bfloat16, jnp.float32
    return pl.pallas_call(
        functools.partial(expert_kernel, n_tp=n_tp, chunks=chunks, tight=tight),
        out_shape=jax.ShapeDtypeStruct(residual.shape, bf16),
        in_specs=[vmem] + [hbm] * 2 + [vmem] * 5 + [hbm] * 3,
        out_specs=vmem,
        scratch_shapes=[
            pltpu.VMEM(out_weight.shape, bf16),
            pltpu.VMEM(residual.shape, bf16),
            pltpu.VMEM((n, cap, width), bf16),
            pltpu.VMEM((n, cap, width), bf16),
            pltpu.VMEM((n, cap, width), bf16),
            pltpu.VMEM((n, cap, width), bf16),
            pltpu.VMEM(w_gate.shape, bf16),
            pltpu.VMEM(w_up.shape, bf16),
            pltpu.VMEM(w_down.shape, bf16),
            pltpu.VMEM((slots, hidden), f32),
            pltpu.VMEM((slots, hidden), f32),
            pltpu.VMEM((slots, hidden), bf16),
            pltpu.VMEM(residual.shape, f32),
            pltpu.VMEM(residual.shape, bf16),
            pltpu.VMEM(residual.shape, bf16),
            pltpu.VMEM((2, rows_dev, slots), bf16),
            pltpu.SemaphoreType.DMA((4 + chunks,)),
            pltpu.SemaphoreType.DMA((2 * chunks,)),
            pltpu.SemaphoreType.DMA((2 * chunks,)),
            pltpu.SemaphoreType.DMA((2 * chunks,)),
        ],
        compiler_params=pltpu.CompilerParams(
            collective_id=1, has_side_effects=True, vmem_limit_bytes=56 * 2**20
        ),
        name="experts",
    )(heads, out_weight, residual, gain_mix, gain_pre, gain_post, ids, weight, w_gate, w_up, w_down)


def local(
    queries,
    key_rows,
    value_rows,
    cum_gate,
    residual,
    out_weight,
    gain_mix,
    gain_pre,
    gain_post,
    route_ids,
    route_weight,
    w_gate,
    w_up,
    w_down,
):
    n_sp, n_tp = lax.axis_size("sp"), lax.axis_size("tp")
    rows_dev = residual.shape[0]
    head_rows = attend(queries, key_rows, value_rows, cum_gate, n_sp, n_tp)
    top_count = route_ids.shape[1]
    experts_all = n_sp * n_tp
    tight = max(2, (4 * rows_dev * top_count + 3 * experts_all - 1) // (3 * experts_all))
    return experts(
        head_rows, out_weight, residual, gain_mix[None], gain_pre[None], gain_post[None],
        route_ids.T, route_weight.T, w_gate[0], w_up[0], w_down[0], experts_all, n_tp, tight,
    )


def solution(mesh):
    return jax.shard_map(
        local,
        mesh=mesh,
        in_specs=(
            P("sp", "tp"),
            P("sp", "tp"),
            P("sp", "tp"),
            P("tp", None),
            P(("sp", "tp"), None),
            P(),
            P(),
            P(),
            P(),
            P(("sp", "tp"), None),
            P(("sp", "tp"), None),
            P(("sp", "tp"), None, None),
            P(("sp", "tp"), None, None),
            P(("sp", "tp"), None, None),
        ),
        out_specs=P(("sp", "tp"), None),
        check_vma=False,
    )
```

```python
import functools
import math

import jax
import jax.numpy as jnp
from jax import lax
from jax.experimental import pallas as pl
from jax.experimental.pallas import tpu as pltpu
from jax.sharding import PartitionSpec as P

HEAD_DIM = 64
NORM_EPS = 1e-06
MASKED = -1e30
MESH = pl.DeviceIdType.MESH
CHUNKS = 4
GROUPS = 4
EXP2_SCALE = math.log2(math.e)
WEIGH_COLS = 256
KV_PARTS = 4


def attend_kernel(
    q_hbm, k_hbm, v_hbm, gate_ref, o_ref,
    q_in, k_in, v_in, kv_ref, q_ref,
    kv_all, q_all, k_aug, v_turned, q_aug, side_ref, out_ref, heads_ref,
    in_sem, own_sem, q_sem, kv_sem, head_sem, send_sem, *halved, n_tp, local_heads,
):
    halves = len(halved) // 3
    peaks, accs, scores = (halved[i * halves : (i + 1) * halves] for i in range(3))
    groups = local_heads
    n_sp = q_ref.shape[0]
    shares = n_sp // groups
    tok_dev = kv_ref.shape[1]
    f32, bf16 = jnp.float32, jnp.bfloat16
    chunk = 2 * q_ref.shape[1]
    sub = chunk // n_tp
    rows_dev = sub * shares
    half_rows = chunk // halves
    lanes = 2 * HEAD_DIM
    n = n_sp * n_tp
    sp, tp = lax.axis_index("sp"), lax.axis_index("tp")
    me = sp * n_tp + tp
    group, rank = sp // shares, lax.rem(sp, shares)

    def plane(s):
        down = jnp.where(s <= group, group - s, s)
        up = jnp.where(s <= groups - 1 - group, group + s, groups - 1 - s)
        return jnp.where(2 * group < groups, down, up)

    def target(s):
        down = jnp.where(group > 0, groups + group - s, s)
        down = jnp.where(s <= group, group - s, down)
        up = jnp.where(group < groups - 1, s - groups + group, groups - 1 - s)
        up = jnp.where(s <= groups - 1 - group, group + s, up)
        return jnp.where(2 * group < groups, down, up)

    def block_at(i):
        return plane(i // shares) * shares + lax.rem(rank + lax.rem(i, shares), shares)

    loads = [
        pltpu.make_async_copy(src, dst, in_sem.at[i])
        for i, (src, dst) in enumerate(((q_hbm, q_in), (k_hbm, k_in), (v_hbm, v_in)))
    ]
    for load in loads:
        load.start()
    barrier = pltpu.get_barrier_semaphore()

    def greet(o, carry):
        d = lax.rem(me + o, n)
        where = (d // n_tp, lax.rem(d, n_tp))
        pl.semaphore_signal(barrier, inc=1, device_id=where, device_id_type=MESH)
        return carry

    lax.fori_loop(1, n, greet, 0)
    for load in loads:
        load.wait()
    for h in range(groups):
        head = pl.ds(h * HEAD_DIM, HEAD_DIM)
        kv_ref[h] = jnp.concatenate((k_in[:, head], v_in[:, head]), axis=1)
        for r in range(shares):
            for t in range(n_tp // 2):
                low, high = (
                    q_in[pl.ds((t + half) * rows_dev + r * sub, sub), head]
                    for half in (0, n_tp // 2)
                )
                q_ref[h * shares + r, pl.ds(t * sub, sub)] = jnp.concatenate((low, high), axis=1)
    kv_all[sp] = kv_ref[group]
    q_all[sp] = q_ref[sp]
    pl.semaphore_wait(barrier, n - 1)

    def kv_copies(src, index, block, dest, slot):
        size = tok_dev // KV_PARTS
        return [
            pltpu.make_async_remote_copy(
                src_ref=src.at[index, pl.ds(part * size, size)],
                dst_ref=kv_all.at[block, pl.ds(part * size, size)],
                send_sem=send_sem.at[slot], recv_sem=kv_sem.at[block, part],
                device_id=(dest, tp), device_id_type=MESH,
            )
            for part in range(KV_PARTS)
        ]

    def kv_send(*where):
        for copy in kv_copies(*where):
            copy.start()

    def q_copy(src, block, dest):
        return pltpu.make_async_remote_copy(
            src_ref=src, dst_ref=q_all.at[block],
            send_sem=send_sem.at[0], recv_sem=q_sem.at[block],
            device_id=(dest, tp), device_id_type=MESH,
        )

    for s in range(groups):
        for k in range(shares):
            dest = block_at(k) if s == 0 else target(s) * shares + lax.rem(rank + k, shares)
            if s or k:
                q_copy(q_ref.at[dest], sp, dest).start()
            if s == 0 and k:
                kv_send(kv_ref, group, sp, dest, 1)
            if s and k == 0:
                kv_send(kv_ref, target(s), sp, dest, 2)

    slot = lax.broadcasted_iota(jnp.int32, (8, tok_dev), 0)
    place = lax.broadcasted_iota(jnp.int32, (8, lanes), 1) - HEAD_DIM
    place = (place == lax.broadcasted_iota(jnp.int32, (8, lanes), 0)).astype(f32).astype(bf16)

    def spread(rows):
        return lax.dot_general(
            rows.astype(bf16), place, (((0,), (0,)), ((), ())), preferred_element_type=f32
        )

    def sides(block):
        at = pl.ds(pl.multiple_of(block * tok_dev, tok_dev), tok_dev)
        gate = gate_ref[pl.ds(group, 1), at] * EXP2_SCALE
        for_k = (slot < 3).astype(f32)
        for_q = ((slot >= 3) & (slot < 6)).astype(f32)
        for i in range(3):
            piece = gate.astype(bf16).astype(f32)
            gate = gate - piece
            for_k = jnp.where(slot == 3 + i, -piece, for_k)
            for_q = jnp.where(slot == i, piece, for_q)
        side_ref[...] = spread(for_q)
        k_aug[block, :, :lanes] = spread(for_k).astype(bf16)
        for t in range(n_tp):
            rows = pl.ds(t * sub, sub)
            side = side_ref[pl.ds(pl.multiple_of(t * rows_dev + rank * sub, sub), sub)]
            q_aug[block, rows, :lanes] = side.astype(bf16)
        for h in range(halves):
            peaks[h][block] = jnp.full((1, half_rows), MASKED, f32)
            accs[h][block] = jnp.zeros((HEAD_DIM + 16, half_rows), f32)

    def build(block):
        lane = lax.broadcasted_iota(jnp.int32, (tok_dev, lanes), 1)
        kv = kv_all[block].astype(f32)
        k_aug[block, :, :lanes] = jnp.where(
            lane < HEAD_DIM, kv, k_aug[block, :, :lanes].astype(f32)
        ).astype(bf16)
        k_aug[block, :, lanes:] = jnp.where(lane < HEAD_DIM, kv, 0.0).astype(bf16)
        turned = kv.T
        v_turned[block, :HEAD_DIM] = turned[HEAD_DIM:].astype(bf16)
        v_turned[block, HEAD_DIM:] = jnp.ones((16, tok_dev), bf16)
        packed = q_all[block]
        queries = jnp.concatenate((packed[:, :HEAD_DIM], packed[:, HEAD_DIM:]), axis=0)
        queries = queries.astype(f32) * (HEAD_DIM**-0.5 * EXP2_SCALE)
        high = queries.astype(bf16)
        low = (queries - high.astype(f32)).astype(bf16)
        q_aug[block, :, :lanes] = jnp.concatenate((high, q_aug[block, :, HEAD_DIM:lanes]), axis=1)
        q_aug[block, :, lanes:] = jnp.concatenate((low, jnp.zeros_like(low)), axis=1)

    def score(h, i, j):
        found = lax.dot_general(
            k_aug[j], q_aug[i, pl.ds(h * half_rows, half_rows)], (((1,), (1,)), ((), ())),
            preferred_element_type=f32,
        )
        scores[h][...] = found
        return jnp.max(found, axis=0, keepdims=True)

    def weigh(h, top, i, j, masked):
        count = tok_dev // halves * (h + 1) if masked else tok_dev
        found = scores[h][:count]
        if masked:
            key = lax.broadcasted_iota(jnp.int32, (count, 1), 0)
            row = lax.broadcasted_iota(jnp.int32, (1, half_rows), 1) + h * half_rows
            pos = row // sub * rows_dev + rank * sub + lax.rem(row, sub)
            found = jnp.where(key <= pos, found, MASKED)
            top = jnp.max(found, axis=0, keepdims=True)
        before = peaks[h][i]
        peak = jnp.maximum(before, top)
        probs = jnp.exp2(found - peak).astype(bf16)
        peaks[h][i] = peak
        accs[h][i] = accs[h][i] * jnp.exp2(before - peak) + jnp.dot(
            v_turned[j, :, :count], probs, preferred_element_type=f32
        )

    def step(i, j, i_next, j_next, top, masked):
        for h in range(halves):
            ahead = (h + 1, i, j) if h + 1 < halves else (0, i_next, j_next)
            early = h + 1 < halves
            if early:
                found = score(*ahead)
            weigh(h, top, i, j, masked)
            if not early and not masked:
                found = score(*ahead)
            top = found if early or not masked else top
        return top

    def head_copy(block, t):
        slot = block * n_tp + t
        return pltpu.make_async_remote_copy(
            src_ref=out_ref.at[slot], dst_ref=heads_ref.at[me],
            send_sem=send_sem.at[4], recv_sem=head_sem,
            device_id=(block, t), device_id_type=MESH,
        )

    own_head = pltpu.make_async_copy(out_ref.at[me], heads_ref.at[me], own_sem)

    def finish(block):
        parts = [accs[h][block] for h in range(halves)]
        parts = [(acc[:HEAD_DIM] / acc[HEAD_DIM : HEAD_DIM + 1]).T for acc in parts]
        out = jnp.concatenate(parts, axis=0)
        half = sub // 2
        for t in range(n_tp):
            top, low = (out[t * sub + at : t * sub + at + half] for at in (0, half))
            out_ref[block * n_tp + t] = jnp.concatenate((top, low), axis=1).astype(jnp.bfloat16)
        for t in range(n_tp):
            mine = (block == sp) & (tp == t)

            @pl.when(mine)
            def _():
                own_head.start()

            @pl.when(jnp.logical_not(mine))
            def _(t=t):
                head_copy(block, t).start()

    def relay(i):
        block = block_at(i)
        for part in range(KV_PARTS):
            kv_copies(kv_all, block, block, block, 3)[part].wait_recv()
            for k in range(1, shares):
                dest = group * shares + lax.rem(rank + k, shares)
                kv_copies(kv_all, block, block, dest, 3)[part].start()

    def one_block(i, carry):
        block = block_at(i)
        s, k = i // shares, lax.rem(i, shares)
        turn = (k == shares - 1) & (s < groups - 1)
        outer = (group == 0) | (group == groups - 1)
        early = (s > 0) & jnp.where(outer, s < groups - 2, s == groups - 2)

        @pl.when(turn & early)
        def _():
            relay(i + 1)

        @pl.when(i > 0)
        def _():
            q_copy(q_all.at[block], block, block).wait_recv()

        @pl.when(k > 0)
        def _():
            for copy in kv_copies(kv_all, block, block, block, 3):
                copy.wait_recv()

        build(block)

        def blocks(m):
            other = jnp.where(m < i, block_at(jnp.maximum(i - 1 - m, 0)), block)
            return jnp.maximum(block, other), jnp.minimum(block, other)

        def pair(m, top):
            other = block_at(i - 1 - m)
            top = step(*blocks(m), *blocks(m + 1), top, False)

            @pl.when(i == n_sp - 1)
            def _():
                finish(other)

            return top

        top = lax.fori_loop(0, i, pair, score(0, *blocks(0)))
        step(block, block, block, block, top, True)

        @pl.when(turn & jnp.logical_not(early))
        def _():
            relay(i + 1)

        return carry

    def one_side(i, carry):
        sides(block_at(i))
        return carry

    sides(sp)
    one_block(0, 0)
    lax.fori_loop(1, n_sp, one_side, 0)
    lax.fori_loop(1, n_sp, one_block, 0)
    finish(block_at(n_sp - 1))
    own_head.wait()

    def sent(buf, count, slot):
        if count:
            pltpu.make_async_remote_copy(
                src_ref=buf.at[pl.ds(0, count)], dst_ref=buf.at[pl.ds(0, count)],
                send_sem=send_sem.at[slot], recv_sem=head_sem,
                device_id=(sp, tp), device_id_type=MESH,
            ).wait_send()

    pltpu.make_async_remote_copy(
        src_ref=heads_ref.at[pl.ds(0, n - 1)], dst_ref=heads_ref.at[pl.ds(0, n - 1)],
        send_sem=send_sem.at[4], recv_sem=head_sem,
        device_id=(sp, tp), device_id_type=MESH,
    ).wait_recv()
    half = sub // 2
    for t in range(n_tp):
        for h in range(0, local_heads, 2):
            for r in range(shares):
                left = heads_ref[(h * shares + r) * n_tp + t]
                right = heads_ref[((h + 1) * shares + r) * n_tp + t]
                for part in range(2):
                    cols = slice(part * HEAD_DIM, (part + 1) * HEAD_DIM)
                    o_ref[
                        pl.ds((2 * r + part) * half, half),
                        pl.ds((t * local_heads + h) * HEAD_DIM, 2 * HEAD_DIM),
                    ] = jnp.concatenate((left[:, cols], right[:, cols]), axis=1)
    sent(q_ref, n_sp - 1, 0)
    sent(kv_all, shares - 1, 1)
    sent(kv_all, groups - 1, 2)
    sent(kv_all, (groups - 1) * (shares - 1), 3)
    sent(out_ref, n - 1, 4)


def attend(queries, key_rows, value_rows, gate, n_sp, n_tp):
    tok_dev, width = queries.shape
    local_heads = width // HEAD_DIM
    lanes = 2 * HEAD_DIM
    shares = n_sp // local_heads
    rows_dev = tok_dev // n_tp
    sub = rows_dev // shares
    chunk = n_tp * sub
    n = n_sp * n_tp
    halves = 2 if chunk >= 512 else 1
    half_rows = chunk // halves
    bf16, f32 = jnp.bfloat16, jnp.float32
    vmem = pl.BlockSpec(memory_space=pltpu.VMEM)
    hbm = pl.BlockSpec(memory_space=pl.ANY)
    return pl.pallas_call(
        functools.partial(attend_kernel, n_tp=n_tp, local_heads=local_heads),
        out_shape=jax.ShapeDtypeStruct((rows_dev, n_tp * width), bf16),
        in_specs=[hbm] * 3 + [vmem],
        out_specs=vmem,
        scratch_shapes=[pltpu.VMEM((tok_dev, width), bf16)] * 3
        + [
            pltpu.VMEM((local_heads, tok_dev, lanes), bf16),
            pltpu.VMEM((n_sp, chunk // 2, lanes), bf16),
            pltpu.VMEM((n_sp, tok_dev, lanes), bf16),
            pltpu.VMEM((n_sp, chunk // 2, lanes), bf16),
            pltpu.VMEM((n_sp, tok_dev, 2 * lanes), bf16),
            pltpu.VMEM((n_sp, HEAD_DIM + 16, tok_dev), bf16),
            pltpu.VMEM((n_sp, chunk, 2 * lanes), bf16),
            pltpu.VMEM((tok_dev, lanes), f32),
            pltpu.VMEM((n, sub // 2, lanes), bf16),
            pltpu.VMEM((n, sub // 2, lanes), bf16),
            pltpu.SemaphoreType.DMA((3,)),
            pltpu.SemaphoreType.DMA,
            pltpu.SemaphoreType.DMA((n_sp,)),
            pltpu.SemaphoreType.DMA((n_sp, KV_PARTS)),
            pltpu.SemaphoreType.DMA,
            pltpu.SemaphoreType.DMA((5,)),
        ]
        + [pltpu.VMEM((n_sp, 1, half_rows), f32)] * halves
        + [pltpu.VMEM((n_sp, HEAD_DIM + 16, half_rows), f32)] * halves
        + [pltpu.VMEM((tok_dev, half_rows), f32)] * halves,
        compiler_params=pltpu.CompilerParams(
            collective_id=0, has_side_effects=True, vmem_limit_bytes=60 * 2**20
        ),
        name="attend",
    )(queries, key_rows, value_rows, gate)


def expert_kernel(
    heads_ref, ow_hbm, res_hbm, mix_ref, pre_ref, post_ref, ids_ref, weight_ref, wg_hbm, wu_hbm, wd_hbm, o_ref,
    ow_ref, res_ref, sent, arrived, made, returned, wg, wu, wd, gate_acc, up_acc, hidden, comb, stream, normed, weigh,
    w_sem, own_sem, send_sem, recv_sem, *, n_tp, chunks, tight,
):
    n, cap, width = sent.shape
    rows_dev = stream.shape[0]
    part = width // chunks
    last = chunks - 1
    fold = chunks == 4 and cap - tight == 2 and tight > 8
    keep = cap - 8
    group = n // GROUPS
    rows = group * cap
    f32, bf16 = jnp.float32, jnp.bfloat16
    sp, tp = lax.axis_index("sp"), lax.axis_index("tp")
    me = sp * n_tp + tp

    def peer(o):
        d = lax.rem(me + o, n)
        return d, (d // n_tp, lax.rem(d, n_tp))

    firsts = [
        pltpu.make_async_copy(
            ow_hbm.at[:, pl.ds(c * part, part)], ow_ref.at[:, pl.ds(c * part, part)], w_sem.at[4 + c]
        )
        for c in range(chunks)
    ]
    loads = [
        pltpu.make_async_copy(src, dst, w_sem.at[i])
        for i, (src, dst) in enumerate(
            ((wg_hbm, wg), (wu_hbm, wu), (wd_hbm, wd), (res_hbm, res_ref))
        )
    ]
    for load in (*firsts, loads[3], *loads[:3]):
        load.start()

    barrier = pltpu.get_barrier_semaphore()

    def greet(o, carry):
        pl.semaphore_signal(barrier, inc=1, device_id=peer(o)[1], device_id_type=MESH)
        return carry

    lax.fori_loop(1, n, greet, 0)

    def cols(c):
        return pl.ds(c * part, part)

    expert = lax.broadcasted_iota(jnp.int32, (n, rows_dev), 0)
    tri = (
        lax.broadcasted_iota(jnp.int32, (rows_dev, rows_dev), 0)
        < lax.broadcasted_iota(jnp.int32, (rows_dev, rows_dev), 1)
    ).astype(f32).astype(bf16)
    taken = jnp.zeros((n, 1), f32)
    slots = []
    for k in range(ids_ref.shape[0]):
        ids = ids_ref[pl.ds(k, 1), :]
        named = (expert == ids).astype(f32)
        ahead = jnp.dot(named.astype(bf16), tri, preferred_element_type=f32) + taken
        rank = jnp.sum(named * ahead, axis=0, keepdims=True)
        taken = taken + jnp.sum(named, axis=1, keepdims=True)
        slots.append(ids * cap + rank.astype(jnp.int32))

    heads = heads_ref[...]
    total = jnp.zeros((rows_dev, 1), f32)
    for c in range(chunks):
        firsts[c].wait()
        proj = jnp.dot(heads, ow_ref[:, cols(c)], preferred_element_type=f32)
        comb[:, cols(c)] = proj
        total = total + jnp.sum(proj * proj, axis=1, keepdims=True)
    scale = lax.rsqrt(total / width + NORM_EPS)
    total = jnp.zeros((rows_dev, 1), f32)
    loads[3].wait()
    for c in range(chunks):
        wide = res_ref[:, cols(c)].astype(f32) + comb[:, cols(c)] * scale * mix_ref[:, cols(c)]
        stream[:, cols(c)] = wide.astype(bf16)
        wide = stream[:, cols(c)].astype(f32)
        total = total + jnp.sum(wide * wide, axis=1, keepdims=True)
    scale = lax.rsqrt(total / width + NORM_EPS)
    for c in range(chunks):
        wide = stream[:, cols(c)].astype(f32)
        normed[:, cols(c)] = (wide * scale * pre_ref[:, cols(c)]).astype(bf16)
    pl.semaphore_wait(barrier, n - 1)

    def window(ref, at, c):
        if fold and c == last:
            return ref.at[at, pl.ds(0, keep), cols(c)]
        return ref.at[at, :, cols(c)]

    def send_all(src, dst, c, slot):
        def one(o, carry):
            d, where = peer(o)
            pltpu.make_async_remote_copy(
                src_ref=window(src, d, c),
                dst_ref=window(dst, me, c),
                send_sem=send_sem.at[slot],
                recv_sem=recv_sem.at[slot],
                device_id=where,
                device_id_type=MESH,
            ).start()
            return carry

        pltpu.make_async_copy(window(src, me, c), window(dst, me, c), own_sem.at[slot]).start()
        lax.fori_loop(1, n, one, 0)

    def all_copies(src, dst, c, slot):
        return pltpu.make_async_remote_copy(
            src_ref=window(src, pl.ds(0, n - 1), c),
            dst_ref=window(dst, pl.ds(0, n - 1), c),
            send_sem=send_sem.at[slot],
            recv_sem=recv_sem.at[slot],
            device_id=peer(1)[1],
            device_id_type=MESH,
        )

    def wait_all(src, dst, c, slot):
        pltpu.make_async_copy(window(src, me, c), window(dst, me, c), own_sem.at[slot]).wait()
        all_copies(src, dst, c, slot).wait_recv()

    spare = lax.broadcasted_iota(jnp.int32, (group, 8, part), 1)

    def unfold(ref):
        def one(g, carry):
            at = pl.ds(g * group, group)
            new = jnp.zeros((group, 8, part), f32)
            for c in range(last):
                tail = ref[at, keep:cap, cols(c)].astype(f32)
                new = jnp.where(spare == c, tail[:, 6:7], new)
                new = jnp.where(spare == last + c, tail[:, 7:8], new)
            ref[at, keep:cap, cols(last)] = new.astype(bf16)
            return carry

        lax.fori_loop(0, GROUPS, one, 0)

    for c in range(chunks):

        def gather(g, carry, c=c):
            row = g * rows + lax.broadcasted_iota(jnp.int32, (rows, rows_dev), 0)

            def named(target):
                return sum((target == slot).astype(f32) for slot in slots).astype(bf16)

            y = jnp.dot(named(row), normed[:, cols(c)], preferred_element_type=f32)
            if fold and c < last:
                at = lax.rem(row, cap)
                aim = jnp.where(at == tight, row - 6 + c, jnp.where(at == tight + 1, row - 4 + c, -1))
                y = y + jnp.dot(named(aim), normed[:, cols(last)], preferred_element_type=f32)
            sent[pl.ds(g * group, group), :, cols(c)] = y.astype(bf16).reshape(group, cap, part)
            return carry

        lax.fori_loop(0, GROUPS, gather, 0)
        send_all(sent, arrived, c, c)

    def weights(g, carry):
        at = pl.ds(pl.multiple_of(g * WEIGH_COLS, WEIGH_COLS), WEIGH_COLS)
        row = g * WEIGH_COLS + lax.broadcasted_iota(jnp.int32, (WEIGH_COLS, rows_dev), 0)
        mix = sum(
            jnp.where(row == slot, weight_ref[pl.ds(k, 1), :], 0.0) for k, slot in enumerate(slots)
        ).T
        for i in range(weigh.shape[0]):
            piece = mix.astype(bf16)
            weigh[i, :, at] = piece
            mix = mix - piece.astype(f32)
        return carry

    lax.fori_loop(0, n * cap // WEIGH_COLS, weights, 0)
    for load in loads[:2]:
        load.wait()

    for c in range(chunks):
        wait_all(sent, arrived, c, c)

        def gate_up(g, carry, c=c):
            x = arrived[pl.ds(g * group, group), :, cols(c)].reshape(rows, part)
            at = pl.ds(pl.multiple_of(g * rows, rows), rows)
            gate = jnp.dot(x, wg[cols(c), :], preferred_element_type=f32)
            up = jnp.dot(x, wu[cols(c), :], preferred_element_type=f32)
            if c > 0:
                gate, up = gate + gate_acc[at, :], up + up_acc[at, :]
            if c < last:
                gate_acc[at, :] = gate
                up_acc[at, :] = up
            else:
                hidden[at, :] = (jax.nn.silu(gate) * up).astype(bf16)
            return carry

        lax.fori_loop(0, GROUPS, gate_up, 0)
        if fold and c == last - 1:
            unfold(arrived)
    loads[2].wait()
    order = (last, *range(last))
    for c in order:

        def down(g, carry, c=c):
            at = pl.ds(pl.multiple_of(g * rows, rows), rows)
            some = pl.ds(g * group, group)
            y = jnp.dot(hidden[at, :], wd[:, cols(c)], preferred_element_type=f32)
            made[some, :, cols(c)] = y.astype(bf16).reshape(group, cap, part)
            if fold and c < last:
                tail = made[some, keep:cap, cols(c)].astype(f32)
                other = made[some, keep:cap, cols(last)].astype(f32)
                tail = jnp.where(spare == 6, other[:, c : c + 1], tail)
                tail = jnp.where(spare == 7, other[:, last + c : last + c + 1], tail)
                made[some, keep:cap, cols(c)] = tail.astype(bf16)
            return carry

        lax.fori_loop(0, GROUPS, down, 0)
        send_all(made, returned, c, chunks + c)
    total = jnp.zeros((rows_dev, 1), f32)

    def combine(c, total):
        back = returned[:, :, cols(c)].reshape(n * cap, part)
        mixed = sum(
            jnp.dot(weigh[i], back, preferred_element_type=f32) for i in range(weigh.shape[0])
        )
        comb[:, cols(c)] = mixed
        return total + jnp.sum(mixed * mixed, axis=1, keepdims=True)

    for c in order:
        wait_all(made, returned, c, chunks + c)
        if not (fold and c == last):
            total = combine(c, total)
    if fold:
        unfold(returned)
        total = combine(last, total)
    scale = lax.rsqrt(total / width + NORM_EPS)
    for c in range(chunks):
        o_ref[:, cols(c)] = (
            stream[:, cols(c)].astype(f32) + comb[:, cols(c)] * scale * post_ref[:, cols(c)]
        ).astype(bf16)
    for c in range(chunks):
        all_copies(sent, arrived, c, c).wait_send()
        all_copies(made, returned, c, chunks + c).wait_send()


def experts(heads, out_weight, residual, gain_mix, gain_pre, gain_post, ids, weight, w_gate, w_up, w_down, n, n_tp, tight):
    rows_dev, width = residual.shape
    cap = (tight + 7) // 8 * 8
    hidden = w_gate.shape[1]
    slots = n * cap
    chunks = CHUNKS
    vmem = pl.BlockSpec(memory_space=pltpu.VMEM)
    hbm = pl.BlockSpec(memory_space=pl.ANY)
    bf16, f32 = jnp.bfloat16, jnp.float32
    return pl.pallas_call(
        functools.partial(expert_kernel, n_tp=n_tp, chunks=chunks, tight=tight),
        out_shape=jax.ShapeDtypeStruct(residual.shape, bf16),
        in_specs=[vmem] + [hbm] * 2 + [vmem] * 5 + [hbm] * 3,
        out_specs=vmem,
        scratch_shapes=[
            pltpu.VMEM(out_weight.shape, bf16),
            pltpu.VMEM(residual.shape, bf16),
            pltpu.VMEM((n, cap, width), bf16),
            pltpu.VMEM((n, cap, width), bf16),
            pltpu.VMEM((n, cap, width), bf16),
            pltpu.VMEM((n, cap, width), bf16),
            pltpu.VMEM(w_gate.shape, bf16),
            pltpu.VMEM(w_up.shape, bf16),
            pltpu.VMEM(w_down.shape, bf16),
            pltpu.VMEM((slots, hidden), f32),
            pltpu.VMEM((slots, hidden), f32),
            pltpu.VMEM((slots, hidden), bf16),
            pltpu.VMEM(residual.shape, f32),
            pltpu.VMEM(residual.shape, bf16),
            pltpu.VMEM(residual.shape, bf16),
            pltpu.VMEM((2, rows_dev, slots), bf16),
            pltpu.SemaphoreType.DMA((4 + chunks,)),
            pltpu.SemaphoreType.DMA((2 * chunks,)),
            pltpu.SemaphoreType.DMA((2 * chunks,)),
            pltpu.SemaphoreType.DMA((2 * chunks,)),
        ],
        compiler_params=pltpu.CompilerParams(
            collective_id=1, has_side_effects=True, vmem_limit_bytes=56 * 2**20
        ),
        name="experts",
    )(heads, out_weight, residual, gain_mix, gain_pre, gain_post, ids, weight, w_gate, w_up, w_down)


def local(
    queries,
    key_rows,
    value_rows,
    cum_gate,
    residual,
    out_weight,
    gain_mix,
    gain_pre,
    gain_post,
    route_ids,
    route_weight,
    w_gate,
    w_up,
    w_down,
):
    n_sp, n_tp = lax.axis_size("sp"), lax.axis_size("tp")
    rows_dev = residual.shape[0]
    head_rows = attend(queries, key_rows, value_rows, cum_gate, n_sp, n_tp)
    top_count = route_ids.shape[1]
    experts_all = n_sp * n_tp
    tight = max(2, (4 * rows_dev * top_count + 3 * experts_all - 1) // (3 * experts_all))
    return experts(
        head_rows, out_weight, residual, gain_mix[None], gain_pre[None], gain_post[None],
        route_ids.T, route_weight.T, w_gate[0], w_up[0], w_down[0], experts_all, n_tp, tight,
    )


def solution(mesh):
    return jax.shard_map(
        local,
        mesh=mesh,
        in_specs=(
            P("sp", "tp"),
            P("sp", "tp"),
            P("sp", "tp"),
            P("tp", None),
            P(("sp", "tp"), None),
            P(),
            P(),
            P(),
            P(),
            P(("sp", "tp"), None),
            P(("sp", "tp"), None),
            P(("sp", "tp"), None, None),
            P(("sp", "tp"), None, None),
            P(("sp", "tp"), None, None),
        ),
        out_specs=P(("sp", "tp"), None),
        check_vma=False,
    )
```
